32 devices in a mesh: sp: 8 (over z, x), tp: 4 (over y, core).
Axes of the slice: x: 2, y: 2, z: 4, core: 2. Of those that a mesh axis runs over, the one named last changes fastest.
Arguments:
- features: bfloat16 [3072, 2048], P('sp', 'tp'), may hold values from -6 to 6
- norm_gain: float32 [2048], replicated, may hold values from 0.28 to 10
- w_query: bfloat16 [2048, 1024], P(None, 'tp'), may hold values from -0.125 to 0.125
- w_key: bfloat16 [2048, 512], P(None, 'tp'), may hold values from -0.125 to 0.125
- w_value: bfloat16 [2048, 512], P(None, 'tp'), may hold values from -0.125 to 0.125
- head_sinks: float32 [16], P('tp'), may hold values from 1 to 5
- w_query_latent: bfloat16 [2048, 512], replicated, may hold values from -0.125 to 0.125
- w_kv_latent: bfloat16 [2048, 512], replicated, may hold values from -0.125 to 0.125
- w_rope_key: bfloat16 [2048, 64], replicated, may hold values from -0.125 to 0.125
- query_latent_gain: float32 [512], replicated, may hold values from 0.28 to 10
- kv_latent_gain: float32 [512], replicated, may hold values from 0.28 to 10
- w_query_content: bfloat16 [512, 1024], P(None, 'tp'), may hold values from -0.25 to 0.25
- w_query_rotary: bfloat16 [512, 512], P(None, 'tp'), may hold values from -0.25 to 0.25
- w_key_up: bfloat16 [512, 1024], P(None, 'tp'), may hold values from -0.25 to 0.25
- w_value_up: bfloat16 [512, 1024], P(None, 'tp'), may hold values from -0.25 to 0.25
- w_branch_window: bfloat16 [1024, 2048], P('tp'), may hold values from -0.1875 to 0.1875
- w_branch_latent: bfloat16 [1024, 2048], P('tp'), may hold values from -0.1875 to 0.1875
- w_gate_window: bfloat16 [2048, 2048], P(None, 'tp'), may hold values from -0.125 to 0.125
- w_gate_latent: bfloat16 [2048, 2048], P(None, 'tp'), may hold values from -0.125 to 0.125
Outputs:
- mixed: bfloat16 [3072, 2048], P('sp', 'tp')
The draws below stay inside these ranges and needn't reach their ends.
All inputs are finite; a program needn't handle non-finite values.
Results may differ from the reference program's by a relative error of at most 0.018.
The reference program's roundings to bfloat16 on the way count: a program that leaves them out, or rounds other values in their place, can miss the bound.
Values may be sent and summed in bfloat16 or wider, within the bound.
A program may use at most 128 MiB of HBM per device.

```python
import jax
import jax.numpy as jnp
from jax import lax

D = 2048
Q_HEADS = 16
KV_HEADS = 8
HEAD = 64
WINDOW = 128
LAT_HEADS = 8
Q_LATENT = 512
KV_LATENT = 512
NOPE = 128
ROPE = 64
VDIM = 128
TOK_DEV = 384
SEQ = 3072


def gain_draw(key, length):
    return 1.0 + 0.18 * jnp.clip(jax.random.normal(key, (length,), jnp.float32), -4.0, 4.0)


def draw_norm_gain(key, part):
    return gain_draw(jax.random.fold_in(key, 11), D)


def draw_query_latent_gain(key, part):
    return gain_draw(jax.random.fold_in(key, 23), Q_LATENT)


def draw_kv_latent_gain(key, part):
    return gain_draw(jax.random.fold_in(key, 37), KV_LATENT)


def block_levels(stream_key, extent, cuts, smallest, top_value):
    def one(axis_at, blocks):
        steps = jax.random.uniform(jax.random.fold_in(jax.random.fold_in(stream_key, 6), axis_at), (blocks,), jnp.float32, smallest / len(cuts), top_value / len(cuts))
        return jnp.repeat(jnp.exp(steps), extent[axis_at] // blocks).reshape((-1,) + (1,) * (len(extent) - axis_at - 1))

    loudness = one(*cuts[0])
    for cut in cuts[1:]:
        loudness = loudness * one(*cut)
    return loudness


def normal_values(stream_key, dims, width, reach, pieces=(), kind=jnp.bfloat16):
    loudness = block_levels(stream_key, dims, pieces, -0.22, 0.18) if pieces else 1.0
    values = jax.random.normal(stream_key, dims, jnp.float32) * width * loudness
    return jnp.minimum(jnp.maximum(values, -reach), reach).astype(kind)


def setup_inputs(seed: int = 0) -> dict:
    key_of = jax.random.split(jax.random.key(seed), 20)
    return {
        "features": normal_values(key_of[0], (SEQ, D), 1.0, 6.0, ((0, 8), (1, 4))),
        "norm_gain": draw_norm_gain(jax.random.fold_in(key_of[19], 71), 0),
        "w_query": normal_values(key_of[2], (D, Q_HEADS * HEAD), D ** -0.5, 0.125, ((1, 4),)),
        "w_key": normal_values(key_of[3], (D, KV_HEADS * HEAD), D ** -0.5, 0.125, ((1, 4),)),
        "w_value": normal_values(key_of[4], (D, KV_HEADS * HEAD), D ** -0.5, 0.125, ((1, 4),)),
        "head_sinks": jnp.clip(1.0 + 4.0 * jax.random.uniform(key_of[5], (Q_HEADS,), jnp.float32) ** block_levels(key_of[5], (Q_HEADS,), ((0, 4),), -0.2, 0.2), 1.0, 5.0),
        "w_query_latent": normal_values(key_of[6], (D, Q_LATENT), D ** -0.5, 0.125),
        "w_kv_latent": normal_values(key_of[7], (D, KV_LATENT), D ** -0.5, 0.125),
        "w_rope_key": normal_values(key_of[8], (D, ROPE), D ** -0.5, 0.125),
        "query_latent_gain": draw_query_latent_gain(jax.random.fold_in(key_of[19], 71), 0),
        "kv_latent_gain": draw_kv_latent_gain(jax.random.fold_in(key_of[19], 71), 0),
        "w_query_content": normal_values(key_of[11], (Q_LATENT, LAT_HEADS * NOPE), Q_LATENT ** -0.5, 0.25, ((1, 4),)),
        "w_query_rotary": normal_values(key_of[12], (Q_LATENT, LAT_HEADS * ROPE), Q_LATENT ** -0.5, 0.25, ((1, 4),)),
        "w_key_up": normal_values(key_of[13], (KV_LATENT, LAT_HEADS * NOPE), KV_LATENT ** -0.5, 0.25, ((1, 4),)),
        "w_value_up": normal_values(key_of[14], (KV_LATENT, LAT_HEADS * VDIM), KV_LATENT ** -0.5, 0.25, ((1, 4),)),
        "w_branch_window": normal_values(key_of[15], (Q_HEADS * HEAD, D), (Q_HEADS * HEAD) ** -0.5, 0.1875, ((0, 4),)),
        "w_branch_latent": normal_values(key_of[16], (LAT_HEADS * VDIM, D), (LAT_HEADS * VDIM) ** -0.5, 0.1875, ((0, 4),)),
        "w_gate_window": normal_values(key_of[17], (D, D), D ** -0.5, 0.125, ((1, 4),)),
        "w_gate_latent": normal_values(key_of[18], (D, D), D ** -0.5, 0.125, ((1, 4),)),
    }


EPS = 1e-06
THETA = 10000.0
NEGATIVE = -1e+30

def rms_rows(float_rows, gain_vec):
    return float_rows * lax.rsqrt(lax.optimization_barrier(jnp.mean(float_rows * float_rows, axis=-1, keepdims=True)) + EPS) * gain_vec

def rotate(float_rows, positions):
    half_width = float_rows.shape[-1] // 2
    frequencies = THETA ** (-jnp.arange(half_width, dtype=jnp.float32) / half_width)
    angles = positions.astype(jnp.float32)[:, None] * frequencies
    target = (float_rows.shape[0],) + (1,) * (float_rows.ndim - 2) + (half_width,)
    cosine = jnp.cos(angles).reshape(target)
    sine_part = jnp.sin(angles).reshape(target)
    first_half = float_rows[..., :half_width]
    second_half = float_rows[..., half_width:]
    return jnp.concatenate([first_half * cosine - second_half * sine_part, second_half * cosine + first_half * sine_part], axis=-1)

def window_attention(queries, key_ext, value_ext, sink_table, row_start):
    row_count = queries.shape[0]
    kv_heads = key_ext.shape[1] // HEAD
    group_size = queries.shape[1] // HEAD // kv_heads
    blocks = row_count // WINDOW
    query_blocks = queries.reshape(blocks, WINDOW, kv_heads, group_size, HEAD).astype(jnp.float32)

    def banded(table):
        table = table.reshape(blocks + 1, WINDOW, kv_heads, HEAD)
        return jnp.concatenate([table[:-1], table[1:]], axis=1).astype(jnp.float32)
    key_band = banded(key_ext)
    value_band = banded(value_ext)
    scores = jnp.einsum('nqhgd,nkhd->nhgqk', query_blocks, key_band) * HEAD ** (-0.5)
    query_index = jnp.arange(WINDOW, dtype=jnp.int32)[:, None]
    key_index = jnp.arange(2 * WINDOW, dtype=jnp.int32)[None, :]
    offset = query_index + WINDOW - key_index
    key_position = row_start + jnp.arange(blocks, dtype=jnp.int32)[:, None, None] * WINDOW + key_index - WINDOW
    valid_mask = ((offset >= 0) & (offset < WINDOW) & (key_position >= 0))[:, None, None]
    scores = jnp.where(valid_mask, scores, NEGATIVE)
    sink_logit = sink_table.reshape(1, kv_heads, group_size, 1, 1)
    row_top = jnp.maximum(lax.optimization_barrier(jnp.max(scores, axis=-1, keepdims=True)), sink_logit)
    weights = jnp.where(valid_mask, jnp.exp(scores - row_top), 0.0)
    denominator = lax.optimization_barrier(jnp.sum(weights, axis=-1, keepdims=True)) + jnp.exp(sink_logit - row_top)
    probabilities = (weights / denominator).astype(jnp.bfloat16).astype(jnp.float32)
    attended = jnp.einsum('nhgqk,nkhd->nqhgd', probabilities, value_band)
    return attended.astype(jnp.bfloat16).reshape(row_count, kv_heads * group_size * HEAD)

def latent_attention(query_content, query_rotary, head_keys, head_values, rope_key):
    seq_rows = query_content.shape[0]
    lat_heads = query_content.shape[1]
    blocks = seq_rows // TOK_DEV
    scale_factor = (NOPE + ROPE) ** (-0.5)
    key_float = head_keys.astype(jnp.float32)
    value_float = head_values.astype(jnp.float32)
    rope_float = rope_key.astype(jnp.float32)
    content_blocks = query_content.reshape(blocks, TOK_DEV, lat_heads, NOPE)
    rotary_blocks = query_rotary.reshape(blocks, TOK_DEV, lat_heads, ROPE)
    key_position = jnp.arange(seq_rows, dtype=jnp.int32)

    def one_block(inputs):
        content_part, rotary_part, block_index = inputs
        scores = (jnp.einsum('qhd,khd->hqk', content_part.astype(jnp.float32), key_float) + jnp.einsum('qhr,kr->hqk', rotary_part.astype(jnp.float32), rope_float)) * scale_factor
        query_position = block_index * TOK_DEV + jnp.arange(TOK_DEV, dtype=jnp.int32)
        live_mask = key_position[None, :] <= query_position[:, None]
        scores = jnp.where(live_mask, scores, NEGATIVE)
        row_top = lax.optimization_barrier(jnp.max(scores, axis=-1, keepdims=True))
        weights = jnp.where(live_mask, jnp.exp(scores - row_top), 0.0)
        rounded = weights.astype(jnp.bfloat16).astype(jnp.float32)
        attended = jnp.einsum('hqk,khd->qhd', rounded, value_float)
        denominator = jnp.transpose(lax.optimization_barrier(jnp.sum(weights, axis=-1)))[:, :, None]
        return (attended / denominator).astype(jnp.bfloat16)
    result = lax.map(one_block, (content_blocks, rotary_blocks, jnp.arange(blocks, dtype=jnp.int32)))
    return result.reshape(seq_rows, lat_heads * VDIM)

def project(left, right):
    return jnp.dot(left, right, preferred_element_type=jnp.float32)

def reference(features, norm_gain, w_query, w_key, w_value, head_sinks, w_query_latent, w_kv_latent, w_rope_key, query_latent_gain, kv_latent_gain, w_query_content, w_query_rotary, w_key_up, w_value_up, w_branch_window, w_branch_latent, w_gate_window, w_gate_latent):
    seq_rows = features.shape[0]
    positions = jnp.arange(seq_rows, dtype=jnp.int32)
    normed = rms_rows(features.astype(jnp.float32), norm_gain).astype(jnp.bfloat16)
    query_rows = project(normed, w_query).astype(jnp.bfloat16)
    key_rows = project(normed, w_key).astype(jnp.bfloat16)
    value_rows = project(normed, w_value).astype(jnp.bfloat16)
    padding = jnp.zeros((WINDOW, key_rows.shape[1]), jnp.bfloat16)
    window_out = window_attention(query_rows, jnp.concatenate([padding, key_rows], axis=0), jnp.concatenate([padding, value_rows], axis=0), head_sinks, 0)
    latent_query = rms_rows(project(normed, w_query_latent), query_latent_gain).astype(jnp.bfloat16)
    latent_kv = rms_rows(project(normed, w_kv_latent), kv_latent_gain).astype(jnp.bfloat16)
    rope_key = rotate(project(normed, w_rope_key), positions).astype(jnp.bfloat16)
    query_content = project(latent_query, w_query_content).astype(jnp.bfloat16).reshape(seq_rows, LAT_HEADS, NOPE)
    query_rotary = rotate(project(latent_query, w_query_rotary).reshape(seq_rows, LAT_HEADS, ROPE), positions).astype(jnp.bfloat16)
    head_keys = project(latent_kv, w_key_up).astype(jnp.bfloat16).reshape(seq_rows, LAT_HEADS, NOPE)
    head_values = project(latent_kv, w_value_up).astype(jnp.bfloat16).reshape(seq_rows, LAT_HEADS, VDIM)
    latent_out = latent_attention(query_content, query_rotary, head_keys, head_values, rope_key)
    window_branch = project(window_out, w_branch_window)
    latent_branch = project(latent_out, w_branch_latent)
    window_gate = jax.nn.sigmoid(project(normed, w_gate_window))
    latent_gate = jax.nn.sigmoid(project(normed, w_gate_latent))
    return (window_gate * window_branch + latent_gate * latent_branch).astype(jnp.bfloat16)
```

```python
import functools
import types

import jax
import jax.numpy as jnp
import numpy as np
from jax import lax
from jax.experimental import pallas as pl
from jax.experimental.pallas import tpu as pltpu
from jax.sharding import PartitionSpec as P

HEAD = 64
WINDOW = 128
NOPE = 128
ROPE = 64
VDIM = 128


EPS = 1e-06
THETA = 10000.0
NEGATIVE = -1e30
LANES = 128
LOG2_E = 1.4426950408889634
MESH = pl.DeviceIdType.MESH
BF16 = jnp.bfloat16
F32 = jnp.float32
PIECES = 4


def dot(left, right):
    return jnp.dot(left, right, preferred_element_type=F32)


def dot_t(left, right):
    return lax.dot_general(left, right, (((1,), (1,)), ((), ())), preferred_element_type=F32)


def dot_tl(left, right):
    return lax.dot_general(left, right, (((0,), (0,)), ((), ())), preferred_element_type=F32)


def rms_rows(rows, gain):
    return rows * lax.rsqrt(jnp.mean(rows * rows, axis=-1, keepdims=True) + EPS) * gain


def swap_halves(rows):
    half = rows.shape[1] // 2
    return jnp.concatenate([rows[:, half:], rows[:, :half]], axis=1)


SMALL = ("norm_gain", "sinks", "q_gain", "kv_gain", "frequency")
WEIGHTS = (
    "kv_latent", "rope", "key", "value", "query", "query_latent", "content", "rotary",
    "key_up", "value_up", "gate_window", "gate_latent",
)
def bundle(names, values):
    return types.SimpleNamespace(**dict(zip(names, values)))


MERGED = ("key", "value", "query")


def kernel(dims, names, *refs):
    n_sp, n_tp, n_x = dims
    n_z, n_y = n_sp // n_x, n_tp // 2
    features = refs[0]
    small_hbm = bundle(SMALL, refs[1:6])
    w_hbm = bundle(WEIGHTS, refs[6:18])
    window_hbm, latent_hbm = refs[18:20]
    out = refs[20]
    s = bundle(names, refs[21:])
    small = bundle(SMALL, [getattr(s, "small_" + name) for name in SMALL])
    merged = "w_qkv" in names
    kept = [name for name in WEIGHTS if "w_" + name in names]
    w = bundle(kept, [getattr(s, "w_" + name) for name in kept])
    ownf, feat, normed = s.ownf, s.feat, s.normed
    kvb, local_kv, halo, queries, q_full, latq = s.kvb, s.local_kv, s.halo, s.queries, s.q_full, s.latq
    gates, winb, lat, top, total, acc = s.gates, s.winb, s.lat, s.top, s.total, s.acc
    wcol, columns, psend, precv = s.wcol, s.columns, s.psend, s.precv
    cosine, sine = s.cosine, s.sine

    sp, tp = lax.axis_index("sp"), lax.axis_index("tp")
    z, x = sp // n_x, lax.rem(sp, n_x)
    y, core = tp // 2, lax.rem(tp, 2)
    other = 1 - core
    sibling = y * 2 + other
    rows, block = features.shape
    half = rows // 2
    pieces = normed.shape[1]
    piece = half // pieces
    lat_heads = w_hbm.key_up.shape[1] // NOPE
    kv_width = w_hbm.key.shape[1]
    kv_heads = kv_width // HEAD
    group = w_hbm.query.shape[1] // kv_width
    latent = w_hbm.kv_latent.shape[1]
    out_parts = lat.shape[1]
    out_rows = rows // out_parts

    def remote(src, dst, send, recv, where):
        return pltpu.make_async_remote_copy(
            src_ref=src, dst_ref=dst, send_sem=send, recv_sem=recv,
            device_id=where, device_id_type=MESH,
        )

    to_sibling = {"sp": sp, "tp": sibling}

    def arrival(ref, recv):
        return remote(ref, ref, recv, recv, to_sibling)

    def start(copies):
        for copy in copies:
            copy.start()

    def own_rows(c, h):
        return ownf.at[pl.ds(pl.multiple_of(c * half + h * piece, 16), piece)]

    def feat_rows(j, h):
        return feat.at[j, pl.ds(h * piece, piece)]

    own_load = [
        pltpu.make_async_copy(features, ownf, s.own_sem.at[0]),
        pltpu.make_async_copy(
            features.at[pl.ds(pl.multiple_of(core * half, 16), half)], feat.at[tp], s.own_sem.at[1]),
    ]
    start(own_load)
    loads = bundle(SMALL, [
        pltpu.make_async_copy(getattr(small_hbm, name), getattr(small, name), s.small_sem.at[i])
        for i, name in enumerate(SMALL)
    ])
    for name in SMALL:
        getattr(loads, name).start()

    barrier = pltpu.get_barrier_semaphore()

    def greet(where):
        pl.semaphore_signal(barrier, inc=1, device_id=where, device_id_type=MESH)

    for d in range(1, n_tp):
        greet({"sp": sp, "tp": lax.rem(tp + d, n_tp)})
    for d in range(1, n_x):
        greet({"sp": z * n_x + lax.rem(x + d, n_x), "tp": tp})

    @pl.when(z + 1 < n_z)
    def _():
        greet({"sp": sp + n_x, "tp": tp})

    @pl.when(z > 0)
    def _():
        greet({"sp": sp - n_x, "tp": tp})

    @pl.when(sp + 1 < n_sp)
    def _():
        greet({"sp": sp + 1, "tp": tp})

    @pl.when(sp > 0)
    def _():
        greet({"sp": sp - 1, "tp": tp})

    one, none = jnp.int32(1), jnp.int32(0)
    pl.semaphore_wait(
        barrier,
        n_tp - 1 + n_x - 1
        + jnp.where(z + 1 < n_z, one, none) + jnp.where(z > 0, one, none)
        + jnp.where(sp + 1 < n_sp, one, none) + jnp.where(sp > 0, one, none),
    )

    def feature_sends(h):
        sends = []
        for d in range(1, n_y):
            for c in range(2):
                sends.append(remote(
                    own_rows(c, h), feat_rows(tp, h), s.f_send.at[d], s.f_recv.at[h],
                    {"sp": sp, "tp": lax.rem(y + d, n_y) * 2 + c}))
        sends.append(remote(
            own_rows(other, h), feat_rows(tp, h), s.f_send.at[0], s.f_recv.at[h], to_sibling))
        return sends

    def feature_wait(h):
        arrival(feat.at[pl.ds(0, n_tp - 1), pl.ds(h * piece, piece)], s.f_recv.at[h]).wait_recv()

    for copy in own_load:
        copy.wait()
    for h in range(pieces):
        start(feature_sends(h))

    first = 0
    for i, name in enumerate(WEIGHTS):
        source = getattr(w_hbm, name)
        if name in kept:
            to = getattr(w, name)
        else:
            to = s.w_qkv.at[:, pl.ds(first, source.shape[1])]
            first += source.shape[1]
        copy = pltpu.make_async_copy(source, to, s.w_sem.at[i])
        copy.start()
        setattr(loads, name, copy)

    def window_columns():
        local, sends = [], []
        for j in range(n_y):
            local.append(pltpu.make_async_copy(
                window_hbm.at[:, pl.ds(pl.multiple_of((j * 2 + core) * block, LANES), block)],
                wcol.at[core, j], s.w_sems.at[0]))
            sends.append(remote(
                window_hbm.at[:, pl.ds(pl.multiple_of((j * 2 + other) * block, LANES), block)],
                wcol.at[core, j], s.w_sems.at[1], s.w_sems.at[2], to_sibling))
        return local, sends

    paired = n_z % 2 == 0
    parity = lax.rem(z, 2)
    partner = {"sp": sp + n_x * (1 - 2 * parity), "tp": tp}

    def column_send(to, d):
        return remote(
            latent_hbm.at[:, pl.ds(pl.multiple_of(to * block, LANES), block)],
            columns.at[tp], s.col_send.at[d], s.col_recv.at[d], {"sp": sp, "tp": to})

    def when_across(act):
        if paired:
            pl.when(core == parity)(act)
        else:
            act()

    def column_start():
        column_send(sibling, 0).start()

        @when_across
        def _():
            for d in range(1, n_y):
                for c in range(2):
                    column_send(lax.rem(y + d, n_y) * 2 + c, d).start()

    def pair_copy(d):
        ref = columns.at[lax.rem(y + n_y - d, n_y) * 2 + parity]
        return remote(ref, ref, s.pair_send.at[d - 1], s.pair_recv.at[d - 1], partner)

    def pair_forward():
        if paired:
            for d in range(1, n_y):
                source = lax.rem(y + n_y - d, n_y) * 2 + parity
                arrival(columns.at[source], s.col_recv.at[d]).wait_recv()
                pair_copy(d).start()

    column_local = pltpu.make_async_copy(
        latent_hbm.at[:, pl.ds(pl.multiple_of(tp * block, LANES), block)],
        columns.at[tp], s.col_own.at[0])

    wcol_local, wcol_sends = window_columns()

    loads.frequency.wait()
    positions = (sp * rows + lax.broadcasted_iota(jnp.int32, (rows, ROPE), 0)).astype(F32)
    angles = positions * small.frequency[...]
    lane = lax.broadcasted_iota(jnp.int32, (rows, ROPE), 1)
    cosine[...] = jnp.cos(angles).reshape(cosine.shape)
    turned = jnp.sin(angles)
    sine[...] = jnp.where(lane < ROPE // 2, -turned, turned).reshape(sine.shape)

    def normalize(h):
        squares = jnp.zeros((piece, 1), F32)
        part = slice(h * piece, (h + 1) * piece)
        for j in range(n_tp):
            values = feat[j, part].astype(F32)
            squares = squares + jnp.sum(values * values, axis=-1, keepdims=True)
        scale = lax.rsqrt(squares / (n_tp * block) + EPS)
        for j in range(n_tp):
            span = slice(j * block, (j + 1) * block)
            values = feat[j, part].astype(F32) * scale * small.norm_gain[:, span]
            normed[core, h, :, span] = values.astype(BF16)

    def normed_copy(h):
        return remote(normed.at[core, h], normed.at[core, h], s.n_sems.at[0], s.n_sems.at[1], to_sibling)

    def latents(h):
        own = normed[core, h]
        rope = dot_t(own, w.rope[...])
        rope = rope * cosine[core, h] + swap_halves(rope) * sine[core, h]
        rope = jnp.concatenate([rope, jnp.zeros((piece, LANES - ROPE), F32)], axis=1).astype(BF16)
        kvb[sp, core, h, :, :latent] = rms_rows(dot(own, w.kv_latent[...]), small.kv_gain[...]).astype(BF16)
        kvb[sp, core, h, :, latent:] = rope

    def column_slot(k):
        return (z - k) * n_x + x

    def row_slot(k, d):
        return (z - k) * n_x + lax.rem(x + n_x - d, n_x)

    def z_copy(k, h):
        ref = kvb.at[column_slot(k), core, h]
        return remote(ref, ref, s.z_send.at[k], s.z_recv.at[h, k], {"sp": sp + n_x, "tp": tp})

    def x_copy(k, d, h):
        ref = kvb.at[column_slot(k), core, h]
        return remote(ref, ref, s.x_send.at[k, d - 1], s.x_recv.at[h, k, d - 1],
                      {"sp": z * n_x + lax.rem(x + d, n_x), "tp": tp})

    def c_copy(k, h):
        ref = kvb.at[column_slot(k), core, h]
        return remote(ref, ref, s.c_send.at[k], s.c_recv.at[k], to_sibling)

    def d_copy(k, d, h):
        ref = kvb.at[row_slot(k, d), core, h]
        return remote(ref, ref, s.d_send.at[k, d - 1], s.d_recv.at[k, d - 1], to_sibling)

    def wait_column(k):
        arrival(kvb.at[column_slot(k), other], s.c_recv.at[k]).wait_recv()

    def wait_row(k, d):
        arrival(kvb.at[row_slot(k, d), other], s.d_recv.at[k, d - 1]).wait_recv()

    def sends_row(k, d):
        return (k > 0) | (x + d < n_x)

    def takes_row(k, d):
        return (k > 0) | (x >= d)

    def pass_on(k, h):
        @pl.when(z + 1 < n_z)
        def _():
            z_copy(k, h).start()

        for d in range(1, n_x):
            @pl.when(sends_row(k, d))
            def _():
                x_copy(k, d, h).start()

        c_copy(k, h).start()

    def take_column(k, h):
        arrival(kvb.at[column_slot(k), core, h], s.z_recv.at[h, k - 1]).wait_recv()
        pass_on(k, h)

    def take_row(k, h):
        for d in range(1, n_x):
            @pl.when(takes_row(k, d))
            def _():
                arrival(kvb.at[row_slot(k, d), core, h], s.x_recv.at[h, k, d - 1]).wait_recv()
                d_copy(k, d, h).start()

    early = min(2, pieces)

    def take_first(h):
        @pl.when(z >= 1)
        def _():
            take_column(1, h)

    start(wcol_local)
    start(wcol_sends)
    column_local.start()
    for name in ("norm_gain", "kv_gain", "kv_latent", "rope"):
        getattr(loads, name).wait()
    for h in range(pieces):
        feature_wait(h)
        if h == pieces - 1:
            column_start()
        normalize(h)
        normed_copy(h).start()
        latents(h)
        pass_on(0, h)
        if h >= early:
            take_first(h - early)

    loads.query_latent.wait()
    loads.q_gain.wait()
    own_normed = normed[core].reshape(half, n_tp * block)
    latq[core] = rms_rows(dot(own_normed, w.query_latent[...]), small.q_gain[...]).astype(BF16)
    latq_copy = remote(latq.at[core], latq.at[core], s.q_sems.at[0], s.q_sems.at[1], to_sibling)
    latq_copy.start()

    for h in range(pieces - early, pieces - 1):
        take_first(h)

    arrival(normed.at[other], s.n_sems.at[1]).wait_recv()

    def all_normed():
        return normed[...].reshape(rows, n_tp * block)

    for name in MERGED:
        getattr(loads, name).wait()
    if merged:
        qkv = dot(all_normed(), s.w_qkv[...]).astype(BF16)
    else:
        qkv = jnp.concatenate([dot(all_normed(), getattr(w, name)[...]) for name in MERGED], axis=1).astype(BF16)
    local_kv[...] = qkv[:, : 2 * kv_width]
    queries[...] = qkv[:, 2 * kv_width :]
    tail = local_kv.at[pl.ds(rows - WINDOW, WINDOW)]
    halo_copy = remote(tail, halo, s.halo_sem.at[0], s.halo_sem.at[1], {"sp": sp + 1, "tp": tp})

    @pl.when(sp + 1 < n_sp)
    def _():
        halo_copy.start()

    take_first(pieces - 1)

    def queries_up():
        arrival(latq.at[other], s.q_sems.at[1]).wait_recv()
        loads.content.wait()
        loads.rotary.wait()
        latent_query = latq[...].reshape(rows, latent)
        content = dot(latent_query, w.content[...])
        rotary = dot(latent_query, w.rotary[...])
        cos_all, sin_all = cosine[...].reshape(rows, ROPE), sine[...].reshape(rows, ROPE)
        padding = jnp.zeros((rows, LANES - ROPE), F32)
        for h in range(lat_heads):
            turned = rotary[:, h * ROPE : (h + 1) * ROPE]
            turned = turned * cos_all + swap_halves(turned) * sin_all
            q_full[h, :NOPE, :] = content[:, h * NOPE : (h + 1) * NOPE].T.astype(BF16)
            q_full[h, NOPE:, :] = jnp.concatenate([turned, padding], axis=1).T.astype(BF16)
        loads.key_up.wait()
        loads.value_up.wait()

    def attend(slot, diagonal):
        both = kvb[slot].reshape(rows, latent + LANES)
        source, rope_part = both[:, :latent], both[:, latent:]
        keys = dot(source, w.key_up[...]).astype(BF16)
        values = dot(source, w.value_up[...]).astype(BF16)
        heads = range(lat_heads)
        scores = []
        for h in heads:
            key = jnp.concatenate([keys[:, h * NOPE : (h + 1) * NOPE], rope_part], axis=1)
            scores.append(dot(key, q_full[h]) * ((NOPE + ROPE) ** (-0.5) * LOG2_E))
        if diagonal:
            live = (lax.broadcasted_iota(jnp.int32, (rows, rows), 0)
                    <= lax.broadcasted_iota(jnp.int32, (rows, rows), 1))
            scores = [jnp.where(live, part, NEGATIVE) for part in scores]
        weights, fades = [], []
        for h in heads:
            peak = jnp.max(scores[h], axis=0, keepdims=True)
            if not diagonal:
                before = top[h]
                peak = jnp.maximum(peak, before)
                fades.append(jnp.exp2(before - peak))
            top[h] = peak
            weights.append(jnp.exp2(scores[h] - peak))
        for h in heads:
            weight_sum = jnp.sum(weights[h], axis=0, keepdims=True)
            part = dot_tl(values[:, h * VDIM : (h + 1) * VDIM], weights[h].astype(BF16))
            if not diagonal:
                weight_sum = total[h] * fades[h] + weight_sum
                part = acc[h] * fades[h] + part
            total[h] = weight_sum
            acc[h] = part

    def window():
        loads.sinks.wait()

        @pl.when(sp > 0)
        def _():
            arrival(halo, s.halo_sem.at[1]).wait_recv()

        @pl.when(sp == 0)
        def _():
            halo[...] = jnp.zeros(halo.shape, BF16)

        row = lax.broadcasted_iota(jnp.int32, (2 * WINDOW, WINDOW), 1)
        column = lax.broadcasted_iota(jnp.int32, (2 * WINDOW, WINDOW), 0)
        offset = row + WINDOW - column
        in_band = (offset >= 0) & (offset < WINDOW)
        in_band = jnp.concatenate([in_band] * group, axis=1)
        later = jnp.concatenate([(sp > 0) | (column >= WINDOW)] * group, axis=1)
        units = [(n, g) for n in range(rows // WINDOW) for g in range(kv_heads)]
        scores, values, sinks, weights = [], [], [], []
        for n, g in units:
            at = slice(n * WINDOW, (n + 1) * WINDOW)
            earlier = halo[...] if n == 0 else local_kv[(n - 1) * WINDOW : n * WINDOW]
            band = jnp.concatenate([earlier, local_kv[at]], axis=0)
            valid = in_band & later if n == 0 else in_band
            key = band[:, g * HEAD : (g + 1) * HEAD]
            values.append(band[:, kv_width + g * HEAD : kv_width + (g + 1) * HEAD])
            members = range(g * group, (g + 1) * group)
            query = jnp.concatenate([queries[at, q * HEAD : (q + 1) * HEAD] for q in members], axis=0)
            sinks.append(jnp.concatenate([jnp.full((1, WINDOW), small.sinks[0, q], F32) for q in members], axis=1))
            scores.append(jnp.where(valid, dot_t(key, query) * HEAD ** (-0.5), NEGATIVE))
        for u in range(len(units)):
            peak = jnp.maximum(jnp.max(scores[u], axis=0, keepdims=True), sinks[u])
            part = jnp.exp(scores[u] - peak)
            bottom = jnp.sum(part, axis=0, keepdims=True) + jnp.exp(sinks[u] - peak)
            weights.append((part * (1.0 / bottom)).astype(BF16))
        mixed = [dot_tl(values[u], weights[u]) for u in range(len(units))]
        for n in range(rows // WINDOW):
            heads = [
                mixed[n * kv_heads + g][:, i * WINDOW : (i + 1) * WINDOW]
                for g in range(kv_heads) for i in range(group)
            ]
            winb[core, n * WINDOW : (n + 1) * WINDOW, :] = jnp.concatenate(heads, axis=0).T.astype(BF16)

    win_copy = remote(winb.at[core], winb.at[core], s.win_sem.at[0], s.win_sem.at[1], to_sibling)

    def window_part(j):
        return dot(winb[0], wcol[0, j]) + dot(winb[1], wcol[1, j])

    def part_copy(d):
        return remote(psend.at[d - 1], precv.at[d - 1], s.p_send.at[d - 1], s.p_recv.at[d - 1],
                      {"sp": sp, "tp": lax.rem(y + d, n_y) * 2 + core})

    def window_parts():
        pltpu.make_async_copy(wcol.at[core], wcol.at[core], s.w_sems.at[0]).wait()
        arrival(wcol.at[other], s.w_sems.at[2]).wait_recv()
        arrival(winb.at[other], s.win_sem.at[1]).wait_recv()
        for d in range(1, n_y):
            psend[d - 1] = window_part(lax.rem(y + d, n_y)).astype(BF16)
            part_copy(d).start()

    def gate(b):
        name = WEIGHTS[10 + b]
        getattr(loads, name).wait()

        def step(i, _):
            at = pl.ds(pl.multiple_of(i * 256, LANES), 256)
            gates[b, :, at] = jax.nn.sigmoid(dot(all_normed(), getattr(w, name)[:, at]))
            return 0

        lax.fori_loop(0, block // 256, step, 0)

    def take_second(lo, hi):
        for h in range(lo, hi):
            @pl.when(z >= 2)
            def _():
                take_column(2, h)

    def take_rows(k):
        for h in range(pieces):
            take_row(k, h)

    def attend_row(k, d):
        wait_row(k, d)
        attend(row_slot(k, d), False)

    if n_z > 2:
        take_second(0, pieces // 2)
    queries_up()
    if n_z > 2:
        take_second(pieces // 2, pieces - pieces // 4)
    take_rows(0)
    wait_column(0)
    attend(sp, True)
    if n_z > 2:
        take_second(pieces - pieces // 4, pieces)
    pair_forward()

    def step(k, _):
        @pl.when(k == 3)
        def _():
            window()
            win_copy.start()

        @pl.when(z >= k - 1)
        def _():
            wait_column(k - 1)
            attend(column_slot(k - 1), False)

        @pl.when(k == 3)
        def _():
            window_parts()

        @pl.when((k > 2) & (z >= k))
        def _():
            for h in range(pieces):
                take_column(k, h)

        @pl.when(z >= k - 1)
        def _():
            take_rows(k - 1)

        for d in range(1, n_x):
            @pl.when((z >= k - 2) & takes_row(k - 2, d))
            def _():
                attend_row(k - 2, d)

        return 0

    lax.fori_loop(2, max(n_z, 2) + 2, step, 0)

    def gather(part):
        own = lat.at[tp, part]
        sends = [
            remote(own, own, s.y_send.at[d - 1], s.y_recv.at[part, d - 1],
                   {"sp": sp, "tp": lax.rem(y + d, n_y) * 2 + core})
            for d in range(1, n_y)
        ]
        sends.append(remote(own, own, s.s_send.at[0], s.s_recv.at[part], to_sibling))
        return sends

    def forward(part):
        for d in range(1, n_y):
            ref = lat.at[lax.rem(y + n_y - d, n_y) * 2 + core, part]
            arrival(ref, s.y_recv.at[part, d - 1]).wait_recv()
            remote(ref, ref, s.s_send.at[d], s.s_recv.at[part], to_sibling).start()

    def arrived(part):
        arrival(lat.at[pl.ds(0, n_y), part], s.s_recv.at[part]).wait_recv()

    for part in range(out_parts):
        at = slice(part * out_rows, (part + 1) * out_rows)
        for h in range(lat_heads):
            lat[tp, part, :, h * VDIM : (h + 1) * VDIM] = (
                acc[h, :, at] / total[h, :, at]).T.astype(BF16)
        start(gather(part))
    gate(0)
    gate(1)
    window_branch = window_part(y)
    for d in range(1, n_y):
        arrival(precv.at[d - 1], s.p_recv.at[d - 1]).wait_recv()
        window_branch = window_branch + precv[d - 1].astype(F32)
    gates[0] = gates[0] * window_branch
    column_local.wait()
    arrival(columns.at[sibling], s.col_recv.at[0]).wait_recv()
    for d in range(1, n_y):
        base = lax.rem(y + n_y - d, n_y) * 2
        if paired:
            arrival(columns.at[base + 1 - parity], s.pair_recv.at[d - 1]).wait_recv()
        else:
            arrival(columns.at[pl.ds(base, 2)], s.col_recv.at[d]).wait_recv()
    for part in range(out_parts):
        at = slice(part * out_rows, (part + 1) * out_rows)
        forward(part)
        arrived(part)
        latent_branch = jnp.zeros((out_rows, block), F32)
        for j in range(n_tp):
            latent_branch = latent_branch + dot(lat[j, part], columns[j])
        out[at, :] = (gates[0, at] + gates[1, at] * latent_branch).astype(BF16)

    def leave(ref, send):
        remote(ref, ref, send, send, to_sibling).wait_send()

    leave(ownf.at[pl.ds(0, half)], s.f_send.at[0])
    for d in range(1, n_y):
        leave(ownf, s.f_send.at[d])
    leave(normed.at[core], s.n_sems.at[0])
    latq_copy.wait_send()
    leave(wcol.at[core], s.w_sems.at[1])
    leave(columns.at[tp], s.col_send.at[0])

    @when_across
    def _():
        for d in range(1, n_y):
            leave(columns.at[pl.ds(0, 2)], s.col_send.at[d])

    if paired:
        for d in range(1, n_y):
            pair_copy(d).wait_send()
    win_copy.wait_send()
    for d in range(1, n_y):
        part_copy(d).wait_send()
        leave(lat.at[tp], s.y_send.at[d - 1])
        leave(lat.at[tp], s.s_send.at[d])
    leave(lat.at[tp], s.s_send.at[0])

    @pl.when(sp + 1 < n_sp)
    def _():
        halo_copy.wait_send()

    def drain(k, _):
        @pl.when(z >= k)
        def _():
            own = kvb.at[column_slot(k), core]

            @pl.when(z + 1 < n_z)
            def _():
                leave(own, s.z_send.at[k])

            leave(own, s.c_send.at[k])
            for d in range(1, n_x):
                @pl.when(sends_row(k, d))
                def _():
                    leave(own, s.x_send.at[k, d - 1])

                @pl.when(takes_row(k, d))
                def _():
                    leave(own, s.d_send.at[k, d - 1])

        return 0

    lax.fori_loop(0, n_z, drain, 0)


def on_device(dims, features, norm_gain, w_query, w_key, w_value, head_sinks, w_query_latent,
              w_kv_latent, w_rope_key, query_latent_gain, kv_latent_gain, w_query_content,
              w_query_rotary, w_key_up, w_value_up, w_branch_window, w_branch_latent,
              w_gate_window, w_gate_latent):
    n_sp, n_tp, n_x = dims
    n_z, n_y = n_sp // n_x, n_tp // 2
    rows, block = features.shape
    width = norm_gain.shape[0]
    latent = w_kv_latent.shape[1]
    lat_heads = w_key_up.shape[1] // NOPE
    half_width = ROPE // 2
    entry = np.arange(ROPE, dtype=np.int32) % half_width
    frequency = (np.float32(THETA) ** (-entry.astype(np.float32) / np.float32(half_width))).astype(np.float32)[None, :]
    weights = (w_kv_latent, w_rope_key.T, w_key, w_value, w_query, w_query_latent, w_query_content,
               w_query_rotary, w_key_up, w_value_up, w_gate_window, w_gate_latent)
    smalls = (norm_gain[None, :], head_sinks[None, :], query_latent_gain[None, :], kv_latent_gain[None, :],
              jnp.asarray(frequency))
    branch_rows = w_branch_window.shape[0]
    pieces = PIECES if (rows // 2) % (16 * PIECES) == 0 else 1
    piece = rows // 2 // pieces
    out_parts = rows // LANES
    merge = w_key.shape[1] % LANES == 0
    hbm = pl.BlockSpec(memory_space=pl.ANY)
    dma = pltpu.SemaphoreType.DMA
    vm = pltpu.VMEM
    scratch = dict(
        **{"small_" + n: (pltpu.SMEM if n == "sinks" else vm)(a.shape, F32) for n, a in zip(SMALL, smalls)},
        **{"w_" + n: vm(a.shape, BF16) for n, a in zip(WEIGHTS, weights) if not (merge and n in MERGED)},
        **(dict(w_qkv=vm((width, 2 * w_key.shape[1] + w_query.shape[1]), BF16)) if merge else {}),
        ownf=vm((rows, block), BF16),
        feat=vm((n_tp, rows // 2, block), BF16),
        normed=vm((2, pieces, piece, width), BF16),
        latq=vm((2, rows // 2, latent), BF16),
        wcol=vm((2, n_y, branch_rows, block), BF16),
        columns=vm((n_tp, w_branch_latent.shape[0], block), BF16),
        psend=vm((n_y - 1, rows, block), BF16),
        precv=vm((n_y - 1, rows, block), BF16),
        kvb=vm((n_sp, 2, pieces, piece, latent + LANES), BF16),
        local_kv=vm((rows, 2 * w_key.shape[1]), BF16),
        halo=vm((WINDOW, 2 * w_key.shape[1]), BF16),
        queries=vm((rows, w_query.shape[1]), BF16),
        q_full=vm((lat_heads, NOPE + LANES, rows), BF16),
        gates=vm((2, rows, block), F32),
        winb=vm((2, rows, w_query.shape[1]), BF16),
        lat=vm((n_tp, out_parts, rows // out_parts, lat_heads * VDIM), BF16),
        top=vm((lat_heads, 1, rows), F32),
        total=vm((lat_heads, 1, rows), F32),
        acc=vm((lat_heads, VDIM, rows), F32),
        cosine=vm((2, pieces, piece, ROPE), F32),
        sine=vm((2, pieces, piece, ROPE), F32),
        own_sem=dma((2,)),
        small_sem=dma((len(SMALL),)),
        w_sem=dma((len(weights),)),
        f_send=dma((n_y,)),
        f_recv=dma((pieces,)),
        n_sems=dma((2,)),
        q_sems=dma((2,)),
        w_sems=dma((3,)),
        col_own=dma((1,)),
        col_send=dma((n_y,)),
        col_recv=dma((n_y,)),
        pair_send=dma((n_y - 1,)),
        pair_recv=dma((n_y - 1,)),
        halo_sem=dma((2,)),
        win_sem=dma((2,)),
        p_send=dma((n_y - 1,)),
        p_recv=dma((n_y - 1,)),
        y_send=dma((n_y - 1,)),
        y_recv=dma((out_parts, n_y - 1)),
        s_send=dma((n_y,)),
        s_recv=dma((out_parts,)),
        z_send=dma((n_z - 1,)),
        z_recv=dma((pieces, n_z - 1)),
        x_send=dma((n_z, n_x - 1)),
        x_recv=dma((pieces, n_z, n_x - 1)),
        c_send=dma((n_z,)),
        c_recv=dma((n_z,)),
        d_send=dma((n_z, n_x - 1)),
        d_recv=dma((n_z, n_x - 1)),
    )
    return pl.pallas_call(
        functools.partial(kernel, dims, tuple(scratch)),
        out_shape=pltpu.VMEM((rows, block), BF16),
        in_specs=[hbm] * (1 + len(smalls) + len(weights) + 2),
        out_specs=pl.BlockSpec(memory_space=pltpu.VMEM),
        scratch_shapes=list(scratch.values()),
        compiler_params=pltpu.CompilerParams(
            collective_id=0, has_side_effects=True, vmem_limit_bytes=60 * 1024 * 1024
        ),
    )(features, *smalls, *weights, w_branch_window, w_branch_latent)


def solution(mesh):
    n_sp, n_tp = mesh.shape["sp"], mesh.shape["tp"]
    n_x = 1
    while n_sp % (2 * n_x) == 0 and 8 * n_x * n_x <= n_sp:
        n_x *= 2
    return jax.shard_map(
        functools.partial(on_device, (n_sp, n_tp, n_x)),
        mesh=mesh,
        in_specs=(
            P("sp", "tp"),
            P(),
            P(None, "tp"),
            P(None, "tp"),
            P(None, "tp"),
            P("tp"),
            P(),
            P(),
            P(),
            P(),
            P(),
            P(None, "tp"),
            P(None, "tp"),
            P(None, "tp"),
            P(None, "tp"),
            P("tp", None),
            P("tp", None),
            P(None, "tp"),
            P(None, "tp"),
        ),
        out_specs=P("sp", "tp"),
        check_vma=False,
    )
```

```python
import functools
import types

import jax
import jax.numpy as jnp
import numpy as np
from jax import lax
from jax.experimental import pallas as pl
from jax.experimental.pallas import tpu as pltpu
from jax.sharding import PartitionSpec as P

HEAD = 64
WINDOW = 128
NOPE = 128
ROPE = 64
VDIM = 128


EPS = 1e-06
THETA = 10000.0
NEGATIVE = -1e30
LANES = 128
LOG2_E = 1.4426950408889634
MESH = pl.DeviceIdType.MESH
BF16 = jnp.bfloat16
F32 = jnp.float32
PIECES = 4
SUBLANES = 8
DETOURS = (0, PIECES - 1)


def dot(left, right):
    return jnp.dot(left, right, preferred_element_type=F32)


def dot_t(left, right):
    return lax.dot_general(left, right, (((1,), (1,)), ((), ())), preferred_element_type=F32)


def dot_tl(left, right):
    return lax.dot_general(left, right, (((0,), (0,)), ((), ())), preferred_element_type=F32)


def rms_rows(rows, gain):
    return rows * lax.rsqrt(jnp.mean(rows * rows, axis=-1, keepdims=True) + EPS) * gain


def swap_halves(rows):
    half = rows.shape[1] // 2
    return jnp.concatenate([rows[:, half:], rows[:, :half]], axis=1)


SMALL = ("norm_gain", "sinks", "q_gain", "kv_gain", "frequency")
WEIGHTS = (
    "kv_latent", "rope", "key", "value", "query", "query_latent", "content", "rotary",
    "key_up", "value_up", "gate_window", "gate_latent",
)
def bundle(names, values):
    return types.SimpleNamespace(**dict(zip(names, values)))


MERGED = ("key", "value", "query")


def kernel(dims, names, *refs):
    n_sp, n_tp, n_x = dims
    n_z, n_y = n_sp // n_x, n_tp // 2
    features = refs[0]
    small_hbm = bundle(SMALL, refs[1:6])
    w_hbm = bundle(WEIGHTS, refs[6:18])
    window_hbm, latent_hbm = refs[18:20]
    out = refs[20]
    s = bundle(names, refs[21:])
    small = bundle(SMALL, [getattr(s, "small_" + name) for name in SMALL])
    merged = "w_qkv" in names
    kept = [name for name in WEIGHTS if "w_" + name in names]
    w = bundle(kept, [getattr(s, "w_" + name) for name in kept])
    ownf, feat, normed = s.ownf, s.feat, s.normed
    kvb, local_kv, halo, queries, q_full, latq = s.kvb, s.local_kv, s.halo, s.queries, s.q_full, s.latq
    gates, winb, lat, top, total, acc = s.gates, s.winb, s.lat, s.top, s.total, s.acc
    wcol, columns, psend, precv = s.wcol, s.columns, s.psend, s.precv
    cosine, sine = s.cosine, s.sine

    sp, tp = lax.axis_index("sp"), lax.axis_index("tp")
    z, x = sp // n_x, lax.rem(sp, n_x)
    y, core = tp // 2, lax.rem(tp, 2)
    other = 1 - core
    sibling = y * 2 + other
    rows, block = features.shape
    half = rows // 2
    pieces = normed.shape[1]
    piece = half // pieces
    lat_heads = w_hbm.key_up.shape[1] // NOPE
    kv_width = w_hbm.key.shape[1]
    kv_heads = kv_width // HEAD
    group = w_hbm.query.shape[1] // kv_width
    latent = w_hbm.kv_latent.shape[1]
    out_parts = lat.shape[1]
    out_rows = rows // out_parts

    def remote(src, dst, send, recv, where):
        return pltpu.make_async_remote_copy(
            src_ref=src, dst_ref=dst, send_sem=send, recv_sem=recv,
            device_id=where, device_id_type=MESH,
        )

    to_sibling = {"sp": sp, "tp": sibling}

    def arrival(ref, recv):
        return remote(ref, ref, recv, recv, to_sibling)

    def start(copies):
        for copy in copies:
            copy.start()

    def own_rows(c, h):
        return ownf.at[pl.ds(pl.multiple_of(c * half + h * piece, 16), piece)]

    def feat_rows(j, h):
        return feat.at[j, pl.ds(h * piece, piece)]

    own_load = [
        pltpu.make_async_copy(features, ownf, s.own_sem.at[0]),
        pltpu.make_async_copy(
            features.at[pl.ds(pl.multiple_of(core * half, 16), half)], feat.at[tp], s.own_sem.at[1]),
    ]
    start(own_load)
    loads = bundle(SMALL, [
        pltpu.make_async_copy(getattr(small_hbm, name), getattr(small, name), s.small_sem.at[i])
        for i, name in enumerate(SMALL)
    ])
    for name in SMALL:
        getattr(loads, name).start()

    barrier = pltpu.get_barrier_semaphore()

    def greet(where):
        pl.semaphore_signal(barrier, inc=1, device_id=where, device_id_type=MESH)

    for d in range(1, n_tp):
        greet({"sp": sp, "tp": lax.rem(tp + d, n_tp)})
    for d in range(1, n_x):
        greet({"sp": z * n_x + lax.rem(x + d, n_x), "tp": tp})

    @pl.when(z + 1 < n_z)
    def _():
        greet({"sp": sp + n_x, "tp": tp})

    @pl.when(z > 0)
    def _():
        greet({"sp": sp - n_x, "tp": tp})

    @pl.when(sp + 1 < n_sp)
    def _():
        greet({"sp": sp + 1, "tp": tp})

    @pl.when(sp > 0)
    def _():
        greet({"sp": sp - 1, "tp": tp})

    one, none = jnp.int32(1), jnp.int32(0)
    pl.semaphore_wait(
        barrier,
        n_tp - 1 + n_x - 1
        + jnp.where(z + 1 < n_z, one, none) + jnp.where(z > 0, one, none)
        + jnp.where(sp + 1 < n_sp, one, none) + jnp.where(sp > 0, one, none),
    )

    def feature_sends(h):
        sends = []
        for d in range(1, n_y):
            for c in range(2):
                sends.append(remote(
                    own_rows(c, h), feat_rows(tp, h), s.f_send.at[d], s.f_recv.at[h],
                    {"sp": sp, "tp": lax.rem(y + d, n_y) * 2 + c}))
        sends.append(remote(
            own_rows(other, h), feat_rows(tp, h), s.f_send.at[0], s.f_recv.at[h], to_sibling))
        return sends

    def feature_wait(h):
        arrival(feat.at[pl.ds(0, n_tp - 1), pl.ds(h * piece, piece)], s.f_recv.at[h]).wait_recv()

    for copy in own_load:
        copy.wait()
    for h in range(pieces):
        start(feature_sends(h))

    first = 0
    for i, name in enumerate(WEIGHTS):
        source = getattr(w_hbm, name)
        if name in kept:
            to = getattr(w, name)
        else:
            to = s.w_qkv.at[:, pl.ds(first, source.shape[1])]
            first += source.shape[1]
        copy = pltpu.make_async_copy(source, to, s.w_sem.at[i])
        copy.start()
        setattr(loads, name, copy)

    def window_columns():
        local, sends = [], []
        for j in range(n_y):
            local.append(pltpu.make_async_copy(
                window_hbm.at[:, pl.ds(pl.multiple_of((j * 2 + core) * block, LANES), block)],
                wcol.at[core, j], s.w_sems.at[0]))
            sends.append(remote(
                window_hbm.at[:, pl.ds(pl.multiple_of((j * 2 + other) * block, LANES), block)],
                wcol.at[core, j], s.w_sems.at[1], s.w_sems.at[2], to_sibling))
        return local, sends

    paired = n_z % 2 == 0
    parity = lax.rem(z, 2)
    partner = {"sp": sp + n_x * (1 - 2 * parity), "tp": tp}

    def column_send(to, d):
        return remote(
            latent_hbm.at[:, pl.ds(pl.multiple_of(to * block, LANES), block)],
            columns.at[tp], s.col_send.at[d], s.col_recv.at[d], {"sp": sp, "tp": to})

    def when_across(act):
        if paired:
            pl.when(core == parity)(act)
        else:
            act()

    def column_start():
        column_send(sibling, 0).start()

        @when_across
        def _():
            for d in range(1, n_y):
                for c in range(2):
                    column_send(lax.rem(y + d, n_y) * 2 + c, d).start()

    def pair_copy(d):
        ref = columns.at[lax.rem(y + n_y - d, n_y) * 2 + parity]
        return remote(ref, ref, s.pair_send.at[d - 1], s.pair_recv.at[d - 1], partner)

    def pair_forward():
        if paired:
            for d in range(1, n_y):
                source = lax.rem(y + n_y - d, n_y) * 2 + parity
                arrival(columns.at[source], s.col_recv.at[d]).wait_recv()
                pair_copy(d).start()

    column_local = pltpu.make_async_copy(
        latent_hbm.at[:, pl.ds(pl.multiple_of(tp * block, LANES), block)],
        columns.at[tp], s.col_own.at[0])

    wcol_local, wcol_sends = window_columns()

    loads.frequency.wait()
    positions = (sp * rows + lax.broadcasted_iota(jnp.int32, (rows, ROPE), 0)).astype(F32)
    angles = positions * small.frequency[...]
    lane = lax.broadcasted_iota(jnp.int32, (rows, ROPE), 1)
    cosine[...] = jnp.cos(angles).reshape(cosine.shape)
    turned = jnp.sin(angles)
    sine[...] = jnp.where(lane < ROPE // 2, -turned, turned).reshape(sine.shape)

    def normalize(h):
        squares = jnp.zeros((piece, 1), F32)
        part = slice(h * piece, (h + 1) * piece)
        for j in range(n_tp):
            values = feat[j, part].astype(F32)
            squares = squares + jnp.sum(values * values, axis=-1, keepdims=True)
        scale = lax.rsqrt(squares / (n_tp * block) + EPS)
        for j in range(n_tp):
            span = slice(j * block, (j + 1) * block)
            values = feat[j, part].astype(F32) * scale * small.norm_gain[:, span]
            normed[core, h, :, span] = values.astype(BF16)

    def normed_copy(h):
        return remote(normed.at[core, h], normed.at[core, h], s.n_sems.at[0], s.n_sems.at[1], to_sibling)

    def latents(h):
        own = normed[core, h]
        rope = dot_t(own, w.rope[...])
        rope = rope * cosine[core, h] + swap_halves(rope) * sine[core, h]
        rope = jnp.concatenate([rope[: piece // 2], rope[piece // 2 :]], axis=1)
        rope = [rope[i : i + SUBLANES] for i in range(0, piece // 2, SUBLANES)]
        rope.append(jnp.zeros((SUBLANES, latent - len(rope) * LANES), F32))
        kvb[sp, core, h, :piece, :] = rms_rows(dot(own, w.kv_latent[...]), small.kv_gain[...]).astype(BF16)
        kvb[sp, core, h, piece:, :] = jnp.concatenate(rope, axis=1).astype(BF16)

    def rope_rows(slot):
        parts = []
        for c in range(2):
            for h in range(pieces):
                packed = kvb[slot, c, h, piece:, :].astype(F32)
                pair = jnp.concatenate(
                    [packed[:, i * LANES : (i + 1) * LANES] for i in range(piece // 2 // SUBLANES)], axis=0)
                parts += [pair, pltpu.roll(pair, ROPE, 1)]
        return jnp.concatenate(parts, axis=0).astype(BF16)

    def column_slot(k):
        return (z - k) * n_x + x

    def row_slot(k, d):
        return (z - k) * n_x + lax.rem(x + n_x - d, n_x)

    def z_copy(k, h):
        ref = kvb.at[column_slot(k), core, h]
        return remote(ref, ref, s.z_send.at[k], s.z_recv.at[h, k], {"sp": sp + n_x, "tp": tp})

    def x_copy(k, d, h):
        ref = kvb.at[column_slot(k), core, h]
        return remote(ref, ref, s.x_send.at[k, d - 1], s.x_recv.at[h, k, d - 1],
                      {"sp": z * n_x + lax.rem(x + d, n_x), "tp": tp})

    def c_copy(k, h):
        ref = kvb.at[column_slot(k), core, h]
        return remote(ref, ref, s.c_send.at[k], s.c_recv.at[k], to_sibling)

    def d_copy(k, d, h):
        ref = kvb.at[row_slot(k, d), core, h]
        return remote(ref, ref, s.d_send.at[k, d - 1], s.d_recv.at[k, d - 1], to_sibling)

    def wait_column(k):
        arrival(kvb.at[column_slot(k), other], s.c_recv.at[k]).wait_recv()

    def wait_row(k, d):
        arrival(kvb.at[row_slot(k, d), other], s.d_recv.at[k, d - 1]).wait_recv()

    def sends_row(k, d):
        return (k > 0) | (x + d < n_x)

    def takes_row(k, d):
        return (k > 0) | (x >= d)

    def detoured(k, h, to):
        if h == DETOURS[0]:
            return k >= 2
        return (k >= 3) & (to == 0)

    def pass_on(k, h):
        @pl.when(z + 1 < n_z)
        def _():
            z_copy(k, h).start()

        for d in range(1, n_x):
            to = lax.rem(x + d, n_x)

            @pl.when(sends_row(k, d) & ~detoured(k, h, to) if h in DETOURS else sends_row(k, d))
            def _():
                x_copy(k, d, h).start()

        c_copy(k, h).start()

    def take_column(k, h):
        arrival(kvb.at[column_slot(k), core, h], s.z_recv.at[h, k - 1]).wait_recv()
        pass_on(k, h)

    def detour_copy(k, d, i):
        ref = kvb.at[row_slot(k, d), core, DETOURS[i]]
        return remote(ref, ref, s.r_send.at[i, k, d - 1], s.r_recv.at[i, k + 1, d - 1], {"sp": sp + n_x, "tp": tp})

    def passes_detour(k, i):
        return (z + 1 < n_z) & detoured(k + 1, DETOURS[i], x)

    def take_row(k, h):
        for d in range(1, n_x):
            def from_x():
                arrival(kvb.at[row_slot(k, d), core, h], s.x_recv.at[h, k, d - 1]).wait_recv()

            def from_z():
                arrival(kvb.at[row_slot(k, d), core, h], s.r_recv.at[DETOURS.index(h), k, d - 1]).wait_recv()

            @pl.when(takes_row(k, d))
            def _():
                if h in DETOURS:
                    pl.when(~detoured(k, h, x))(from_x)
                    pl.when(detoured(k, h, x))(from_z)

                    @pl.when(passes_detour(k, DETOURS.index(h)))
                    def _():
                        detour_copy(k, d, DETOURS.index(h)).start()
                else:
                    from_x()
                d_copy(k, d, h).start()

    early = min(2, pieces)

    def take_first(h):
        @pl.when(z >= 1)
        def _():
            take_column(1, h)

    start(wcol_local)
    start(wcol_sends)
    column_local.start()
    for name in ("norm_gain", "kv_gain", "kv_latent", "rope"):
        getattr(loads, name).wait()
    for h in range(pieces):
        feature_wait(h)
        if h == pieces - 1:
            column_start()
        normalize(h)
        normed_copy(h).start()
        latents(h)
        pass_on(0, h)
        if h >= early:
            take_first(h - early)

    loads.query_latent.wait()
    loads.q_gain.wait()
    own_normed = normed[core].reshape(half, n_tp * block)
    latq[core] = rms_rows(dot(own_normed, w.query_latent[...]), small.q_gain[...]).astype(BF16)
    latq_copy = remote(latq.at[core], latq.at[core], s.q_sems.at[0], s.q_sems.at[1], to_sibling)
    latq_copy.start()

    arrival(normed.at[other], s.n_sems.at[1]).wait_recv()

    def all_normed():
        return normed[...].reshape(rows, n_tp * block)

    for name in MERGED:
        getattr(loads, name).wait()
    if merged:
        qkv = dot(all_normed(), s.w_qkv[...]).astype(BF16)
    else:
        qkv = jnp.concatenate([dot(all_normed(), getattr(w, name)[...]) for name in MERGED], axis=1).astype(BF16)
    local_kv[...] = qkv[:, : 2 * kv_width]
    queries[...] = qkv[:, 2 * kv_width :]
    tail = local_kv.at[pl.ds(rows - WINDOW, WINDOW)]
    halo_copy = remote(tail, halo, s.halo_sem.at[0], s.halo_sem.at[1], {"sp": sp + 1, "tp": tp})

    take_first(pieces - 2)

    def queries_up():
        arrival(latq.at[other], s.q_sems.at[1]).wait_recv()
        loads.content.wait()
        loads.rotary.wait()
        latent_query = latq[...].reshape(rows, latent)
        content = dot(latent_query, w.content[...])
        rotary = dot(latent_query, w.rotary[...])
        cos_all, sin_all = cosine[...].reshape(rows, ROPE), sine[...].reshape(rows, ROPE)
        padding = jnp.zeros((rows, LANES - ROPE), F32)
        for h in range(lat_heads):
            turned = rotary[:, h * ROPE : (h + 1) * ROPE]
            turned = turned * cos_all + swap_halves(turned) * sin_all
            q_full[h, :NOPE, :] = content[:, h * NOPE : (h + 1) * NOPE].T.astype(BF16)
            q_full[h, NOPE:, :] = jnp.concatenate([turned, padding], axis=1).T.astype(BF16)
        loads.key_up.wait()
        loads.value_up.wait()

    def attend(slot, diagonal):
        source = kvb[slot, :, :, :piece, :].reshape(rows, latent)
        rope_part = rope_rows(slot)
        keys = dot(source, w.key_up[...]).astype(BF16)
        values = dot(source, w.value_up[...]).astype(BF16)
        heads = range(lat_heads)
        scores = []
        for h in heads:
            key = jnp.concatenate([keys[:, h * NOPE : (h + 1) * NOPE], rope_part], axis=1)
            scores.append(dot(key, q_full[h]) * ((NOPE + ROPE) ** (-0.5) * LOG2_E))
        if diagonal:
            live = (lax.broadcasted_iota(jnp.int32, (rows, rows), 0)
                    <= lax.broadcasted_iota(jnp.int32, (rows, rows), 1))
            scores = [jnp.where(live, part, NEGATIVE) for part in scores]
        weights, fades = [], []
        for h in heads:
            peak = jnp.max(scores[h], axis=0, keepdims=True)
            if not diagonal:
                before = top[h]
                peak = jnp.maximum(peak, before)
                fades.append(jnp.exp2(before - peak))
            top[h] = peak
            weights.append(jnp.exp2(scores[h] - peak))
        for h in heads:
            weight_sum = jnp.sum(weights[h], axis=0, keepdims=True)
            part = dot_tl(values[:, h * VDIM : (h + 1) * VDIM], weights[h].astype(BF16))
            if not diagonal:
                weight_sum = total[h] * fades[h] + weight_sum
                part = acc[h] * fades[h] + part
            total[h] = weight_sum
            acc[h] = part

    def take_halo():
        @pl.when(sp > 0)
        def _():
            arrival(halo, s.halo_sem.at[1]).wait_recv()

        @pl.when(sp == 0)
        def _():
            halo[...] = jnp.zeros(halo.shape, BF16)

    def window(blocks):
        row = lax.broadcasted_iota(jnp.int32, (2 * WINDOW, WINDOW), 1)
        column = lax.broadcasted_iota(jnp.int32, (2 * WINDOW, WINDOW), 0)
        offset = row + WINDOW - column
        in_band = (offset >= 0) & (offset < WINDOW)
        in_band = jnp.concatenate([in_band] * group, axis=1)
        later = jnp.concatenate([(sp > 0) | (column >= WINDOW)] * group, axis=1)
        units = [(n, g) for n in blocks for g in range(kv_heads)]
        scores, values, sinks, weights = [], [], [], []
        for n, g in units:
            at = slice(n * WINDOW, (n + 1) * WINDOW)
            earlier = halo[...] if n == 0 else local_kv[(n - 1) * WINDOW : n * WINDOW]
            band = jnp.concatenate([earlier, local_kv[at]], axis=0)
            valid = in_band & later if n == 0 else in_band
            key = band[:, g * HEAD : (g + 1) * HEAD]
            values.append(band[:, kv_width + g * HEAD : kv_width + (g + 1) * HEAD])
            members = range(g * group, (g + 1) * group)
            query = jnp.concatenate([queries[at, q * HEAD : (q + 1) * HEAD] for q in members], axis=0)
            sinks.append(jnp.concatenate([jnp.full((1, WINDOW), small.sinks[0, q], F32) for q in members], axis=1))
            scores.append(jnp.where(valid, dot_t(key, query) * HEAD ** (-0.5), NEGATIVE))
        for u in range(len(units)):
            peak = jnp.maximum(jnp.max(scores[u], axis=0, keepdims=True), sinks[u])
            part = jnp.exp(scores[u] - peak)
            bottom = jnp.sum(part, axis=0, keepdims=True) + jnp.exp(sinks[u] - peak)
            weights.append((part * (1.0 / bottom)).astype(BF16))
        mixed = [dot_tl(values[u], weights[u]) for u in range(len(units))]
        for b, n in enumerate(blocks):
            heads = [
                mixed[b * kv_heads + g][:, i * WINDOW : (i + 1) * WINDOW]
                for g in range(kv_heads) for i in range(group)
            ]
            winb[core, n * WINDOW : (n + 1) * WINDOW, :] = jnp.concatenate(heads, axis=0).T.astype(BF16)

    def win_copy(i):
        ref = winb.at[core, win_rows[i]]
        return remote(ref, ref, s.win_send.at[i], s.win_recv.at[i], to_sibling)

    win_rows = (pl.ds(WINDOW, rows - WINDOW), pl.ds(0, WINDOW))

    def window_part(j, at):
        return dot(winb[0, at], wcol[0, j]) + dot(winb[1, at], wcol[1, j])

    def part_copy(d, at):
        return remote(psend.at[d - 1, at], precv.at[d - 1, at], s.p_send.at[d - 1], s.p_recv.at[d - 1],
                      {"sp": sp, "tp": lax.rem(y + d, n_y) * 2 + core})

    def window_parts(i):
        at = win_rows[i]
        arrival(winb.at[other, at], s.win_recv.at[i]).wait_recv()
        for d in range(1, n_y):
            psend[d - 1, at] = window_part(lax.rem(y + d, n_y), at).astype(BF16)
            part_copy(d, at).start()

    def gate(b):
        name = WEIGHTS[10 + b]
        getattr(loads, name).wait()

        def step(i, _):
            at = pl.ds(pl.multiple_of(i * 256, LANES), 256)
            gates[b, :, at] = jax.nn.sigmoid(dot(all_normed(), getattr(w, name)[:, at]))
            return 0

        lax.fori_loop(0, block // 256, step, 0)

    def take_second(lo, hi):
        for h in range(lo, hi):
            @pl.when(z >= 2)
            def _():
                take_column(2, h)

    def take_rows(k):
        for h in range(pieces):
            take_row(k, h)

    def attend_row(k, d):
        wait_row(k, d)
        attend(row_slot(k, d), False)

    loads.sinks.wait()
    window(range(1, rows // WINDOW))
    win_copy(0).start()
    take_first(pieces - 1)
    queries_up()
    if n_z > 2:
        take_second(0, pieces // 2)
    pltpu.make_async_copy(wcol.at[core], wcol.at[core], s.w_sems.at[0]).wait()
    arrival(wcol.at[other], s.w_sems.at[2]).wait_recv()
    window_parts(0)
    take_rows(0)
    wait_column(0)
    attend(sp, True)
    if n_z > 2:
        take_second(pieces // 2, pieces - 1)

    @pl.when(sp + 1 < n_sp)
    def _():
        halo_copy.start()

    def take_pieces(k, lo, hi):
        @pl.when(z >= k)
        def _():
            for h in range(lo, hi):
                take_column(k, h)

    near = (x > 0) | (z == 0)

    def first_window():
        take_halo()
        window(range(1))
        win_copy(1).start()

    def last_parts():
        window_parts(1)

    def step(k, _):
        @pl.when((k == 3) & (parity == 1))
        def _():
            pair_forward()

        @pl.when(z >= k - 1)
        def _():
            wait_column(k - 1)
            attend(column_slot(k - 1), False)

        @pl.when(k == 2)
        def _():
            take_pieces(k, pieces - 1, pieces)

        pl.when((k == 4) & near)(last_parts)
        pl.when((k == 4) & ~near)(first_window)

        @pl.when((k == 4) & (z == 0))
        def _():
            pair_forward()

        @pl.when(k > 2)
        def _():
            take_pieces(k, 0, pieces // 2)

        @pl.when((z >= k - 1) & (k == n_z) & near)
        def _():
            take_rows(k - 1)

        for d in range(1, n_x):
            @pl.when((z >= k - 2) & takes_row(k - 2, d))
            def _():
                attend_row(k - 2, d)


        @pl.when(k > 2)
        def _():
            take_pieces(k, pieces // 2, pieces)

        pl.when((k == 3) & near)(first_window)
        pl.when((k == 4) & ~near)(last_parts)

        @pl.when((z >= k - 1) & ~((k == n_z) & near))
        def _():
            take_rows(k - 1)

        return 0

    lax.fori_loop(2, max(n_z, 3) + 2, step, 0)

    @pl.when((parity == 0) & (z > 0))
    def _():
        pair_forward()

    def gather(part):
        own = lat.at[tp, part]
        sends = [
            remote(own, own, s.y_send.at[d - 1], s.y_recv.at[part, d - 1],
                   {"sp": sp, "tp": lax.rem(y + d, n_y) * 2 + core})
            for d in range(1, n_y)
        ]
        sends.append(remote(own, own, s.s_send.at[0], s.s_recv.at[part], to_sibling))
        return sends

    def forward(part):
        for d in range(1, n_y):
            ref = lat.at[lax.rem(y + n_y - d, n_y) * 2 + core, part]
            arrival(ref, s.y_recv.at[part, d - 1]).wait_recv()
            remote(ref, ref, s.s_send.at[d], s.s_recv.at[part], to_sibling).start()

    def arrived(part):
        arrival(lat.at[pl.ds(0, n_y), part], s.s_recv.at[part]).wait_recv()

    for part in range(out_parts):
        at = slice(part * out_rows, (part + 1) * out_rows)
        for h in range(lat_heads):
            lat[tp, part, :, h * VDIM : (h + 1) * VDIM] = (
                acc[h, :, at] / total[h, :, at]).T.astype(BF16)
        start(gather(part))
    gate(0)
    gate(1)
    window_branch = window_part(y, pl.ds(0, rows))
    for d in range(1, n_y):
        arrival(precv.at[d - 1], s.p_recv.at[d - 1]).wait_recv()
        window_branch = window_branch + precv[d - 1].astype(F32)
    gates[0] = gates[0] * window_branch
    column_local.wait()
    arrival(columns.at[sibling], s.col_recv.at[0]).wait_recv()
    for d in range(1, n_y):
        base = lax.rem(y + n_y - d, n_y) * 2
        if paired:
            arrival(columns.at[base + 1 - parity], s.pair_recv.at[d - 1]).wait_recv()
        else:
            arrival(columns.at[pl.ds(base, 2)], s.col_recv.at[d]).wait_recv()
    for part in range(out_parts):
        at = slice(part * out_rows, (part + 1) * out_rows)
        forward(part)
        arrived(part)
        latent_branch = jnp.zeros((out_rows, block), F32)
        for j in range(n_tp):
            latent_branch = latent_branch + dot(lat[j, part], columns[j])
        out[at, :] = (gates[0, at] + gates[1, at] * latent_branch).astype(BF16)

    def leave(ref, send):
        remote(ref, ref, send, send, to_sibling).wait_send()

    leave(ownf.at[pl.ds(0, half)], s.f_send.at[0])
    for d in range(1, n_y):
        leave(ownf, s.f_send.at[d])
    leave(normed.at[core], s.n_sems.at[0])
    latq_copy.wait_send()
    leave(wcol.at[core], s.w_sems.at[1])
    leave(columns.at[tp], s.col_send.at[0])

    @when_across
    def _():
        for d in range(1, n_y):
            leave(columns.at[pl.ds(0, 2)], s.col_send.at[d])

    if paired:
        for d in range(1, n_y):
            pair_copy(d).wait_send()
    for i in range(2):
        win_copy(i).wait_send()
    for d in range(1, n_y):
        leave(psend.at[d - 1], s.p_send.at[d - 1])
        leave(lat.at[tp], s.y_send.at[d - 1])
        leave(lat.at[tp], s.s_send.at[d])
    leave(lat.at[tp], s.s_send.at[0])

    @pl.when(sp + 1 < n_sp)
    def _():
        halo_copy.wait_send()

    def drain(k, _):
        @pl.when(z >= k)
        def _():
            own = kvb.at[column_slot(k), core]

            @pl.when(z + 1 < n_z)
            def _():
                leave(own, s.z_send.at[k])

            leave(own, s.c_send.at[k])
            for d in range(1, n_x):
                to = lax.rem(x + d, n_x)
                fewer = [detoured(k, h, to) for h in DETOURS]

                @pl.when(sends_row(k, d) & ~fewer[0])
                def _():
                    leave(own, s.x_send.at[k, d - 1])

                @pl.when(fewer[0] & ~fewer[1])
                def _():
                    leave(own.at[pl.ds(0, pieces - 1)], s.x_send.at[k, d - 1])

                @pl.when(fewer[1])
                def _():
                    leave(own.at[pl.ds(0, pieces - 2)], s.x_send.at[k, d - 1])

                for i in range(2):
                    @pl.when(takes_row(k, d) & passes_detour(k, i))
                    def _():
                        detour_copy(k, d, i).wait_send()

                @pl.when(takes_row(k, d))
                def _():
                    leave(own, s.d_send.at[k, d - 1])

        return 0

    lax.fori_loop(0, n_z, drain, 0)


def on_device(dims, features, norm_gain, w_query, w_key, w_value, head_sinks, w_query_latent,
              w_kv_latent, w_rope_key, query_latent_gain, kv_latent_gain, w_query_content,
              w_query_rotary, w_key_up, w_value_up, w_branch_window, w_branch_latent,
              w_gate_window, w_gate_latent):
    n_sp, n_tp, n_x = dims
    n_z, n_y = n_sp // n_x, n_tp // 2
    rows, block = features.shape
    width = norm_gain.shape[0]
    latent = w_kv_latent.shape[1]
    lat_heads = w_key_up.shape[1] // NOPE
    half_width = ROPE // 2
    entry = np.arange(ROPE, dtype=np.int32) % half_width
    frequency = (np.float32(THETA) ** (-entry.astype(np.float32) / np.float32(half_width))).astype(np.float32)[None, :]
    weights = (w_kv_latent, w_rope_key.T, w_key, w_value, w_query, w_query_latent, w_query_content,
               w_query_rotary, w_key_up, w_value_up, w_gate_window, w_gate_latent)
    smalls = (norm_gain[None, :], head_sinks[None, :], query_latent_gain[None, :], kv_latent_gain[None, :],
              jnp.asarray(frequency))
    branch_rows = w_branch_window.shape[0]
    pieces = PIECES
    piece = rows // 2 // pieces
    out_parts = rows // LANES
    merge = w_key.shape[1] % LANES == 0
    hbm = pl.BlockSpec(memory_space=pl.ANY)
    dma = pltpu.SemaphoreType.DMA
    vm = pltpu.VMEM
    scratch = dict(
        **{"small_" + n: (pltpu.SMEM if n == "sinks" else vm)(a.shape, F32) for n, a in zip(SMALL, smalls)},
        **{"w_" + n: vm(a.shape, BF16) for n, a in zip(WEIGHTS, weights) if not (merge and n in MERGED)},
        **(dict(w_qkv=vm((width, 2 * w_key.shape[1] + w_query.shape[1]), BF16)) if merge else {}),
        ownf=vm((rows, block), BF16),
        feat=vm((n_tp, rows // 2, block), BF16),
        normed=vm((2, pieces, piece, width), BF16),
        latq=vm((2, rows // 2, latent), BF16),
        wcol=vm((2, n_y, branch_rows, block), BF16),
        columns=vm((n_tp, w_branch_latent.shape[0], block), BF16),
        psend=vm((n_y - 1, rows, block), BF16),
        precv=vm((n_y - 1, rows, block), BF16),
        kvb=vm((n_sp, 2, pieces, piece + SUBLANES, latent), BF16),
        local_kv=vm((rows, 2 * w_key.shape[1]), BF16),
        halo=vm((WINDOW, 2 * w_key.shape[1]), BF16),
        queries=vm((rows, w_query.shape[1]), BF16),
        q_full=vm((lat_heads, NOPE + LANES, rows), BF16),
        gates=vm((2, rows, block), F32),
        winb=vm((2, rows, w_query.shape[1]), BF16),
        lat=vm((n_tp, out_parts, rows // out_parts, lat_heads * VDIM), BF16),
        top=vm((lat_heads, 1, rows), F32),
        total=vm((lat_heads, 1, rows), F32),
        acc=vm((lat_heads, VDIM, rows), F32),
        cosine=vm((2, pieces, piece, ROPE), F32),
        sine=vm((2, pieces, piece, ROPE), F32),
        own_sem=dma((2,)),
        small_sem=dma((len(SMALL),)),
        w_sem=dma((len(weights),)),
        f_send=dma((n_y,)),
        f_recv=dma((pieces,)),
        n_sems=dma((2,)),
        q_sems=dma((2,)),
        w_sems=dma((3,)),
        col_own=dma((1,)),
        col_send=dma((n_y,)),
        col_recv=dma((n_y,)),
        pair_send=dma((n_y - 1,)),
        pair_recv=dma((n_y - 1,)),
        halo_sem=dma((2,)),
        win_send=dma((2,)),
        win_recv=dma((2,)),
        p_send=dma((n_y - 1,)),
        p_recv=dma((n_y - 1,)),
        y_send=dma((n_y - 1,)),
        y_recv=dma((out_parts, n_y - 1)),
        s_send=dma((n_y,)),
        s_recv=dma((out_parts,)),
        z_send=dma((n_z - 1,)),
        z_recv=dma((pieces, n_z - 1)),
        r_send=dma((2, n_z, n_x - 1)),
        r_recv=dma((2, n_z, n_x - 1)),
        x_send=dma((n_z, n_x - 1)),
        x_recv=dma((pieces, n_z, n_x - 1)),
        c_send=dma((n_z,)),
        c_recv=dma((n_z,)),
        d_send=dma((n_z, n_x - 1)),
        d_recv=dma((n_z, n_x - 1)),
    )
    return pl.pallas_call(
        functools.partial(kernel, dims, tuple(scratch)),
        out_shape=pltpu.VMEM((rows, block), BF16),
        in_specs=[hbm] * (1 + len(smalls) + len(weights) + 2),
        out_specs=pl.BlockSpec(memory_space=pltpu.VMEM),
        scratch_shapes=list(scratch.values()),
        compiler_params=pltpu.CompilerParams(
            collective_id=0, has_side_effects=True, vmem_limit_bytes=60 * 1024 * 1024
        ),
    )(features, *smalls, *weights, w_branch_window, w_branch_latent)


def solution(mesh):
    n_sp, n_tp = mesh.shape["sp"], mesh.shape["tp"]
    n_x = 1
    while n_sp % (2 * n_x) == 0 and 8 * n_x * n_x <= n_sp:
        n_x *= 2
    return jax.shard_map(
        functools.partial(on_device, (n_sp, n_tp, n_x)),
        mesh=mesh,
        in_specs=(
            P("sp", "tp"),
            P(),
            P(None, "tp"),
            P(None, "tp"),
            P(None, "tp"),
            P("tp"),
            P(),
            P(),
            P(),
            P(),
            P(),
            P(None, "tp"),
            P(None, "tp"),
            P(None, "tp"),
            P(None, "tp"),
            P("tp", None),
            P("tp", None),
            P(None, "tp"),
            P(None, "tp"),
        ),
        out_specs=P("sp", "tp"),
        check_vma=False,
    )
```

```python
import functools
import types

import jax
import jax.numpy as jnp
import numpy as np
from jax import lax
from jax.experimental import pallas as pl
from jax.experimental.pallas import tpu as pltpu
from jax.sharding import PartitionSpec as P

HEAD = 64
WINDOW = 128
NOPE = 128
ROPE = 64
VDIM = 128


EPS = 1e-06
THETA = 10000.0
NEGATIVE = -1e30
LANES = 128
LOG2_E = 1.4426950408889634
MESH = pl.DeviceIdType.MESH
BF16 = jnp.bfloat16
F32 = jnp.float32
PIECES = 4
SUBLANES = 8
DETOURS = (0, PIECES - 1)


def dot(left, right):
    return jnp.dot(left, right, preferred_element_type=F32)


def dot_t(left, right):
    return lax.dot_general(left, right, (((1,), (1,)), ((), ())), preferred_element_type=F32)


def dot_tl(left, right):
    return lax.dot_general(left, right, (((0,), (0,)), ((), ())), preferred_element_type=F32)


def rms_rows(rows, gain):
    return rows * lax.rsqrt(jnp.mean(rows * rows, axis=-1, keepdims=True) + EPS) * gain


def swap_halves(rows):
    half = rows.shape[1] // 2
    return jnp.concatenate([rows[:, half:], rows[:, :half]], axis=1)


SMALL = ("norm_gain", "sinks", "q_gain", "kv_gain", "frequency")
WEIGHTS = (
    "kv_latent", "rope", "key", "value", "query", "query_latent", "content", "rotary",
    "key_up", "value_up", "gate_window", "gate_latent",
)
def bundle(names, values):
    return types.SimpleNamespace(**dict(zip(names, values)))


MERGED = ("key", "value", "query")


def kernel(dims, names, *refs):
    n_sp, n_tp, n_x = dims
    n_z, n_y = n_sp // n_x, n_tp // 2
    features = refs[0]
    small_hbm = bundle(SMALL, refs[1:6])
    w_hbm = bundle(WEIGHTS, refs[6:18])
    window_hbm, latent_hbm = refs[18:20]
    out = refs[20]
    s = bundle(names, refs[21:])
    small = bundle(SMALL, [getattr(s, "small_" + name) for name in SMALL])
    merged = "w_qkv" in names
    kept = [name for name in WEIGHTS if "w_" + name in names]
    w = bundle(kept, [getattr(s, "w_" + name) for name in kept])
    ownf, feat, normed = s.ownf, s.feat, s.normed
    turn = s.turn
    kvb, local_kv, halo, queries, q_full, latq = s.kvb, s.local_kv, s.halo, s.queries, s.q_full, s.latq
    gates, winb, lat, top, total, acc = s.gates, s.winb, s.lat, s.top, s.total, s.acc
    wcol, columns, psend, precv = s.wcol, s.columns, s.psend, s.precv
    cosine, sine = s.cosine, s.sine

    sp, tp = lax.axis_index("sp"), lax.axis_index("tp")
    z, x = sp // n_x, lax.rem(sp, n_x)
    y, core = tp // 2, lax.rem(tp, 2)
    other = 1 - core
    sibling = y * 2 + other
    rows, block = features.shape
    half = rows // 2
    pieces = normed.shape[1]
    piece = half // pieces
    lat_heads = w_hbm.key_up.shape[1] // NOPE
    kv_width = w_hbm.key.shape[1]
    kv_heads = kv_width // HEAD
    group = w_hbm.query.shape[1] // kv_width
    latent = w_hbm.kv_latent.shape[1]
    out_parts = lat.shape[1]
    out_rows = rows // out_parts

    def remote(src, dst, send, recv, where):
        return pltpu.make_async_remote_copy(
            src_ref=src, dst_ref=dst, send_sem=send, recv_sem=recv,
            device_id=where, device_id_type=MESH,
        )

    to_sibling = {"sp": sp, "tp": sibling}

    def arrival(ref, recv):
        return remote(ref, ref, recv, recv, to_sibling)

    def start(copies):
        for copy in copies:
            copy.start()

    def own_rows(c, h):
        return ownf.at[pl.ds(pl.multiple_of(c * half + h * piece, 16), piece)]

    def feat_rows(j, h):
        return feat.at[j, pl.ds(h * piece, piece)]

    own_load = [
        pltpu.make_async_copy(features, ownf, s.own_sem.at[0]),
        pltpu.make_async_copy(
            features.at[pl.ds(pl.multiple_of(core * half, 16), half)], feat.at[tp], s.own_sem.at[1]),
    ]
    start(own_load)
    loads = bundle(SMALL, [
        pltpu.make_async_copy(getattr(small_hbm, name), getattr(small, name), s.small_sem.at[i])
        for i, name in enumerate(SMALL)
    ])
    for name in SMALL:
        getattr(loads, name).start()

    barrier = pltpu.get_barrier_semaphore()

    def greet(where):
        pl.semaphore_signal(barrier, inc=1, device_id=where, device_id_type=MESH)

    for d in range(1, n_tp):
        greet({"sp": sp, "tp": lax.rem(tp + d, n_tp)})
    for d in range(1, n_x):
        greet({"sp": z * n_x + lax.rem(x + d, n_x), "tp": tp})

    @pl.when(z + 1 < n_z)
    def _():
        greet({"sp": sp + n_x, "tp": tp})

    @pl.when(z > 0)
    def _():
        greet({"sp": sp - n_x, "tp": tp})

    @pl.when(sp + 1 < n_sp)
    def _():
        greet({"sp": sp + 1, "tp": tp})

    @pl.when(sp > 0)
    def _():
        greet({"sp": sp - 1, "tp": tp})

    one, none = jnp.int32(1), jnp.int32(0)
    pl.semaphore_wait(
        barrier,
        n_tp - 1 + n_x - 1
        + jnp.where(z + 1 < n_z, one, none) + jnp.where(z > 0, one, none)
        + jnp.where(sp + 1 < n_sp, one, none) + jnp.where(sp > 0, one, none),
    )

    def feature_sends(h):
        sends = []
        for d in range(1, n_y):
            for c in range(2):
                sends.append(remote(
                    own_rows(c, h), feat_rows(tp, h), s.f_send.at[d], s.f_recv.at[h],
                    {"sp": sp, "tp": lax.rem(y + d, n_y) * 2 + c}))
        sends.append(remote(
            own_rows(other, h), feat_rows(tp, h), s.f_send.at[0], s.f_recv.at[h], to_sibling))
        return sends

    def feature_wait(h):
        arrival(feat.at[pl.ds(0, n_tp - 1), pl.ds(h * piece, piece)], s.f_recv.at[h]).wait_recv()

    for copy in own_load:
        copy.wait()
    for h in range(pieces):
        start(feature_sends(h))

    first = 0
    for i, name in enumerate(WEIGHTS):
        source = getattr(w_hbm, name)
        if name in kept:
            to = getattr(w, name)
        else:
            to = s.w_qkv.at[:, pl.ds(first, source.shape[1])]
            first += source.shape[1]
        copy = pltpu.make_async_copy(source, to, s.w_sem.at[i])
        copy.start()
        setattr(loads, name, copy)

    def window_columns():
        local, sends = [], []
        for j in range(n_y):
            local.append(pltpu.make_async_copy(
                window_hbm.at[:, pl.ds(pl.multiple_of((j * 2 + core) * block, LANES), block)],
                wcol.at[core, j], s.w_sems.at[0]))
            sends.append(remote(
                window_hbm.at[:, pl.ds(pl.multiple_of((j * 2 + other) * block, LANES), block)],
                wcol.at[core, j], s.w_sems.at[1], s.w_sems.at[2], to_sibling))
        return local, sends

    paired = n_z % 2 == 0
    parity = lax.rem(z, 2)
    partner = {"sp": sp + n_x * (1 - 2 * parity), "tp": tp}

    def column_send(to, d):
        return remote(
            latent_hbm.at[:, pl.ds(pl.multiple_of(to * block, LANES), block)],
            columns.at[tp], s.col_send.at[d], s.col_recv.at[d], {"sp": sp, "tp": to})

    def when_across(act):
        if paired:
            pl.when(core == parity)(act)
        else:
            act()

    def column_start():
        column_send(sibling, 0).start()

        @when_across
        def _():
            for d in range(1, n_y):
                for c in range(2):
                    column_send(lax.rem(y + d, n_y) * 2 + c, d).start()

    def pair_copy(d):
        ref = columns.at[lax.rem(y + n_y - d, n_y) * 2 + parity]
        return remote(ref, ref, s.pair_send.at[d - 1], s.pair_recv.at[d - 1], partner)

    def pair_forward():
        if paired:
            for d in range(1, n_y):
                source = lax.rem(y + n_y - d, n_y) * 2 + parity
                arrival(columns.at[source], s.col_recv.at[d]).wait_recv()
                pair_copy(d).start()

    column_local = pltpu.make_async_copy(
        latent_hbm.at[:, pl.ds(pl.multiple_of(tp * block, LANES), block)],
        columns.at[tp], s.col_own.at[0])

    wcol_local, wcol_sends = window_columns()

    loads.frequency.wait()
    positions = (sp * rows + lax.broadcasted_iota(jnp.int32, (rows, ROPE), 0)).astype(F32)
    angles = positions * small.frequency[...]
    lane = lax.broadcasted_iota(jnp.int32, (rows, ROPE), 1)
    cosine[...] = jnp.cos(angles).reshape(cosine.shape)
    turned = jnp.sin(angles)
    sine[...] = jnp.where(lane < ROPE // 2, -turned, turned).reshape(sine.shape)

    def normalize(h):
        squares = jnp.zeros((piece, 1), F32)
        part = slice(h * piece, (h + 1) * piece)
        for j in range(n_tp):
            values = feat[j, part].astype(F32)
            squares = squares + jnp.sum(values * values, axis=-1, keepdims=True)
        scale = lax.rsqrt(squares / (n_tp * block) + EPS)
        for j in range(n_tp):
            span = slice(j * block, (j + 1) * block)
            values = feat[j, part].astype(F32) * scale * small.norm_gain[:, span]
            normed[core, h, :, span] = values.astype(BF16)

    def normed_copy(h):
        return remote(normed.at[core, h], normed.at[core, h], s.n_sems.at[0], s.n_sems.at[1], to_sibling)

    def latents(h):
        own = normed[core, h]
        rope = dot_t(own, w.rope[...])
        rope = rope * cosine[core, h] + swap_halves(rope) * sine[core, h]
        rope = jnp.concatenate([rope[: piece // 2], rope[piece // 2 :]], axis=1)
        rope = [rope[i : i + SUBLANES] for i in range(0, piece // 2, SUBLANES)]
        rope.append(jnp.zeros((SUBLANES, latent - len(rope) * LANES), F32))
        kvb[sp, core, h, :piece, :] = rms_rows(dot(own, w.kv_latent[...]), small.kv_gain[...]).astype(BF16)
        kvb[sp, core, h, piece:, :] = jnp.concatenate(rope, axis=1).astype(BF16)

    def rope_rows(slot):
        parts = []
        for c in range(2):
            for h in range(pieces):
                packed = kvb[slot, c, h, piece:, :].astype(F32)
                pair = jnp.concatenate(
                    [packed[:, i * LANES : (i + 1) * LANES] for i in range(piece // 2 // SUBLANES)], axis=0)
                parts += [pair, pltpu.roll(pair, ROPE, 1)]
        return jnp.concatenate(parts, axis=0).astype(BF16)

    def column_slot(k):
        return (z - k) * n_x + x

    def row_slot(k, d):
        return (z - k) * n_x + lax.rem(x + n_x - d, n_x)

    def z_copy(k, h):
        ref = kvb.at[column_slot(k), core, h]
        return remote(ref, ref, s.z_send.at[k], s.z_recv.at[h, k], {"sp": sp + n_x, "tp": tp})

    def x_copy(k, d, h):
        ref = kvb.at[column_slot(k), core, h]
        return remote(ref, ref, s.x_send.at[k, d - 1], s.x_recv.at[h, k, d - 1],
                      {"sp": z * n_x + lax.rem(x + d, n_x), "tp": tp})

    def c_copy(k, h):
        ref = kvb.at[column_slot(k), core, h]
        return remote(ref, ref, s.c_send.at[k], s.c_recv.at[k], to_sibling)

    def d_copy(k, d, h):
        ref = kvb.at[row_slot(k, d), core, h]
        return remote(ref, ref, s.d_send.at[k, d - 1], s.d_recv.at[k, d - 1], to_sibling)

    def wait_column(k):
        arrival(kvb.at[column_slot(k), other], s.c_recv.at[k]).wait_recv()

    def wait_row(k, d):
        arrival(kvb.at[row_slot(k, d), other], s.d_recv.at[k, d - 1]).wait_recv()

    def sends_row(k, d):
        return (k > 0) | (x + d < n_x)

    def takes_row(k, d):
        return (k > 0) | (x >= d)

    def detoured(k, h, to):
        if h == DETOURS[0]:
            return (k >= 2) & (to > 0)
        return (k >= 3) & (to == 0)

    def pass_on(k, h):
        @pl.when(z + 1 < n_z)
        def _():
            z_copy(k, h).start()

        for d in range(1, n_x):
            to = lax.rem(x + d, n_x)

            @pl.when(sends_row(k, d) & ~detoured(k, h, to) if h in DETOURS else sends_row(k, d))
            def _():
                x_copy(k, d, h).start()

        c_copy(k, h).start()

    def take_column(k, h):
        arrival(kvb.at[column_slot(k), core, h], s.z_recv.at[h, k - 1]).wait_recv()
        pass_on(k, h)

    def detour_copy(k, d, i):
        ref = kvb.at[row_slot(k, d), core, DETOURS[i]]
        return remote(ref, ref, s.r_send.at[i, k - 1, d - 1], s.r_recv.at[i, k - 1, d - 1], {"sp": sp + n_x, "tp": tp})

    def passes_detour(k, i):
        return (z + 1 < n_z) & detoured(k + 1, DETOURS[i], x)

    def take_row(k, h):
        for d in range(1, n_x):
            def from_x():
                arrival(kvb.at[row_slot(k, d), core, h], s.x_recv.at[h, k, d - 1]).wait_recv()

            def from_z():
                arrival(kvb.at[row_slot(k, d), core, h], s.r_recv.at[DETOURS.index(h), k - 2, d - 1]).wait_recv()

            @pl.when(takes_row(k, d))
            def _():
                if h in DETOURS:
                    pl.when(~detoured(k, h, x))(from_x)
                    pl.when(detoured(k, h, x))(from_z)

                    @pl.when(passes_detour(k, DETOURS.index(h)))
                    def _():
                        detour_copy(k, d, DETOURS.index(h)).start()
                else:
                    from_x()
                d_copy(k, d, h).start()

    def take_second(lo, hi):
        for h in range(lo, hi):
            @pl.when(z >= 2)
            def _():
                take_column(2, h)

    def take_first(h):
        @pl.when(z >= 1)
        def _():
            take_column(1, h)

    start(wcol_local)
    start(wcol_sends)
    column_local.start()
    for name in ("norm_gain", "kv_gain", "kv_latent", "rope"):
        getattr(loads, name).wait()
    for h in range(pieces):
        feature_wait(h)
        if h == pieces - 1:
            column_start()
        normalize(h)
        normed_copy(h).start()
        latents(h)
        pass_on(0, h)
        if 1 <= h <= pieces // 2:
            take_first(h - 1)

    loads.query_latent.wait()
    loads.q_gain.wait()
    own_normed = normed[core].reshape(half, n_tp * block)
    latq[core] = rms_rows(dot(own_normed, w.query_latent[...]), small.q_gain[...]).astype(BF16)
    latq_copy = remote(latq.at[core], latq.at[core], s.q_sems.at[0], s.q_sems.at[1], to_sibling)
    latq_copy.start()

    arrival(normed.at[other], s.n_sems.at[1]).wait_recv()

    if n_z > 2:
        take_second(0, 1)

    def all_normed():
        return normed[...].reshape(rows, n_tp * block)

    for name in MERGED:
        getattr(loads, name).wait()
    if merged:
        qkv = dot(all_normed(), s.w_qkv[...]).astype(BF16)
    else:
        qkv = jnp.concatenate([dot(all_normed(), getattr(w, name)[...]) for name in MERGED], axis=1).astype(BF16)
    local_kv[...] = qkv[:, : 2 * kv_width]
    queries[...] = qkv[:, 2 * kv_width :]
    tail = local_kv.at[pl.ds(rows - WINDOW, WINDOW)]
    halo_copy = remote(tail, halo, s.halo_sem.at[0], s.halo_sem.at[1], {"sp": sp + 1, "tp": tp})
    turn_copy = remote(tail, turn, s.halo_sem.at[0], s.halo_sem.at[2], {"sp": z * n_x, "tp": tp})
    relay_copy = remote(turn, halo, s.halo_sem.at[3], s.halo_sem.at[1], {"sp": sp + n_x, "tp": tp})

    @pl.when((x + 1 == n_x) & (z + 1 < n_z))
    def _():
        turn_copy.start()

    take_first(pieces - 2)

    def queries_up():
        arrival(latq.at[other], s.q_sems.at[1]).wait_recv()
        loads.content.wait()
        loads.rotary.wait()
        latent_query = latq[...].reshape(rows, latent)
        content = dot(latent_query, w.content[...])
        rotary = dot(latent_query, w.rotary[...])
        cos_all, sin_all = cosine[...].reshape(rows, ROPE), sine[...].reshape(rows, ROPE)
        padding = jnp.zeros((rows, LANES - ROPE), F32)
        for h in range(lat_heads):
            turned = rotary[:, h * ROPE : (h + 1) * ROPE]
            turned = turned * cos_all + swap_halves(turned) * sin_all
            q_full[h, :NOPE, :] = content[:, h * NOPE : (h + 1) * NOPE].T.astype(BF16)
            q_full[h, NOPE:, :] = jnp.concatenate([turned, padding], axis=1).T.astype(BF16)
        loads.key_up.wait()
        loads.value_up.wait()

    def attend(slot, diagonal):
        source = kvb[slot, :, :, :piece, :].reshape(rows, latent)
        rope_part = rope_rows(slot)
        keys = dot(source, w.key_up[...]).astype(BF16)
        values = dot(source, w.value_up[...]).astype(BF16)
        heads = range(lat_heads)
        scores = []
        for h in heads:
            key = jnp.concatenate([keys[:, h * NOPE : (h + 1) * NOPE], rope_part], axis=1)
            scores.append(dot(key, q_full[h]) * ((NOPE + ROPE) ** (-0.5) * LOG2_E))
        if diagonal:
            live = (lax.broadcasted_iota(jnp.int32, (rows, rows), 0)
                    <= lax.broadcasted_iota(jnp.int32, (rows, rows), 1))
            scores = [jnp.where(live, part, NEGATIVE) for part in scores]
        weights, fades = [], []
        for h in heads:
            peak = jnp.max(scores[h], axis=0, keepdims=True)
            if not diagonal:
                before = top[h]
                peak = jnp.maximum(peak, before)
                fades.append(jnp.exp2(before - peak))
            top[h] = peak
            weights.append(jnp.exp2(scores[h] - peak))
        for h in heads:
            weight_sum = jnp.sum(weights[h], axis=0, keepdims=True)
            part = dot_tl(values[:, h * VDIM : (h + 1) * VDIM], weights[h].astype(BF16))
            if not diagonal:
                weight_sum = total[h] * fades[h] + weight_sum
                part = acc[h] * fades[h] + part
            total[h] = weight_sum
            acc[h] = part

    def take_halo():
        @pl.when(sp > 0)
        def _():
            arrival(halo, s.halo_sem.at[1]).wait_recv()

        @pl.when(sp == 0)
        def _():
            halo[...] = jnp.zeros(halo.shape, BF16)

    def window(blocks):
        row = lax.broadcasted_iota(jnp.int32, (2 * WINDOW, WINDOW), 1)
        column = lax.broadcasted_iota(jnp.int32, (2 * WINDOW, WINDOW), 0)
        offset = row + WINDOW - column
        in_band = (offset >= 0) & (offset < WINDOW)
        in_band = jnp.concatenate([in_band] * group, axis=1)
        later = jnp.concatenate([(sp > 0) | (column >= WINDOW)] * group, axis=1)
        units = [(n, g) for n in blocks for g in range(kv_heads)]
        scores, values, sinks, weights = [], [], [], []
        for n, g in units:
            at = slice(n * WINDOW, (n + 1) * WINDOW)
            earlier = halo[...] if n == 0 else local_kv[(n - 1) * WINDOW : n * WINDOW]
            band = jnp.concatenate([earlier, local_kv[at]], axis=0)
            valid = in_band & later if n == 0 else in_band
            key = band[:, g * HEAD : (g + 1) * HEAD]
            values.append(band[:, kv_width + g * HEAD : kv_width + (g + 1) * HEAD])
            members = range(g * group, (g + 1) * group)
            query = jnp.concatenate([queries[at, q * HEAD : (q + 1) * HEAD] for q in members], axis=0)
            sinks.append(jnp.concatenate([jnp.full((1, WINDOW), small.sinks[0, q], F32) for q in members], axis=1))
            scores.append(jnp.where(valid, dot_t(key, query) * HEAD ** (-0.5), NEGATIVE))
        for u in range(len(units)):
            peak = jnp.maximum(jnp.max(scores[u], axis=0, keepdims=True), sinks[u])
            part = jnp.exp(scores[u] - peak)
            bottom = jnp.sum(part, axis=0, keepdims=True) + jnp.exp(sinks[u] - peak)
            weights.append((part * (1.0 / bottom)).astype(BF16))
        mixed = [dot_tl(values[u], weights[u]) for u in range(len(units))]
        for b, n in enumerate(blocks):
            heads = [
                mixed[b * kv_heads + g][:, i * WINDOW : (i + 1) * WINDOW]
                for g in range(kv_heads) for i in range(group)
            ]
            winb[core, n * WINDOW : (n + 1) * WINDOW, :] = jnp.concatenate(heads, axis=0).T.astype(BF16)

    def win_copy(i):
        ref = winb.at[core, win_rows[i]]
        return remote(ref, ref, s.win_send.at[i], s.win_recv.at[i], to_sibling)

    win_rows = (pl.ds(WINDOW, rows - WINDOW), pl.ds(0, WINDOW))

    def window_part(j, at):
        return dot(winb[0, at], wcol[0, j]) + dot(winb[1, at], wcol[1, j])

    def part_copy(d, at):
        return remote(psend.at[d - 1, at], precv.at[d - 1, at], s.p_send.at[d - 1], s.p_recv.at[d - 1],
                      {"sp": sp, "tp": lax.rem(y + d, n_y) * 2 + core})

    def window_parts(i):
        at = win_rows[i]
        arrival(winb.at[other, at], s.win_recv.at[i]).wait_recv()
        for d in range(1, n_y):
            psend[d - 1, at] = window_part(lax.rem(y + d, n_y), at).astype(BF16)
            part_copy(d, at).start()

    def gate(b):
        name = WEIGHTS[10 + b]
        getattr(loads, name).wait()

        def step(i, _):
            at = pl.ds(pl.multiple_of(i * 256, LANES), 256)
            gates[b, :, at] = jax.nn.sigmoid(dot(all_normed(), getattr(w, name)[:, at]))
            return 0

        lax.fori_loop(0, block // 256, step, 0)

    def take_rows(k):
        for h in range(pieces):
            take_row(k, h)

    def attend_row(k, d):
        wait_row(k, d)
        attend(row_slot(k, d), False)

    loads.sinks.wait()
    window(range(1, rows // WINDOW))
    win_copy(0).start()
    take_first(pieces - 1)
    queries_up()
    if n_z > 2:
        take_second(1, pieces // 2)
    pltpu.make_async_copy(wcol.at[core], wcol.at[core], s.w_sems.at[0]).wait()
    arrival(wcol.at[other], s.w_sems.at[2]).wait_recv()
    window_parts(0)
    take_rows(0)
    wait_column(0)
    attend(sp, True)
    if n_z > 2:
        take_second(pieces // 2, pieces - 1)

    @pl.when(x + 1 < n_x)
    def _():
        halo_copy.start()


    def take_pieces(k, lo, hi):
        @pl.when(z >= k)
        def _():
            for h in range(lo, hi):
                take_column(k, h)

    near = (x > 0) | (z == 0)

    def first_window():
        take_halo()
        window(range(1))
        win_copy(1).start()

    def last_parts():
        window_parts(1)

    def step(k, _):
        @pl.when(k == 4 - parity)
        def _():
            pair_forward()

        @pl.when(z >= k - 1)
        def _():
            wait_column(k - 1)
            attend(column_slot(k - 1), False)

        @pl.when(k == 2)
        def _():
            take_pieces(k, pieces - 1, pieces)

            @pl.when((x == 0) & (z + 1 < n_z))
            def _():
                arrival(turn, s.halo_sem.at[2]).wait_recv()
                relay_copy.start()

        pl.when((k == 4) & near)(last_parts)
        pl.when((k == 4) & ~near)(first_window)

        @pl.when(k > 2)
        def _():
            pl.when(x == 0)(functools.partial(take_pieces, k, 0, 1))
            take_pieces(k, 1, pieces // 2)

        @pl.when((z >= k - 1) & (k == n_z))
        def _():
            take_rows(k - 1)

        pl.when((k == 4) & ~near)(last_parts)

        for d in range(1, n_x):
            @pl.when((z >= k - 2) & takes_row(k - 2, d))
            def _():
                attend_row(k - 2, d)


        @pl.when(k > 2)
        def _():
            take_pieces(k, pieces // 2, pieces - 1)

        pl.when((k == 3) & near)(first_window)

        @pl.when(k > 2)
        def _():
            take_pieces(k, pieces - 1, pieces)


        @pl.when((z >= k - 1) & (k != n_z))
        def _():
            take_rows(k - 1)

        @pl.when(x > 0)
        def _():
            take_pieces(k + 1, 0, 1)

        return 0

    lax.fori_loop(2, max(n_z, 3) + 2, step, 0)


    def gather(part):
        own = lat.at[tp, part]
        sends = [
            remote(own, own, s.y_send.at[d - 1], s.y_recv.at[part, d - 1],
                   {"sp": sp, "tp": lax.rem(y + d, n_y) * 2 + core})
            for d in range(1, n_y)
        ]
        sends.append(remote(own, own, s.s_send.at[0], s.s_recv.at[part], to_sibling))
        return sends

    def forward(part):
        for d in range(1, n_y):
            ref = lat.at[lax.rem(y + n_y - d, n_y) * 2 + core, part]
            arrival(ref, s.y_recv.at[part, d - 1]).wait_recv()
            remote(ref, ref, s.s_send.at[d], s.s_recv.at[part], to_sibling).start()

    def arrived(part):
        arrival(lat.at[pl.ds(0, n_y), part], s.s_recv.at[part]).wait_recv()

    for part in range(out_parts):
        at = slice(part * out_rows, (part + 1) * out_rows)
        for h in range(lat_heads):
            lat[tp, part, :, h * VDIM : (h + 1) * VDIM] = (
                acc[h, :, at] / total[h, :, at]).T.astype(BF16)
        start(gather(part))
    gate(0)
    gate(1)
    window_branch = window_part(y, pl.ds(0, rows))
    for d in range(1, n_y):
        arrival(precv.at[d - 1], s.p_recv.at[d - 1]).wait_recv()
        window_branch = window_branch + precv[d - 1].astype(F32)
    gates[0] = gates[0] * window_branch
    column_local.wait()
    arrival(columns.at[sibling], s.col_recv.at[0]).wait_recv()
    for d in range(1, n_y):
        base = lax.rem(y + n_y - d, n_y) * 2
        if paired:
            arrival(columns.at[base + 1 - parity], s.pair_recv.at[d - 1]).wait_recv()
        else:
            arrival(columns.at[pl.ds(base, 2)], s.col_recv.at[d]).wait_recv()
    for part in range(out_parts):
        at = slice(part * out_rows, (part + 1) * out_rows)
        forward(part)
        arrived(part)
        latent_branch = jnp.zeros((out_rows, block), F32)
        for j in range(n_tp):
            latent_branch = latent_branch + dot(lat[j, part], columns[j])
        out[at, :] = (gates[0, at] + gates[1, at] * latent_branch).astype(BF16)

    def leave(ref, send):
        remote(ref, ref, send, send, to_sibling).wait_send()

    leave(ownf.at[pl.ds(0, half)], s.f_send.at[0])
    for d in range(1, n_y):
        leave(ownf, s.f_send.at[d])
    leave(normed.at[core], s.n_sems.at[0])
    latq_copy.wait_send()
    leave(wcol.at[core], s.w_sems.at[1])
    leave(columns.at[tp], s.col_send.at[0])

    @when_across
    def _():
        for d in range(1, n_y):
            leave(columns.at[pl.ds(0, 2)], s.col_send.at[d])

    if paired:
        for d in range(1, n_y):
            pair_copy(d).wait_send()
    for i in range(2):
        win_copy(i).wait_send()
    for d in range(1, n_y):
        leave(psend.at[d - 1], s.p_send.at[d - 1])
        leave(lat.at[tp], s.y_send.at[d - 1])
        leave(lat.at[tp], s.s_send.at[d])
    leave(lat.at[tp], s.s_send.at[0])

    @pl.when((x + 1 < n_x) | (z + 1 < n_z))
    def _():
        halo_copy.wait_send()

    @pl.when((x == 0) & (z + 1 < n_z))
    def _():
        relay_copy.wait_send()

    def drain(k, _):
        @pl.when(z >= k)
        def _():
            own = kvb.at[column_slot(k), core]

            @pl.when(z + 1 < n_z)
            def _():
                leave(own, s.z_send.at[k])

            leave(own, s.c_send.at[k])
            for d in range(1, n_x):
                to = lax.rem(x + d, n_x)
                fewer = [detoured(k, h, to) for h in DETOURS]

                @pl.when(sends_row(k, d) & ~(fewer[0] | fewer[1]))
                def _():
                    leave(own, s.x_send.at[k, d - 1])

                @pl.when(fewer[0] | fewer[1])
                def _():
                    leave(own.at[pl.ds(0, pieces - 1)], s.x_send.at[k, d - 1])

                for i in range(2):
                    @pl.when(takes_row(k, d) & passes_detour(k, i))
                    def _():
                        detour_copy(k, d, i).wait_send()

                @pl.when(takes_row(k, d))
                def _():
                    leave(own, s.d_send.at[k, d - 1])

        return 0

    lax.fori_loop(0, n_z, drain, 0)


def on_device(dims, features, norm_gain, w_query, w_key, w_value, head_sinks, w_query_latent,
              w_kv_latent, w_rope_key, query_latent_gain, kv_latent_gain, w_query_content,
              w_query_rotary, w_key_up, w_value_up, w_branch_window, w_branch_latent,
              w_gate_window, w_gate_latent):
    n_sp, n_tp, n_x = dims
    n_z, n_y = n_sp // n_x, n_tp // 2
    rows, block = features.shape
    width = norm_gain.shape[0]
    latent = w_kv_latent.shape[1]
    lat_heads = w_key_up.shape[1] // NOPE
    half_width = ROPE // 2
    entry = np.arange(ROPE, dtype=np.int32) % half_width
    frequency = (np.float32(THETA) ** (-entry.astype(np.float32) / np.float32(half_width))).astype(np.float32)[None, :]
    weights = (w_kv_latent, w_rope_key.T, w_key, w_value, w_query, w_query_latent, w_query_content,
               w_query_rotary, w_key_up, w_value_up, w_gate_window, w_gate_latent)
    smalls = (norm_gain[None, :], head_sinks[None, :], query_latent_gain[None, :], kv_latent_gain[None, :],
              jnp.asarray(frequency))
    branch_rows = w_branch_window.shape[0]
    pieces = PIECES
    piece = rows // 2 // pieces
    out_parts = rows // LANES
    merge = w_key.shape[1] % LANES == 0
    hbm = pl.BlockSpec(memory_space=pl.ANY)
    dma = pltpu.SemaphoreType.DMA
    vm = pltpu.VMEM
    scratch = dict(
        **{"small_" + n: (pltpu.SMEM if n == "sinks" else vm)(a.shape, F32) for n, a in zip(SMALL, smalls)},
        **{"w_" + n: vm(a.shape, BF16) for n, a in zip(WEIGHTS, weights) if not (merge and n in MERGED)},
        **(dict(w_qkv=vm((width, 2 * w_key.shape[1] + w_query.shape[1]), BF16)) if merge else {}),
        ownf=vm((rows, block), BF16),
        feat=vm((n_tp, rows // 2, block), BF16),
        normed=vm((2, pieces, piece, width), BF16),
        latq=vm((2, rows // 2, latent), BF16),
        wcol=vm((2, n_y, branch_rows, block), BF16),
        columns=vm((n_tp, w_branch_latent.shape[0], block), BF16),
        psend=vm((n_y - 1, rows, block), BF16),
        precv=vm((n_y - 1, rows, block), BF16),
        kvb=vm((n_sp, 2, pieces, piece + SUBLANES, latent), BF16),
        local_kv=vm((rows, 2 * w_key.shape[1]), BF16),
        halo=vm((WINDOW, 2 * w_key.shape[1]), BF16),
        turn=vm((WINDOW, 2 * w_key.shape[1]), BF16),
        queries=vm((rows, w_query.shape[1]), BF16),
        q_full=vm((lat_heads, NOPE + LANES, rows), BF16),
        gates=vm((2, rows, block), F32),
        winb=vm((2, rows, w_query.shape[1]), BF16),
        lat=vm((n_tp, out_parts, rows // out_parts, lat_heads * VDIM), BF16),
        top=vm((lat_heads, 1, rows), F32),
        total=vm((lat_heads, 1, rows), F32),
        acc=vm((lat_heads, VDIM, rows), F32),
        cosine=vm((2, pieces, piece, ROPE), F32),
        sine=vm((2, pieces, piece, ROPE), F32),
        own_sem=dma((2,)),
        small_sem=dma((len(SMALL),)),
        w_sem=dma((len(weights),)),
        f_send=dma((n_y,)),
        f_recv=dma((pieces,)),
        n_sems=dma((2,)),
        q_sems=dma((2,)),
        w_sems=dma((3,)),
        col_own=dma((1,)),
        col_send=dma((n_y,)),
        col_recv=dma((n_y,)),
        pair_send=dma((n_y - 1,)),
        pair_recv=dma((n_y - 1,)),
        halo_sem=dma((4,)),
        win_send=dma((2,)),
        win_recv=dma((2,)),
        p_send=dma((n_y - 1,)),
        p_recv=dma((n_y - 1,)),
        y_send=dma((n_y - 1,)),
        y_recv=dma((out_parts, n_y - 1)),
        s_send=dma((n_y,)),
        s_recv=dma((out_parts,)),
        z_send=dma((n_z - 1,)),
        z_recv=dma((pieces, n_z - 1)),
        r_send=dma((2, n_z - 2, n_x - 1)),
        r_recv=dma((2, n_z - 2, n_x - 1)),
        x_send=dma((n_z, n_x - 1)),
        x_recv=dma((pieces, n_z, n_x - 1)),
        c_send=dma((n_z,)),
        c_recv=dma((n_z,)),
        d_send=dma((n_z, n_x - 1)),
        d_recv=dma((n_z, n_x - 1)),
    )
    return pl.pallas_call(
        functools.partial(kernel, dims, tuple(scratch)),
        out_shape=pltpu.VMEM((rows, block), BF16),
        in_specs=[hbm] * (1 + len(smalls) + len(weights) + 2),
        out_specs=pl.BlockSpec(memory_space=pltpu.VMEM),
        scratch_shapes=list(scratch.values()),
        compiler_params=pltpu.CompilerParams(
            collective_id=0, has_side_effects=True, vmem_limit_bytes=60 * 1024 * 1024
        ),
    )(features, *smalls, *weights, w_branch_window, w_branch_latent)


def solution(mesh):
    n_sp, n_tp = mesh.shape["sp"], mesh.shape["tp"]
    n_x = 1
    while n_sp % (2 * n_x) == 0 and 8 * n_x * n_x <= n_sp:
        n_x *= 2
    return jax.shard_map(
        functools.partial(on_device, (n_sp, n_tp, n_x)),
        mesh=mesh,
        in_specs=(
            P("sp", "tp"),
            P(),
            P(None, "tp"),
            P(None, "tp"),
            P(None, "tp"),
            P("tp"),
            P(),
            P(),
            P(),
            P(),
            P(),
            P(None, "tp"),
            P(None, "tp"),
            P(None, "tp"),
            P(None, "tp"),
            P("tp", None),
            P("tp", None),
            P(None, "tp"),
            P(None, "tp"),
        ),
        out_specs=P("sp", "tp"),
        check_vma=False,
    )
```

```python
import functools
import types

import jax
import jax.numpy as jnp
import numpy as np
from jax import lax
from jax.experimental import pallas as pl
from jax.experimental.pallas import tpu as pltpu
from jax.sharding import PartitionSpec as P

HEAD = 64
WINDOW = 128
NOPE = 128
ROPE = 64
VDIM = 128


EPS = 1e-06
THETA = 10000.0
NEGATIVE = -1e30
LANES = 128
LOG2_E = 1.4426950408889634
MESH = pl.DeviceIdType.MESH
BF16 = jnp.bfloat16
F32 = jnp.float32
PIECES = 4
SUBLANES = 8
DETOURS = (0, PIECES - 1)


def dot(left, right):
    return jnp.dot(left, right, preferred_element_type=F32)


def dot_t(left, right):
    return lax.dot_general(left, right, (((1,), (1,)), ((), ())), preferred_element_type=F32)


def dot_tl(left, right):
    return lax.dot_general(left, right, (((0,), (0,)), ((), ())), preferred_element_type=F32)


def rms_rows(rows, gain):
    return rows * lax.rsqrt(jnp.mean(rows * rows, axis=-1, keepdims=True) + EPS) * gain


def swap_halves(rows):
    half = rows.shape[1] // 2
    return jnp.concatenate([rows[:, half:], rows[:, :half]], axis=1)


SMALL = ("norm_gain", "sinks", "q_gain", "kv_gain", "frequency")
WEIGHTS = (
    "kv_latent", "rope", "key", "value", "query", "query_latent", "content", "rotary",
    "key_up", "value_up", "gate_window", "gate_latent",
)
def bundle(names, values):
    return types.SimpleNamespace(**dict(zip(names, values)))


MERGED = ("key", "value", "query")


def kernel(dims, names, *refs):
    n_sp, n_tp, n_x = dims
    n_z, n_y = n_sp // n_x, n_tp // 2
    features = refs[0]
    small_hbm = bundle(SMALL, refs[1:6])
    w_hbm = bundle(WEIGHTS, refs[6:18])
    window_hbm, latent_hbm = refs[18:20]
    out = refs[20]
    s = bundle(names, refs[21:])
    small = bundle(SMALL, [getattr(s, "small_" + name) for name in SMALL])
    merged = "w_qkv" in names
    kept = [name for name in WEIGHTS if "w_" + name in names]
    w = bundle(kept, [getattr(s, "w_" + name) for name in kept])
    ownf, feat, normed = s.ownf, s.feat, s.normed
    turn = s.turn
    kvb, local_kv, halo, queries, q_full, latq = s.kvb, s.local_kv, s.halo, s.queries, s.q_full, s.latq
    gates, winb, lat, top, total, acc = s.gates, s.winb, s.lat, s.top, s.total, s.acc
    wcol, columns, psend, precv = s.wcol, s.columns, s.psend, s.precv
    cosine, sine = s.cosine, s.sine

    sp, tp = lax.axis_index("sp"), lax.axis_index("tp")
    z, x = sp // n_x, lax.rem(sp, n_x)
    y, core = tp // 2, lax.rem(tp, 2)
    other = 1 - core
    sibling = y * 2 + other
    rows, block = features.shape
    half = rows // 2
    pieces = normed.shape[1]
    piece = half // pieces
    lat_heads = w_hbm.key_up.shape[1] // NOPE
    kv_width = w_hbm.key.shape[1]
    kv_heads = kv_width // HEAD
    group = w_hbm.query.shape[1] // kv_width
    latent = w_hbm.kv_latent.shape[1]
    out_parts = lat.shape[1]
    out_rows = rows // out_parts

    def remote(src, dst, send, recv, where):
        return pltpu.make_async_remote_copy(
            src_ref=src, dst_ref=dst, send_sem=send, recv_sem=recv,
            device_id=where, device_id_type=MESH,
        )

    to_sibling = {"sp": sp, "tp": sibling}

    def arrival(ref, recv):
        return remote(ref, ref, recv, recv, to_sibling)

    def start(copies):
        for copy in copies:
            copy.start()

    def own_rows(c, h):
        return ownf.at[pl.ds(pl.multiple_of(c * half + h * piece, 16), piece)]

    def feat_rows(j, h):
        return feat.at[j, pl.ds(h * piece, piece)]

    own_load = [
        pltpu.make_async_copy(features, ownf, s.own_sem.at[0]),
        pltpu.make_async_copy(
            features.at[pl.ds(pl.multiple_of(core * half, 16), half)], feat.at[tp], s.own_sem.at[1]),
    ]
    start(own_load)
    loads = bundle(SMALL, [
        pltpu.make_async_copy(getattr(small_hbm, name), getattr(small, name), s.small_sem.at[i])
        for i, name in enumerate(SMALL)
    ])
    for name in SMALL:
        getattr(loads, name).start()

    barrier = pltpu.get_barrier_semaphore()

    def greet(where):
        pl.semaphore_signal(barrier, inc=1, device_id=where, device_id_type=MESH)

    for d in range(1, n_tp):
        greet({"sp": sp, "tp": lax.rem(tp + d, n_tp)})
    for d in range(1, n_x):
        greet({"sp": z * n_x + lax.rem(x + d, n_x), "tp": tp})

    @pl.when(z + 1 < n_z)
    def _():
        greet({"sp": sp + n_x, "tp": tp})

    @pl.when(z > 0)
    def _():
        greet({"sp": sp - n_x, "tp": tp})

    one, none = jnp.int32(1), jnp.int32(0)
    pl.semaphore_wait(
        barrier,
        n_tp - 1 + n_x - 1
        + jnp.where(z + 1 < n_z, one, none) + jnp.where(z > 0, one, none),
    )

    def feature_sends(h):
        sends = []
        for d in range(1, n_y):
            for c in range(2):
                sends.append(remote(
                    own_rows(c, h), feat_rows(tp, h), s.sent.at[0], s.f_recv.at[h],
                    {"sp": sp, "tp": lax.rem(y + d, n_y) * 2 + c}))
        sends.append(remote(
            own_rows(other, h), feat_rows(tp, h), s.sent.at[0], s.f_recv.at[h], to_sibling))
        return sends

    def feature_wait(h):
        arrival(feat.at[pl.ds(0, n_tp - 1), pl.ds(h * piece, piece)], s.f_recv.at[h]).wait_recv()

    for copy in own_load:
        copy.wait()
    for h in range(pieces):
        start(feature_sends(h))

    first = 0
    for i, name in enumerate(WEIGHTS):
        source = getattr(w_hbm, name)
        if name in kept:
            to = getattr(w, name)
        else:
            to = s.w_qkv.at[:, pl.ds(first, source.shape[1])]
            first += source.shape[1]
        copy = pltpu.make_async_copy(source, to, s.w_sem.at[i])
        copy.start()
        setattr(loads, name, copy)

    def window_columns():
        local, sends = [], []
        for j in range(n_y):
            local.append(pltpu.make_async_copy(
                window_hbm.at[:, pl.ds(pl.multiple_of((j * 2 + core) * block, LANES), block)],
                wcol.at[core, j], s.w_sems.at[0]))
            sends.append(remote(
                window_hbm.at[:, pl.ds(pl.multiple_of((j * 2 + other) * block, LANES), block)],
                wcol.at[core, j], s.sent.at[0], s.w_sems.at[1], to_sibling))
        return local, sends

    paired = n_z % 2 == 0
    parity = lax.rem(z, 2)
    partner = {"sp": sp + n_x * (1 - 2 * parity), "tp": tp}

    def column_send(to, d):
        return remote(
            latent_hbm.at[:, pl.ds(pl.multiple_of(to * block, LANES), block)],
            columns.at[tp], s.sent.at[0], s.col_recv.at[d], {"sp": sp, "tp": to})

    def when_across(act):
        if paired:
            pl.when(core == parity)(act)
        else:
            act()

    def column_start():
        column_send(sibling, 0).start()

        @when_across
        def _():
            for d in range(1, n_y):
                for c in range(2):
                    column_send(lax.rem(y + d, n_y) * 2 + c, d).start()

    def pair_copy(d):
        ref = columns.at[lax.rem(y + n_y - d, n_y) * 2 + parity]
        return remote(ref, ref, s.sent.at[0], s.pair_recv.at[d - 1], partner)

    def pair_forward():
        if paired:
            for d in range(1, n_y):
                source = lax.rem(y + n_y - d, n_y) * 2 + parity
                arrival(columns.at[source], s.col_recv.at[d]).wait_recv()
                pair_copy(d).start()

    column_local = pltpu.make_async_copy(
        latent_hbm.at[:, pl.ds(pl.multiple_of(tp * block, LANES), block)],
        columns.at[tp], s.col_own.at[0])

    wcol_local, wcol_sends = window_columns()

    loads.frequency.wait()
    positions = (sp * rows + lax.broadcasted_iota(jnp.int32, (rows, ROPE), 0)).astype(F32)
    angles = positions * small.frequency[...]
    lane = lax.broadcasted_iota(jnp.int32, (rows, ROPE), 1)
    cosine[...] = jnp.cos(angles).reshape(cosine.shape)
    turned = jnp.sin(angles)
    sine[...] = jnp.where(lane < ROPE // 2, -turned, turned).reshape(sine.shape)

    def normalize(h):
        squares = jnp.zeros((piece, 1), F32)
        part = slice(h * piece, (h + 1) * piece)
        for j in range(n_tp):
            values = feat[j, part].astype(F32)
            squares = squares + jnp.sum(values * values, axis=-1, keepdims=True)
        scale = lax.rsqrt(squares / (n_tp * block) + EPS)
        for j in range(n_tp):
            span = slice(j * block, (j + 1) * block)
            values = feat[j, part].astype(F32) * scale * small.norm_gain[:, span]
            normed[core, h, :, span] = values.astype(BF16)

    def normed_copy(h):
        return remote(normed.at[core, h], normed.at[core, h], s.sent.at[0], s.n_sems.at[0], to_sibling)

    def latents(h):
        own = normed[core, h]
        rope = dot_t(own, w.rope[...])
        rope = rope * cosine[core, h] + swap_halves(rope) * sine[core, h]
        rope = jnp.concatenate([rope[: piece // 2], rope[piece // 2 :]], axis=1)
        rope = [rope[i : i + SUBLANES] for i in range(0, piece // 2, SUBLANES)]
        rope.append(jnp.zeros((SUBLANES, latent - len(rope) * LANES), F32))
        kvb[sp, core, h, :piece, :] = rms_rows(dot(own, w.kv_latent[...]), small.kv_gain[...]).astype(BF16)
        kvb[sp, core, h, piece:, :] = jnp.concatenate(rope, axis=1).astype(BF16)

    def rope_rows(slot, halves=range(2)):
        parts = []
        for c in halves:
            for h in range(pieces):
                packed = kvb[slot, c, h, piece:, :].astype(F32)
                pair = jnp.concatenate(
                    [packed[:, i * LANES : (i + 1) * LANES] for i in range(piece // 2 // SUBLANES)], axis=0)
                parts += [pair, pltpu.roll(pair, ROPE, 1)]
        return jnp.concatenate(parts, axis=0).astype(BF16)

    def column_slot(k):
        return (z - k) * n_x + x

    def row_slot(k, d):
        return (z - k) * n_x + lax.rem(x + n_x - d, n_x)

    def z_copy(k, h):
        ref = kvb.at[column_slot(k), core, h]
        return remote(ref, ref, s.sent.at[0], s.z_recv.at[h, k], {"sp": sp + n_x, "tp": tp})

    def x_copy(k, d, h):
        ref = kvb.at[column_slot(k), core, h]
        return remote(ref, ref, s.sent.at[0], s.x_recv.at[h, k, d - 1],
                      {"sp": z * n_x + lax.rem(x + d, n_x), "tp": tp})

    def c_copy(k, h):
        ref = kvb.at[column_slot(k), core, h]
        return remote(ref, ref, s.sent.at[0], s.c_recv.at[k], to_sibling)

    def d_copy(k, d, h):
        ref = kvb.at[row_slot(k, d), core, h]
        return remote(ref, ref, s.sent.at[0], s.d_recv.at[k, d - 1], to_sibling)

    def wait_column(k):
        arrival(kvb.at[column_slot(k), other], s.c_recv.at[k]).wait_recv()

    def wait_row(k, d):
        arrival(kvb.at[row_slot(k, d), other], s.d_recv.at[k, d - 1]).wait_recv()

    def sends_row(k, d):
        return (k > 0) | (x + d < n_x)

    def takes_row(k, d):
        return (k > 0) | (x >= d)

    def detoured(k, h, to):
        if h == DETOURS[0]:
            return (k >= 2) & (to > 0)
        return (k >= 3) & (to == 0)

    def pass_on(k, h):
        @pl.when(z + 1 < n_z)
        def _():
            z_copy(k, h).start()

        for d in range(1, n_x):
            to = lax.rem(x + d, n_x)

            @pl.when(sends_row(k, d) & ~detoured(k, h, to) if h in DETOURS else sends_row(k, d))
            def _():
                x_copy(k, d, h).start()

        c_copy(k, h).start()

    def take_column(k, h):
        arrival(kvb.at[column_slot(k), core, h], s.z_recv.at[h, k - 1]).wait_recv()
        pass_on(k, h)

    def detour_copy(k, d, i):
        ref = kvb.at[row_slot(k, d), core, DETOURS[i]]
        return remote(ref, ref, s.sent.at[0], s.r_recv.at[i, k - 1, d - 1], {"sp": sp + n_x, "tp": tp})

    def passes_detour(k, i):
        return (z + 1 < n_z) & detoured(k + 1, DETOURS[i], x)

    def take_row(k, h):
        for d in range(1, n_x):
            def from_x():
                arrival(kvb.at[row_slot(k, d), core, h], s.x_recv.at[h, k, d - 1]).wait_recv()

            def from_z():
                arrival(kvb.at[row_slot(k, d), core, h], s.r_recv.at[DETOURS.index(h), k - 2, d - 1]).wait_recv()

            @pl.when(takes_row(k, d))
            def _():
                if h in DETOURS:
                    pl.when(~detoured(k, h, x))(from_x)
                    pl.when(detoured(k, h, x))(from_z)

                    @pl.when(passes_detour(k, DETOURS.index(h)))
                    def _():
                        detour_copy(k, d, DETOURS.index(h)).start()
                else:
                    from_x()
                d_copy(k, d, h).start()

    def take_second(lo, hi):
        for h in range(lo, hi):
            @pl.when(z >= 2)
            def _():
                take_column(2, h)

    def take_first(h):
        @pl.when(z >= 1)
        def _():
            take_column(1, h)

    start(wcol_local)
    start(wcol_sends)
    column_local.start()
    for name in ("norm_gain", "kv_gain", "kv_latent", "rope"):
        getattr(loads, name).wait()
    for h in range(pieces):
        feature_wait(h)
        if h == pieces - 1:
            column_start()
        normalize(h)
        normed_copy(h).start()
        latents(h)
        pass_on(0, h)
        if 1 <= h <= pieces // 2:
            take_first(h - 1)

    loads.query_latent.wait()
    loads.q_gain.wait()
    own_normed = normed[core].reshape(half, n_tp * block)
    latq[core] = rms_rows(dot(own_normed, w.query_latent[...]), small.q_gain[...]).astype(BF16)
    latq_copy = remote(latq.at[core], latq.at[core], s.sent.at[0], s.q_sems.at[0], to_sibling)
    latq_copy.start()

    arrival(normed.at[other], s.n_sems.at[0]).wait_recv()

    if n_z > 2:
        take_second(0, 1)

    def all_normed():
        return normed[...].reshape(rows, n_tp * block)

    for name in MERGED:
        getattr(loads, name).wait()
    if merged:
        qkv = dot(all_normed(), s.w_qkv[...]).astype(BF16)
    else:
        qkv = jnp.concatenate([dot(all_normed(), getattr(w, name)[...]) for name in MERGED], axis=1).astype(BF16)
    local_kv[...] = qkv[:, : 2 * kv_width]
    queries[...] = qkv[:, 2 * kv_width :]
    tail = local_kv.at[pl.ds(rows - WINDOW, WINDOW)]
    halo_copy = remote(tail, halo, s.sent.at[0], s.halo_sem.at[0], {"sp": sp + 1, "tp": tp})
    turn_copy = remote(tail, turn, s.sent.at[0], s.halo_sem.at[1], {"sp": z * n_x, "tp": tp})
    relay_copy = remote(turn, halo, s.sent.at[0], s.halo_sem.at[0], {"sp": sp + n_x, "tp": tp})

    @pl.when((x + 1 == n_x) & (z + 1 < n_z))
    def _():
        turn_copy.start()

    take_first(pieces - 2)

    def queries_up():
        arrival(latq.at[other], s.q_sems.at[0]).wait_recv()
        loads.content.wait()
        loads.rotary.wait()
        latent_query = latq[...].reshape(rows, latent)
        content = dot(latent_query, w.content[...])
        rotary = dot(latent_query, w.rotary[...])
        cos_all, sin_all = cosine[...].reshape(rows, ROPE), sine[...].reshape(rows, ROPE)
        padding = jnp.zeros((rows, LANES - ROPE), F32)
        for h in range(lat_heads):
            turned = rotary[:, h * ROPE : (h + 1) * ROPE]
            turned = turned * cos_all + swap_halves(turned) * sin_all
            q_full[h, :NOPE, :] = content[:, h * NOPE : (h + 1) * NOPE].T.astype(BF16)
            q_full[h, NOPE:, :] = jnp.concatenate([turned, padding], axis=1).T.astype(BF16)
        loads.key_up.wait()
        loads.value_up.wait()

    def attend(slot, diagonal, which=None):
        if which is None:
            source = kvb[slot, :, :, :piece, :].reshape(rows, latent)
            rope_part = rope_rows(slot)
        else:
            source = kvb[slot, which, :, :piece, :].reshape(half, latent)
            rope_part = rope_rows(slot, [which])
        keys = dot(source, w.key_up[...]).astype(BF16)
        values = dot(source, w.value_up[...]).astype(BF16)
        heads = range(lat_heads)
        scores = []
        for h in heads:
            key = jnp.concatenate([keys[:, h * NOPE : (h + 1) * NOPE], rope_part], axis=1)
            scores.append(dot(key, q_full[h]) * ((NOPE + ROPE) ** (-0.5) * LOG2_E))
        if diagonal:
            live = (lax.broadcasted_iota(jnp.int32, (rows, rows), 0)
                    <= lax.broadcasted_iota(jnp.int32, (rows, rows), 1))
            scores = [jnp.where(live, part, NEGATIVE) for part in scores]
        weights, fades = [], []
        for h in heads:
            peak = jnp.max(scores[h], axis=0, keepdims=True)
            if not diagonal:
                before = top[h]
                peak = jnp.maximum(peak, before)
                fades.append(jnp.exp2(before - peak))
            top[h] = peak
            weights.append(jnp.exp2(scores[h] - peak))
        for h in heads:
            weight_sum = jnp.sum(weights[h], axis=0, keepdims=True)
            part = dot_tl(values[:, h * VDIM : (h + 1) * VDIM], weights[h].astype(BF16))
            if not diagonal:
                weight_sum = total[h] * fades[h] + weight_sum
                part = acc[h] * fades[h] + part
            total[h] = weight_sum
            acc[h] = part

    def take_halo():
        @pl.when(sp > 0)
        def _():
            arrival(halo, s.halo_sem.at[0]).wait_recv()

        @pl.when(sp == 0)
        def _():
            halo[...] = jnp.zeros(halo.shape, BF16)

    def window(blocks):
        row = lax.broadcasted_iota(jnp.int32, (2 * WINDOW, WINDOW), 1)
        column = lax.broadcasted_iota(jnp.int32, (2 * WINDOW, WINDOW), 0)
        offset = row + WINDOW - column
        in_band = (offset >= 0) & (offset < WINDOW)
        in_band = jnp.concatenate([in_band] * group, axis=1)
        later = jnp.concatenate([(sp > 0) | (column >= WINDOW)] * group, axis=1)
        units = [(n, g) for n in blocks for g in range(kv_heads)]
        scores, values, sinks, weights = [], [], [], []
        for n, g in units:
            at = slice(n * WINDOW, (n + 1) * WINDOW)
            earlier = halo[...] if n == 0 else local_kv[(n - 1) * WINDOW : n * WINDOW]
            band = jnp.concatenate([earlier, local_kv[at]], axis=0)
            valid = in_band & later if n == 0 else in_band
            key = band[:, g * HEAD : (g + 1) * HEAD]
            values.append(band[:, kv_width + g * HEAD : kv_width + (g + 1) * HEAD])
            members = range(g * group, (g + 1) * group)
            query = jnp.concatenate([queries[at, q * HEAD : (q + 1) * HEAD] for q in members], axis=0)
            sinks.append(jnp.concatenate([jnp.full((1, WINDOW), small.sinks[0, q], F32) for q in members], axis=1))
            scores.append(jnp.where(valid, dot_t(key, query) * HEAD ** (-0.5), NEGATIVE))
        for u in range(len(units)):
            peak = jnp.maximum(jnp.max(scores[u], axis=0, keepdims=True), sinks[u])
            part = jnp.exp(scores[u] - peak)
            bottom = jnp.sum(part, axis=0, keepdims=True) + jnp.exp(sinks[u] - peak)
            weights.append((part * (1.0 / bottom)).astype(BF16))
        mixed = [dot_tl(values[u], weights[u]) for u in range(len(units))]
        for b, n in enumerate(blocks):
            heads = [
                mixed[b * kv_heads + g][:, i * WINDOW : (i + 1) * WINDOW]
                for g in range(kv_heads) for i in range(group)
            ]
            winb[core, n * WINDOW : (n + 1) * WINDOW, :] = jnp.concatenate(heads, axis=0).T.astype(BF16)

    def win_copy(i):
        ref = winb.at[core, win_rows[i]]
        return remote(ref, ref, s.sent.at[0], s.win_recv.at[i], to_sibling)

    win_rows = (pl.ds(WINDOW, rows - WINDOW), pl.ds(0, WINDOW))

    def window_part(j, at):
        return dot(winb[0, at], wcol[0, j]) + dot(winb[1, at], wcol[1, j])

    def part_copy(d, at):
        return remote(psend.at[d - 1, at], precv.at[d - 1, at], s.sent.at[0], s.p_recv.at[d - 1],
                      {"sp": sp, "tp": lax.rem(y + d, n_y) * 2 + core})

    def window_parts(i):
        at = win_rows[i]
        arrival(winb.at[other, at], s.win_recv.at[i]).wait_recv()
        for d in range(1, n_y):
            psend[d - 1, at] = window_part(lax.rem(y + d, n_y), at).astype(BF16)
            part_copy(d, at).start()

    def gate(b):
        name = WEIGHTS[10 + b]
        getattr(loads, name).wait()

        def step(i, _):
            at = pl.ds(pl.multiple_of(i * 256, LANES), 256)
            gates[b, :, at] = jax.nn.sigmoid(dot(all_normed(), getattr(w, name)[:, at]))
            return 0

        lax.fori_loop(0, block // 256, step, 0)

    def take_rows(k):
        for h in range(pieces):
            take_row(k, h)

    def attend_row(k, d):
        wait_row(k, d)
        attend(row_slot(k, d), False)

    loads.sinks.wait()
    window(range(1, rows // WINDOW))
    win_copy(0).start()
    take_first(pieces - 1)
    queries_up()
    if n_z > 2:
        take_second(1, pieces // 2)
    pltpu.make_async_copy(wcol.at[core], wcol.at[core], s.w_sems.at[0]).wait()
    arrival(wcol.at[other], s.w_sems.at[1]).wait_recv()
    window_parts(0)
    take_rows(0)
    wait_column(0)
    attend(sp, True)
    if n_z > 2:
        take_second(pieces // 2, pieces - 1)

    @pl.when(x + 1 < n_x)
    def _():
        halo_copy.start()

    @pl.when((x == 0) & (z + 1 < n_z))
    def _():
        arrival(turn, s.halo_sem.at[1]).wait_recv()
        relay_copy.start()


    def take_pieces(k, lo, hi):
        @pl.when(z >= k)
        def _():
            for h in range(lo, hi):
                take_column(k, h)

    def first_window():
        take_halo()
        window(range(1))
        win_copy(1).start()

    def last_parts():
        window_parts(1)

    def step(k, _):
        @pl.when(k == 4 - parity)
        def _():
            pair_forward()

        @pl.when(z >= k - 1)
        def _():
            wait_column(k - 1)
            attend(column_slot(k - 1), False)

        @pl.when(k == 2)
        def _():
            take_pieces(k, pieces - 1, pieces)

        pl.when(k == 4)(last_parts)

        @pl.when(k > 2)
        def _():
            pl.when(x == 0)(functools.partial(take_pieces, k, 0, 1))
            take_pieces(k, 1, pieces // 2)

        for d in range(1, n_x):
            @pl.when((z >= k - 2) & takes_row(k - 2, d) & (k <= n_z))
            def _():
                attend_row(k - 2, d)

            @pl.when((z >= k - 2) & (k == n_z + 1))
            def _():
                def halves(i, _):
                    @pl.when(i == 1)
                    def _():
                        wait_row(k - 2, d)

                    attend(row_slot(k - 2, d), False, jnp.where(i == 0, core, other))
                    return 0

                lax.fori_loop(0, 2, halves, 0)


        @pl.when(k > 2)
        def _():
            take_pieces(k, pieces // 2, pieces - 1)

        pl.when(k == 3)(first_window)

        @pl.when(k > 2)
        def _():
            take_pieces(k, pieces - 1, pieces)


        @pl.when(z >= k - 1)
        def _():
            take_rows(k - 1)

        @pl.when(x > 0)
        def _():
            take_pieces(k + 1, 0, 1)

        return 0

    lax.fori_loop(2, max(n_z, 3) + 2, step, 0)


    def gather(part):
        own = lat.at[tp, part]
        sends = [
            remote(own, own, s.sent.at[0], s.y_recv.at[part, d - 1],
                   {"sp": sp, "tp": lax.rem(y + d, n_y) * 2 + core})
            for d in range(1, n_y)
        ]
        sends.append(remote(own, own, s.sent.at[0], s.s_recv.at[part], to_sibling))
        return sends

    def forward(part):
        for d in range(1, n_y):
            ref = lat.at[lax.rem(y + n_y - d, n_y) * 2 + core, part]
            arrival(ref, s.y_recv.at[part, d - 1]).wait_recv()
            remote(ref, ref, s.sent.at[0], s.s_recv.at[part], to_sibling).start()

    def arrived(part):
        arrival(lat.at[pl.ds(0, n_y), part], s.s_recv.at[part]).wait_recv()

    for part in range(out_parts):
        at = slice(part * out_rows, (part + 1) * out_rows)
        for h in range(lat_heads):
            lat[tp, part, :, h * VDIM : (h + 1) * VDIM] = (
                acc[h, :, at] / total[h, :, at]).T.astype(BF16)
        start(gather(part))
    gate(0)
    gate(1)
    window_branch = window_part(y, pl.ds(0, rows))
    for d in range(1, n_y):
        arrival(precv.at[d - 1], s.p_recv.at[d - 1]).wait_recv()
        window_branch = window_branch + precv[d - 1].astype(F32)
    gates[0] = gates[0] * window_branch
    column_local.wait()
    arrival(columns.at[sibling], s.col_recv.at[0]).wait_recv()
    for d in range(1, n_y):
        base = lax.rem(y + n_y - d, n_y) * 2
        if paired:
            arrival(columns.at[base + 1 - parity], s.pair_recv.at[d - 1]).wait_recv()
        else:
            arrival(columns.at[pl.ds(base, 2)], s.col_recv.at[d]).wait_recv()
    for part in range(out_parts):
        at = slice(part * out_rows, (part + 1) * out_rows)
        forward(part)
        arrived(part)
        latent_branch = jnp.zeros((out_rows, block), F32)
        for j in range(n_tp):
            latent_branch = latent_branch + dot(lat[j, part], columns[j])
        out[at, :] = (gates[0, at] + gates[1, at] * latent_branch).astype(BF16)

    def leave(ref, send):
        remote(ref, ref, send, send, to_sibling).wait_send()

    leave(ownf.at[pl.ds(0, half)], s.sent.at[0])
    for d in range(1, n_y):
        leave(ownf, s.sent.at[0])
    leave(normed.at[core], s.sent.at[0])
    latq_copy.wait_send()
    leave(wcol.at[core], s.sent.at[0])
    leave(columns.at[tp], s.sent.at[0])

    @when_across
    def _():
        for d in range(1, n_y):
            leave(columns.at[pl.ds(0, 2)], s.sent.at[0])

    if paired:
        for d in range(1, n_y):
            pair_copy(d).wait_send()
    for i in range(2):
        win_copy(i).wait_send()
    for d in range(1, n_y):
        leave(psend.at[d - 1], s.sent.at[0])
        leave(lat.at[tp], s.sent.at[0])
        leave(lat.at[tp], s.sent.at[0])
    leave(lat.at[tp], s.sent.at[0])

    @pl.when((x + 1 < n_x) | (z + 1 < n_z))
    def _():
        halo_copy.wait_send()

    @pl.when((x == 0) & (z + 1 < n_z))
    def _():
        relay_copy.wait_send()

    def drain(k, _):
        @pl.when(z >= k)
        def _():
            own = kvb.at[column_slot(k), core]

            @pl.when(z + 1 < n_z)
            def _():
                leave(own, s.sent.at[0])

            leave(own, s.sent.at[0])
            for d in range(1, n_x):
                to = lax.rem(x + d, n_x)
                fewer = [detoured(k, h, to) for h in DETOURS]

                @pl.when(sends_row(k, d) & ~(fewer[0] | fewer[1]))
                def _():
                    leave(own, s.sent.at[0])

                @pl.when(fewer[0] | fewer[1])
                def _():
                    leave(own.at[pl.ds(0, pieces - 1)], s.sent.at[0])

                for i in range(2):
                    @pl.when(takes_row(k, d) & passes_detour(k, i))
                    def _():
                        detour_copy(k, d, i).wait_send()

                @pl.when(takes_row(k, d))
                def _():
                    leave(own, s.sent.at[0])

        return 0

    lax.fori_loop(0, n_z, drain, 0)


def on_device(dims, features, norm_gain, w_query, w_key, w_value, head_sinks, w_query_latent,
              w_kv_latent, w_rope_key, query_latent_gain, kv_latent_gain, w_query_content,
              w_query_rotary, w_key_up, w_value_up, w_branch_window, w_branch_latent,
              w_gate_window, w_gate_latent):
    n_sp, n_tp, n_x = dims
    n_z, n_y = n_sp // n_x, n_tp // 2
    rows, block = features.shape
    width = norm_gain.shape[0]
    latent = w_kv_latent.shape[1]
    lat_heads = w_key_up.shape[1] // NOPE
    half_width = ROPE // 2
    entry = np.arange(ROPE, dtype=np.int32) % half_width
    frequency = (np.float32(THETA) ** (-entry.astype(np.float32) / np.float32(half_width))).astype(np.float32)[None, :]
    weights = (w_kv_latent, w_rope_key.T, w_key, w_value, w_query, w_query_latent, w_query_content,
               w_query_rotary, w_key_up, w_value_up, w_gate_window, w_gate_latent)
    smalls = (norm_gain[None, :], head_sinks[None, :], query_latent_gain[None, :], kv_latent_gain[None, :],
              jnp.asarray(frequency))
    branch_rows = w_branch_window.shape[0]
    pieces = PIECES
    piece = rows // 2 // pieces
    out_parts = rows // LANES
    merge = w_key.shape[1] % LANES == 0
    hbm = pl.BlockSpec(memory_space=pl.ANY)
    dma = pltpu.SemaphoreType.DMA
    vm = pltpu.VMEM
    scratch = dict(
        **{"small_" + n: (pltpu.SMEM if n == "sinks" else vm)(a.shape, F32) for n, a in zip(SMALL, smalls)},
        **{"w_" + n: vm(a.shape, BF16) for n, a in zip(WEIGHTS, weights) if not (merge and n in MERGED)},
        **(dict(w_qkv=vm((width, 2 * w_key.shape[1] + w_query.shape[1]), BF16)) if merge else {}),
        ownf=vm((rows, block), BF16),
        feat=vm((n_tp, rows // 2, block), BF16),
        normed=vm((2, pieces, piece, width), BF16),
        latq=vm((2, rows // 2, latent), BF16),
        wcol=vm((2, n_y, branch_rows, block), BF16),
        columns=vm((n_tp, w_branch_latent.shape[0], block), BF16),
        psend=vm((n_y - 1, rows, block), BF16),
        precv=vm((n_y - 1, rows, block), BF16),
        kvb=vm((n_sp, 2, pieces, piece + SUBLANES, latent), BF16),
        local_kv=vm((rows, 2 * w_key.shape[1]), BF16),
        halo=vm((WINDOW, 2 * w_key.shape[1]), BF16),
        turn=vm((WINDOW, 2 * w_key.shape[1]), BF16),
        queries=vm((rows, w_query.shape[1]), BF16),
        q_full=vm((lat_heads, NOPE + LANES, rows), BF16),
        gates=vm((2, rows, block), F32),
        winb=vm((2, rows, w_query.shape[1]), BF16),
        lat=vm((n_tp, out_parts, rows // out_parts, lat_heads * VDIM), BF16),
        top=vm((lat_heads, 1, rows), F32),
        total=vm((lat_heads, 1, rows), F32),
        acc=vm((lat_heads, VDIM, rows), F32),
        cosine=vm((2, pieces, piece, ROPE), F32),
        sine=vm((2, pieces, piece, ROPE), F32),
        own_sem=dma((2,)),
        sent=dma((1,)),
        small_sem=dma((len(SMALL),)),
        w_sem=dma((len(weights),)),
        f_recv=dma((pieces,)),
        n_sems=dma((1,)),
        q_sems=dma((1,)),
        w_sems=dma((2,)),
        col_own=dma((1,)),
        col_recv=dma((n_y,)),
        pair_recv=dma((n_y - 1,)),
        halo_sem=dma((2,)),
        win_recv=dma((2,)),
        p_recv=dma((n_y - 1,)),
        y_recv=dma((out_parts, n_y - 1)),
        s_recv=dma((out_parts,)),
        z_recv=dma((pieces, n_z - 1)),
        r_recv=dma((2, n_z - 2, n_x - 1)),
        x_recv=dma((pieces, n_z, n_x - 1)),
        c_recv=dma((n_z,)),
        d_recv=dma((n_z, n_x - 1)),
    )
    return pl.pallas_call(
        functools.partial(kernel, dims, tuple(scratch)),
        out_shape=pltpu.VMEM((rows, block), BF16),
        in_specs=[hbm] * (1 + len(smalls) + len(weights) + 2),
        out_specs=pl.BlockSpec(memory_space=pltpu.VMEM),
        scratch_shapes=list(scratch.values()),
        compiler_params=pltpu.CompilerParams(
            collective_id=0, has_side_effects=True, vmem_limit_bytes=60 * 1024 * 1024
        ),
    )(features, *smalls, *weights, w_branch_window, w_branch_latent)


def solution(mesh):
    n_sp, n_tp = mesh.shape["sp"], mesh.shape["tp"]
    n_x = 1
    while n_sp % (2 * n_x) == 0 and 8 * n_x * n_x <= n_sp:
        n_x *= 2
    return jax.shard_map(
        functools.partial(on_device, (n_sp, n_tp, n_x)),
        mesh=mesh,
        in_specs=(
            P("sp", "tp"),
            P(),
            P(None, "tp"),
            P(None, "tp"),
            P(None, "tp"),
            P("tp"),
            P(),
            P(),
            P(),
            P(),
            P(),
            P(None, "tp"),
            P(None, "tp"),
            P(None, "tp"),
            P(None, "tp"),
            P("tp", None),
            P("tp", None),
            P(None, "tp"),
            P(None, "tp"),
        ),
        out_specs=P("sp", "tp"),
        check_vma=False,
    )
```

```python
import functools
import types

import jax
import jax.numpy as jnp
import numpy as np
from jax import lax
from jax.experimental import pallas as pl
from jax.experimental.pallas import tpu as pltpu
from jax.sharding import PartitionSpec as P

HEAD = 64
WINDOW = 128
NOPE = 128
ROPE = 64
VDIM = 128


EPS = 1e-06
THETA = 10000.0
NEGATIVE = -1e30
LANES = 128
LOG2_E = 1.4426950408889634
MESH = pl.DeviceIdType.MESH
BF16 = jnp.bfloat16
F32 = jnp.float32
PIECES = 4
SUBLANES = 8
DETOURS = (0, PIECES - 1)


def dot(left, right):
    return jnp.dot(left, right, preferred_element_type=F32)


def dot_t(left, right):
    return lax.dot_general(left, right, (((1,), (1,)), ((), ())), preferred_element_type=F32)


def dot_tl(left, right):
    return lax.dot_general(left, right, (((0,), (0,)), ((), ())), preferred_element_type=F32)


def rms_rows(rows, gain):
    return rows * lax.rsqrt(jnp.mean(rows * rows, axis=-1, keepdims=True) + EPS) * gain


def swap_halves(rows):
    half = rows.shape[1] // 2
    return jnp.concatenate([rows[:, half:], rows[:, :half]], axis=1)


SMALL = ("norm_gain", "sinks", "q_gain", "kv_gain", "frequency")
WEIGHTS = (
    "kv_latent", "rope", "key", "value", "query", "query_latent", "content", "rotary",
    "key_up", "value_up", "gate_window", "gate_latent",
)
def bundle(names, values):
    return types.SimpleNamespace(**dict(zip(names, values)))


UP = ("key_up", "value_up")
MERGED = ("key", "value", "query")


def kernel(dims, names, *refs):
    n_sp, n_tp, n_x = dims
    n_z, n_y = n_sp // n_x, n_tp // 2
    features = refs[0]
    small_hbm = bundle(SMALL, refs[1:6])
    w_hbm = bundle(WEIGHTS, refs[6:18])
    window_hbm, latent_hbm = refs[18:20]
    out = refs[20]
    s = bundle(names, refs[21:])
    small = bundle(SMALL, [getattr(s, "small_" + name) for name in SMALL])
    merged = "w_qkv" in names
    kept = [name for name in WEIGHTS if "w_" + name in names]
    w = bundle(kept, [getattr(s, "w_" + name) for name in kept])
    ownf, feat, normed = s.ownf, s.feat, s.normed
    turn = s.turn
    kvb, local_kv, halo, queries, q_full, latq = s.kvb, s.local_kv, s.halo, s.queries, s.q_full, s.latq
    gates, winb, lat, top, total, acc = s.gates, s.winb, s.lat, s.top, s.total, s.acc
    wcol, columns, psend, precv = s.wcol, s.columns, s.psend, s.precv
    cosine, sine = s.cosine, s.sine

    sp, tp = lax.axis_index("sp"), lax.axis_index("tp")
    z, x = sp // n_x, lax.rem(sp, n_x)
    y, core = tp // 2, lax.rem(tp, 2)
    other = 1 - core
    sibling = y * 2 + other
    rows, block = features.shape
    half = rows // 2
    pieces = normed.shape[1]
    piece = half // pieces
    lat_heads = w_hbm.key_up.shape[1] // NOPE
    kv_width = w_hbm.key.shape[1]
    kv_heads = kv_width // HEAD
    group = w_hbm.query.shape[1] // kv_width
    latent = w_hbm.kv_latent.shape[1]
    out_parts = lat.shape[1]
    out_rows = rows // out_parts

    def remote(src, dst, send, recv, where):
        return pltpu.make_async_remote_copy(
            src_ref=src, dst_ref=dst, send_sem=send, recv_sem=recv,
            device_id=where, device_id_type=MESH,
        )

    to_sibling = {"sp": sp, "tp": sibling}

    def arrival(ref, recv):
        return remote(ref, ref, recv, recv, to_sibling)

    def start(copies):
        for copy in copies:
            copy.start()

    def own_rows(c, h):
        return ownf.at[pl.ds(pl.multiple_of(c * half + h * piece, 16), piece)]

    def feat_rows(j, h):
        return feat.at[j, pl.ds(h * piece, piece)]

    own_load = [
        pltpu.make_async_copy(features, ownf, s.own_sem.at[0]),
        pltpu.make_async_copy(
            features.at[pl.ds(pl.multiple_of(core * half, 16), half)], feat.at[tp], s.own_sem.at[1]),
    ]
    start(own_load)
    loads = bundle(SMALL, [
        pltpu.make_async_copy(getattr(small_hbm, name), getattr(small, name), s.small_sem.at[i])
        for i, name in enumerate(SMALL)
    ])
    for name in SMALL:
        getattr(loads, name).start()

    barrier = pltpu.get_barrier_semaphore()

    def greet(where):
        pl.semaphore_signal(barrier, inc=1, device_id=where, device_id_type=MESH)

    for d in range(1, n_tp):
        greet({"sp": sp, "tp": lax.rem(tp + d, n_tp)})
    for d in range(1, n_x):
        greet({"sp": z * n_x + lax.rem(x + d, n_x), "tp": tp})

    @pl.when(z + 1 < n_z)
    def _():
        greet({"sp": sp + n_x, "tp": tp})

    @pl.when(z > 0)
    def _():
        greet({"sp": sp - n_x, "tp": tp})

    one, none = jnp.int32(1), jnp.int32(0)
    pl.semaphore_wait(
        barrier,
        n_tp - 1 + n_x - 1
        + jnp.where(z + 1 < n_z, one, none) + jnp.where(z > 0, one, none),
    )

    def feature_sends(h):
        sends = []
        for d in range(1, n_y):
            for c in range(2):
                sends.append(remote(
                    own_rows(c, h), feat_rows(tp, h), s.sent.at[0], s.f_recv.at[h],
                    {"sp": sp, "tp": lax.rem(y + d, n_y) * 2 + c}))
        sends.append(remote(
            own_rows(other, h), feat_rows(tp, h), s.sent.at[0], s.f_recv.at[h], to_sibling))
        return sends

    def feature_wait(h):
        arrival(feat.at[pl.ds(0, n_tp - 1), pl.ds(h * piece, piece)], s.f_recv.at[h]).wait_recv()

    for copy in own_load:
        copy.wait()
    for h in range(pieces):
        start(feature_sends(h))

    first = 0
    for i, name in enumerate(WEIGHTS):
        source = getattr(w_hbm, name)
        if name == "key_up":
            to = s.up.at[:, pl.ds(0, lat_heads * NOPE)]
        elif name == "value_up":
            to = s.up.at[:, pl.ds(lat_heads * NOPE, lat_heads * VDIM)]
        elif name in kept:
            to = getattr(w, name)
        else:
            to = s.w_qkv.at[:, pl.ds(first, source.shape[1])]
            first += source.shape[1]
        copy = pltpu.make_async_copy(source, to, s.w_sem.at[i])
        copy.start()
        setattr(loads, name, copy)

    def window_columns():
        local, sends = [], []
        for j in range(n_y):
            local.append(pltpu.make_async_copy(
                window_hbm.at[:, pl.ds(pl.multiple_of((j * 2 + core) * block, LANES), block)],
                wcol.at[core, j], s.w_sems.at[0]))
            sends.append(remote(
                window_hbm.at[:, pl.ds(pl.multiple_of((j * 2 + other) * block, LANES), block)],
                wcol.at[core, j], s.sent.at[0], s.w_sems.at[1], to_sibling))
        return local, sends

    paired = n_z % 2 == 0
    parity = lax.rem(z, 2)
    partner = {"sp": sp + n_x * (1 - 2 * parity), "tp": tp}

    def column_send(to, d):
        return remote(
            latent_hbm.at[:, pl.ds(pl.multiple_of(to * block, LANES), block)],
            columns.at[tp], s.sent.at[0], s.col_recv.at[d], {"sp": sp, "tp": to})

    def when_across(act):
        if paired:
            pl.when(core == parity)(act)
        else:
            act()

    def column_start():
        column_send(sibling, 0).start()

        @when_across
        def _():
            for d in range(1, n_y):
                for c in range(2):
                    column_send(lax.rem(y + d, n_y) * 2 + c, d).start()

    def pair_copy(d):
        ref = columns.at[lax.rem(y + n_y - d, n_y) * 2 + parity]
        return remote(ref, ref, s.sent.at[0], s.pair_recv.at[d - 1], partner)

    def pair_forward():
        if paired:
            for d in range(1, n_y):
                source = lax.rem(y + n_y - d, n_y) * 2 + parity
                arrival(columns.at[source], s.col_recv.at[d]).wait_recv()
                pair_copy(d).start()

    column_local = pltpu.make_async_copy(
        latent_hbm.at[:, pl.ds(pl.multiple_of(tp * block, LANES), block)],
        columns.at[tp], s.col_own.at[0])

    wcol_local, wcol_sends = window_columns()

    loads.frequency.wait()
    positions = (sp * rows + lax.broadcasted_iota(jnp.int32, (rows, ROPE), 0)).astype(F32)
    angles = positions * small.frequency[...]
    lane = lax.broadcasted_iota(jnp.int32, (rows, ROPE), 1)
    cosine[...] = jnp.cos(angles).reshape(cosine.shape)
    turned = jnp.sin(angles)
    sine[...] = jnp.where(lane < ROPE // 2, -turned, turned).reshape(sine.shape)

    def normalize(h):
        squares = jnp.zeros((piece, 1), F32)
        part = slice(h * piece, (h + 1) * piece)
        for j in range(n_tp):
            values = feat[j, part].astype(F32)
            squares = squares + jnp.sum(values * values, axis=-1, keepdims=True)
        scale = lax.rsqrt(squares / (n_tp * block) + EPS)
        for j in range(n_tp):
            span = slice(j * block, (j + 1) * block)
            values = feat[j, part].astype(F32) * scale * small.norm_gain[:, span]
            normed[core, h, :, span] = values.astype(BF16)

    def normed_copy(h):
        return remote(normed.at[core, h], normed.at[core, h], s.sent.at[0], s.n_sems.at[0], to_sibling)

    def latents(h):
        own = normed[core, h]
        rope = dot_t(own, w.rope[...])
        rope = rope * cosine[core, h] + swap_halves(rope) * sine[core, h]
        rope = jnp.concatenate([rope[: piece // 2], rope[piece // 2 :]], axis=1)
        rope = [rope[i : i + SUBLANES] for i in range(0, piece // 2, SUBLANES)]
        rope.append(jnp.zeros((SUBLANES, latent - len(rope) * LANES), F32))
        kvb[sp, core, h, :piece, :] = rms_rows(dot(own, w.kv_latent[...]), small.kv_gain[...]).astype(BF16)
        kvb[sp, core, h, piece:, :] = jnp.concatenate(rope, axis=1).astype(BF16)

    def rope_rows(slot, halves=range(2)):
        parts = []
        for c in halves:
            for h in range(pieces):
                packed = kvb[slot, c, h, piece:, :].astype(F32)
                pair = jnp.concatenate(
                    [packed[:, i * LANES : (i + 1) * LANES] for i in range(piece // 2 // SUBLANES)], axis=0)
                parts += [pair, pltpu.roll(pair, ROPE, 1)]
        return jnp.concatenate(parts, axis=0).astype(BF16)

    def column_slot(k):
        return (z - k) * n_x + x

    def row_slot(k, d):
        return (z - k) * n_x + lax.rem(x + n_x - d, n_x)

    def z_copy(k, h):
        ref = kvb.at[column_slot(k), core, h]
        return remote(ref, ref, s.sent.at[0], s.z_recv.at[h, k], {"sp": sp + n_x, "tp": tp})

    def x_copy(k, d, h):
        ref = kvb.at[column_slot(k), core, h]
        return remote(ref, ref, s.sent.at[0], s.x_recv.at[k, d - 1],
                      {"sp": z * n_x + lax.rem(x + d, n_x), "tp": tp})

    def c_copy(k, h):
        ref = kvb.at[column_slot(k), core, h]
        return remote(ref, ref, s.sent.at[0], s.c_recv.at[k], to_sibling)

    def d_copy(k, d):
        ref = kvb.at[row_slot(k, d), core]
        return remote(ref, ref, s.sent.at[0], s.d_recv.at[k, d - 1], to_sibling)

    def wait_column(k):
        arrival(kvb.at[column_slot(k), other], s.c_recv.at[k]).wait_recv()

    def wait_row(k, d):
        arrival(kvb.at[row_slot(k, d), other], s.d_recv.at[k, d - 1]).wait_recv()

    def sends_row(k, d):
        return (k > 0) | (x + d < n_x)

    def takes_row(k, d):
        return (k > 0) | (x >= d)

    def detoured(k, h, to):
        if h == DETOURS[0]:
            return (k >= 2) & (to > 0)
        return (k >= 3) & (to == 0)

    def pass_on(k, h):
        @pl.when(z + 1 < n_z)
        def _():
            z_copy(k, h).start()

        for d in range(1, n_x):
            to = lax.rem(x + d, n_x)

            @pl.when(sends_row(k, d) & ~detoured(k, h, to) if h in DETOURS else sends_row(k, d))
            def _():
                x_copy(k, d, h).start()

        c_copy(k, h).start()

    def take_column(k, h):
        arrival(kvb.at[column_slot(k), core, h], s.z_recv.at[h, k - 1]).wait_recv()
        pass_on(k, h)

    def detour_copy(k, d, i):
        ref = kvb.at[row_slot(k, d), core, DETOURS[i]]
        return remote(ref, ref, s.sent.at[0], s.r_recv.at[i, k - 1, d - 1], {"sp": sp + n_x, "tp": tp})

    def passes_detour(k, i):
        return (z + 1 < n_z) & detoured(k + 1, DETOURS[i], x)

    def take_row(k, d):
        own = kvb.at[row_slot(k, d), core]
        shorter = functools.reduce(jnp.logical_or, [detoured(k, h, x) for h in DETOURS])

        @pl.when(~shorter)
        def _():
            arrival(own, s.x_recv.at[k, d - 1]).wait_recv()

        @pl.when(shorter)
        def _():
            arrival(own.at[pl.ds(0, pieces - 1)], s.x_recv.at[k, d - 1]).wait_recv()

        for i, h in enumerate(DETOURS):
            @pl.when(detoured(k, h, x))
            def _():
                arrival(own.at[h], s.r_recv.at[i, k - 2, d - 1]).wait_recv()

            @pl.when(passes_detour(k, i))
            def _():
                detour_copy(k, d, i).start()

        d_copy(k, d).start()

    def take_second(lo, hi):
        for h in range(lo, hi):
            @pl.when(z >= 2)
            def _():
                take_column(2, h)

    def take_first(h):
        @pl.when(z >= 1)
        def _():
            take_column(1, h)

    start(wcol_local)
    start(wcol_sends)
    column_local.start()
    for name in ("norm_gain", "kv_gain", "kv_latent", "rope"):
        getattr(loads, name).wait()
    for h in range(pieces):
        feature_wait(h)
        if h == pieces - 1:
            column_start()
        normalize(h)
        normed_copy(h).start()
        latents(h)
        pass_on(0, h)
        if 1 <= h <= pieces // 2:
            take_first(h - 1)

    loads.query_latent.wait()
    loads.q_gain.wait()
    own_normed = normed[core].reshape(half, n_tp * block)
    latq[core] = rms_rows(dot(own_normed, w.query_latent[...]), small.q_gain[...]).astype(BF16)
    latq_copy = remote(latq.at[core], latq.at[core], s.sent.at[0], s.q_sems.at[0], to_sibling)
    latq_copy.start()

    arrival(normed.at[other], s.n_sems.at[0]).wait_recv()

    if n_z > 2:
        take_second(0, 1)

    def all_normed():
        return normed[...].reshape(rows, n_tp * block)

    for name in MERGED:
        getattr(loads, name).wait()
    if merged:
        qkv = dot(all_normed(), s.w_qkv[...]).astype(BF16)
    else:
        qkv = jnp.concatenate([dot(all_normed(), getattr(w, name)[...]) for name in MERGED], axis=1).astype(BF16)
    local_kv[...] = qkv[:, : 2 * kv_width]
    queries[...] = qkv[:, 2 * kv_width :]
    tail = local_kv.at[pl.ds(rows - WINDOW, WINDOW)]
    halo_copy = remote(tail, halo, s.sent.at[0], s.halo_sem.at[0], {"sp": sp + 1, "tp": tp})
    turn_copy = remote(tail, turn, s.sent.at[0], s.halo_sem.at[1], {"sp": z * n_x, "tp": tp})
    relay_copy = remote(turn, halo, s.sent.at[0], s.halo_sem.at[0], {"sp": sp + n_x, "tp": tp})

    @pl.when((x + 1 == n_x) & (z + 1 < n_z))
    def _():
        turn_copy.start()

    take_first(pieces - 2)

    def queries_up():
        arrival(latq.at[other], s.q_sems.at[0]).wait_recv()
        loads.content.wait()
        loads.rotary.wait()
        latent_query = latq[...].reshape(rows, latent)
        content = dot(latent_query, w.content[...])
        rotary = dot(latent_query, w.rotary[...])
        cos_all, sin_all = cosine[...].reshape(rows, ROPE), sine[...].reshape(rows, ROPE)
        padding = jnp.zeros((rows, LANES - ROPE), F32)
        for h in range(lat_heads):
            turned = rotary[:, h * ROPE : (h + 1) * ROPE]
            turned = turned * cos_all + swap_halves(turned) * sin_all
            q_full[h, :NOPE, :] = content[:, h * NOPE : (h + 1) * NOPE].T.astype(BF16)
            q_full[h, NOPE:, :] = jnp.concatenate([turned, padding], axis=1).T.astype(BF16)
        loads.key_up.wait()
        loads.value_up.wait()

    def attend(slot, diagonal, which=None):
        if which is None:
            source = kvb[slot, :, :, :piece, :].reshape(rows, latent)
            rope_part = rope_rows(slot)
        else:
            source = kvb[slot, which, :, :piece, :].reshape(half, latent)
            rope_part = rope_rows(slot, [which])
        both = dot(source, s.up[...]).astype(BF16)
        keys, values = both[:, : lat_heads * NOPE], both[:, lat_heads * NOPE :]
        heads = range(lat_heads)
        scores = []
        for h in heads:
            key = jnp.concatenate([keys[:, h * NOPE : (h + 1) * NOPE], rope_part], axis=1)
            scores.append(dot(key, q_full[h]) * ((NOPE + ROPE) ** (-0.5) * LOG2_E))
        if diagonal:
            live = (lax.broadcasted_iota(jnp.int32, (rows, rows), 0)
                    <= lax.broadcasted_iota(jnp.int32, (rows, rows), 1))
            scores = [jnp.where(live, part, NEGATIVE) for part in scores]
        weights, fades = [], []
        for h in heads:
            peak = jnp.max(scores[h], axis=0, keepdims=True)
            if not diagonal:
                before = top[h]
                peak = jnp.maximum(peak, before)
                fades.append(jnp.exp2(before - peak))
            top[h] = peak
            weights.append(jnp.exp2(scores[h] - peak))
        for h in heads:
            weight_sum = jnp.sum(weights[h], axis=0, keepdims=True)
            part = dot_tl(values[:, h * VDIM : (h + 1) * VDIM], weights[h].astype(BF16))
            if not diagonal:
                weight_sum = total[h] * fades[h] + weight_sum
                part = acc[h] * fades[h] + part
            total[h] = weight_sum
            acc[h] = part

    def take_halo():
        @pl.when(sp > 0)
        def _():
            arrival(halo, s.halo_sem.at[0]).wait_recv()

        @pl.when(sp == 0)
        def _():
            halo[...] = jnp.zeros(halo.shape, BF16)

    def window(blocks):
        row = lax.broadcasted_iota(jnp.int32, (2 * WINDOW, WINDOW), 1)
        column = lax.broadcasted_iota(jnp.int32, (2 * WINDOW, WINDOW), 0)
        offset = row + WINDOW - column
        in_band = (offset >= 0) & (offset < WINDOW)
        in_band = jnp.concatenate([in_band] * group, axis=1)
        later = jnp.concatenate([(sp > 0) | (column >= WINDOW)] * group, axis=1)
        units = [(n, g) for n in blocks for g in range(kv_heads)]
        scores, values, sinks, weights = [], [], [], []
        for n, g in units:
            at = slice(n * WINDOW, (n + 1) * WINDOW)
            earlier = halo[...] if n == 0 else local_kv[(n - 1) * WINDOW : n * WINDOW]
            band = jnp.concatenate([earlier, local_kv[at]], axis=0)
            valid = in_band & later if n == 0 else in_band
            key = band[:, g * HEAD : (g + 1) * HEAD]
            values.append(band[:, kv_width + g * HEAD : kv_width + (g + 1) * HEAD])
            members = range(g * group, (g + 1) * group)
            query = jnp.concatenate([queries[at, q * HEAD : (q + 1) * HEAD] for q in members], axis=0)
            sinks.append(jnp.concatenate([jnp.full((1, WINDOW), small.sinks[0, q], F32) for q in members], axis=1))
            scores.append(jnp.where(valid, dot_t(key, query) * HEAD ** (-0.5), NEGATIVE))
        for u in range(len(units)):
            peak = jnp.maximum(jnp.max(scores[u], axis=0, keepdims=True), sinks[u])
            part = jnp.exp(scores[u] - peak)
            bottom = jnp.sum(part, axis=0, keepdims=True) + jnp.exp(sinks[u] - peak)
            weights.append((part * (1.0 / bottom)).astype(BF16))
        mixed = [dot_tl(values[u], weights[u]) for u in range(len(units))]
        for b, n in enumerate(blocks):
            heads = [
                mixed[b * kv_heads + g][:, i * WINDOW : (i + 1) * WINDOW]
                for g in range(kv_heads) for i in range(group)
            ]
            winb[core, n * WINDOW : (n + 1) * WINDOW, :] = jnp.concatenate(heads, axis=0).T.astype(BF16)

    def win_copy(i):
        ref = winb.at[core, win_rows[i]]
        return remote(ref, ref, s.sent.at[0], s.win_recv.at[i], to_sibling)

    win_rows = (pl.ds(WINDOW, rows - WINDOW), pl.ds(0, WINDOW))

    def window_part(j, at):
        return dot(winb[0, at], wcol[0, j]) + dot(winb[1, at], wcol[1, j])

    def part_copy(d, at):
        return remote(psend.at[d - 1, at], precv.at[d - 1, at], s.sent.at[0], s.p_recv.at[d - 1],
                      {"sp": sp, "tp": lax.rem(y + d, n_y) * 2 + core})

    def window_parts(i):
        at = win_rows[i]
        arrival(winb.at[other, at], s.win_recv.at[i]).wait_recv()
        for d in range(1, n_y):
            psend[d - 1, at] = window_part(lax.rem(y + d, n_y), at).astype(BF16)
            part_copy(d, at).start()

    def gate(b):
        name = WEIGHTS[10 + b]
        getattr(loads, name).wait()

        def step(i, _):
            at = pl.ds(pl.multiple_of(i * 256, LANES), 256)
            gates[b, :, at] = jax.nn.sigmoid(dot(all_normed(), getattr(w, name)[:, at]))
            return 0

        lax.fori_loop(0, block // 256, step, 0)

    def take_rows(k):
        for d in range(1, n_x):
            pl.when(takes_row(k, d))(functools.partial(take_row, k, d))

    def attend_row(k, d):
        wait_row(k, d)
        attend(row_slot(k, d), False)

    loads.sinks.wait()
    window(range(1, rows // WINDOW))
    win_copy(0).start()
    take_first(pieces - 1)
    queries_up()
    if n_z > 2:
        take_second(1, pieces // 2)
    pltpu.make_async_copy(wcol.at[core], wcol.at[core], s.w_sems.at[0]).wait()
    arrival(wcol.at[other], s.w_sems.at[1]).wait_recv()
    window_parts(0)
    take_rows(0)
    wait_column(0)
    attend(sp, True)
    if n_z > 2:
        take_second(pieces // 2, pieces - 1)

    @pl.when(x + 1 < n_x)
    def _():
        halo_copy.start()

    @pl.when((x == 0) & (z + 1 < n_z))
    def _():
        arrival(turn, s.halo_sem.at[1]).wait_recv()
        relay_copy.start()


    def take_pieces(k, lo, hi):
        @pl.when(z >= k)
        def _():
            for h in range(lo, hi):
                take_column(k, h)

    def first_window():
        take_halo()
        window(range(1))
        win_copy(1).start()

    def last_parts():
        window_parts(1)

    def attend_halves(slot, wait):
        def halves(i, _):
            @pl.when(i == 1)
            def _():
                wait()

            attend(slot, False, jnp.where(i == 0, core, other))
            return 0

        lax.fori_loop(0, 2, halves, 0)

    def step(k, _):
        @pl.when(k == 4 - parity)
        def _():
            pair_forward()

        @pl.when((z >= k - 1) & (k < n_z))
        def _():
            wait_column(k - 1)
            attend(column_slot(k - 1), False)

        @pl.when((z >= k - 1) & (k == n_z))
        def _():
            attend_halves(column_slot(k - 1), functools.partial(wait_column, k - 1))

        @pl.when(k == 2)
        def _():
            take_pieces(k, pieces - 1, pieces)

        pl.when(k == 4)(last_parts)

        @pl.when(k > 2)
        def _():
            pl.when(x == 0)(functools.partial(take_pieces, k, 0, 1))
            take_pieces(k, 1, pieces // 2)

        for d in range(1, n_x):
            @pl.when((z >= k - 2) & takes_row(k - 2, d))
            def _():
                attend_row(k - 2, d)

        @pl.when(k > 2)
        def _():
            take_pieces(k, pieces // 2, pieces - 1)

        pl.when(k == 3)(first_window)

        @pl.when(k > 2)
        def _():
            take_pieces(k, pieces - 1, pieces)


        @pl.when(z >= k - 1)
        def _():
            take_rows(k - 1)

        @pl.when(x > 0)
        def _():
            take_pieces(k + 1, 0, 1)

        return 0

    lax.fori_loop(2, max(n_z, 4) + 1, step, 0)

    @pl.when(z == n_z - 1)
    def _():
        for d in range(1, n_x):
            @pl.when(takes_row(n_z - 1, d))
            def _():
                attend_halves(row_slot(n_z - 1, d), functools.partial(wait_row, n_z - 1, d))


    def gather(part):
        own = lat.at[tp, part]
        sends = [
            remote(own, own, s.sent.at[0], s.y_recv.at[part, d - 1],
                   {"sp": sp, "tp": lax.rem(y + d, n_y) * 2 + core})
            for d in range(1, n_y)
        ]
        sends.append(remote(own, own, s.sent.at[0], s.s_recv.at[part], to_sibling))
        return sends

    def forward(part):
        for d in range(1, n_y):
            ref = lat.at[lax.rem(y + n_y - d, n_y) * 2 + core, part]
            arrival(ref, s.y_recv.at[part, d - 1]).wait_recv()
            remote(ref, ref, s.sent.at[0], s.s_recv.at[part], to_sibling).start()

    def arrived(part):
        arrival(lat.at[pl.ds(0, n_y), part], s.s_recv.at[part]).wait_recv()

    for part in range(out_parts):
        at = slice(part * out_rows, (part + 1) * out_rows)
        for h in range(lat_heads):
            lat[tp, part, :, h * VDIM : (h + 1) * VDIM] = (
                acc[h, :, at] * (1.0 / total[h, :, at])).T.astype(BF16)
        start(gather(part))
    gate(0)
    gate(1)
    window_branch = window_part(y, pl.ds(0, rows))
    for d in range(1, n_y):
        arrival(precv.at[d - 1], s.p_recv.at[d - 1]).wait_recv()
        window_branch = window_branch + precv[d - 1].astype(F32)
    gates[0] = gates[0] * window_branch
    column_local.wait()
    arrival(columns.at[sibling], s.col_recv.at[0]).wait_recv()
    for d in range(1, n_y):
        base = lax.rem(y + n_y - d, n_y) * 2
        if paired:
            arrival(columns.at[base + 1 - parity], s.pair_recv.at[d - 1]).wait_recv()
        else:
            arrival(columns.at[pl.ds(base, 2)], s.col_recv.at[d]).wait_recv()
    for part in range(out_parts):
        at = slice(part * out_rows, (part + 1) * out_rows)
        forward(part)
        arrived(part)
        latent_branch = jnp.zeros((out_rows, block), F32)
        for j in range(n_tp):
            latent_branch = latent_branch + dot(lat[j, part], columns[j])
        out[at, :] = (gates[0, at] + gates[1, at] * latent_branch).astype(BF16)

    def leave(ref, send):
        remote(ref, ref, send, send, to_sibling).wait_send()

    leave(ownf.at[pl.ds(0, half)], s.sent.at[0])
    for d in range(1, n_y):
        leave(ownf, s.sent.at[0])
    leave(normed.at[core], s.sent.at[0])
    latq_copy.wait_send()
    leave(wcol.at[core], s.sent.at[0])
    leave(columns.at[tp], s.sent.at[0])

    @when_across
    def _():
        for d in range(1, n_y):
            leave(columns.at[pl.ds(0, 2)], s.sent.at[0])

    if paired:
        for d in range(1, n_y):
            pair_copy(d).wait_send()
    for i in range(2):
        win_copy(i).wait_send()
    for d in range(1, n_y):
        leave(psend.at[d - 1], s.sent.at[0])
        leave(lat.at[tp], s.sent.at[0])
        leave(lat.at[tp], s.sent.at[0])
    leave(lat.at[tp], s.sent.at[0])

    @pl.when((x + 1 < n_x) | (z + 1 < n_z))
    def _():
        halo_copy.wait_send()

    @pl.when((x == 0) & (z + 1 < n_z))
    def _():
        relay_copy.wait_send()

    def drain(k, _):
        @pl.when(z >= k)
        def _():
            own = kvb.at[column_slot(k), core]

            @pl.when(z + 1 < n_z)
            def _():
                leave(own, s.sent.at[0])

            leave(own, s.sent.at[0])
            for d in range(1, n_x):
                to = lax.rem(x + d, n_x)
                fewer = [detoured(k, h, to) for h in DETOURS]

                @pl.when(sends_row(k, d) & ~(fewer[0] | fewer[1]))
                def _():
                    leave(own, s.sent.at[0])

                @pl.when(fewer[0] | fewer[1])
                def _():
                    leave(own.at[pl.ds(0, pieces - 1)], s.sent.at[0])

                for i in range(2):
                    @pl.when(takes_row(k, d) & passes_detour(k, i))
                    def _():
                        detour_copy(k, d, i).wait_send()

                @pl.when(takes_row(k, d))
                def _():
                    leave(own, s.sent.at[0])

        return 0

    lax.fori_loop(0, n_z, drain, 0)


def on_device(dims, features, norm_gain, w_query, w_key, w_value, head_sinks, w_query_latent,
              w_kv_latent, w_rope_key, query_latent_gain, kv_latent_gain, w_query_content,
              w_query_rotary, w_key_up, w_value_up, w_branch_window, w_branch_latent,
              w_gate_window, w_gate_latent):
    n_sp, n_tp, n_x = dims
    n_z, n_y = n_sp // n_x, n_tp // 2
    rows, block = features.shape
    width = norm_gain.shape[0]
    latent = w_kv_latent.shape[1]
    lat_heads = w_key_up.shape[1] // NOPE
    half_width = ROPE // 2
    entry = np.arange(ROPE, dtype=np.int32) % half_width
    frequency = (np.float32(THETA) ** (-entry.astype(np.float32) / np.float32(half_width))).astype(np.float32)[None, :]
    weights = (w_kv_latent, w_rope_key.T, w_key, w_value, w_query, w_query_latent, w_query_content,
               w_query_rotary, w_key_up, w_value_up, w_gate_window, w_gate_latent)
    smalls = (norm_gain[None, :], head_sinks[None, :], query_latent_gain[None, :], kv_latent_gain[None, :],
              jnp.asarray(frequency))
    branch_rows = w_branch_window.shape[0]
    pieces = PIECES
    piece = rows // 2 // pieces
    out_parts = rows // LANES
    merge = w_key.shape[1] % LANES == 0
    hbm = pl.BlockSpec(memory_space=pl.ANY)
    dma = pltpu.SemaphoreType.DMA
    vm = pltpu.VMEM
    scratch = dict(
        **{"small_" + n: (pltpu.SMEM if n == "sinks" else vm)(a.shape, F32) for n, a in zip(SMALL, smalls)},
        **{"w_" + n: vm(a.shape, BF16) for n, a in zip(WEIGHTS, weights) if not (merge and n in MERGED or n in UP)},
        up=vm((latent, w_key_up.shape[1] + w_value_up.shape[1]), BF16),
        **(dict(w_qkv=vm((width, 2 * w_key.shape[1] + w_query.shape[1]), BF16)) if merge else {}),
        ownf=vm((rows, block), BF16),
        feat=vm((n_tp, rows // 2, block), BF16),
        normed=vm((2, pieces, piece, width), BF16),
        latq=vm((2, rows // 2, latent), BF16),
        wcol=vm((2, n_y, branch_rows, block), BF16),
        columns=vm((n_tp, w_branch_latent.shape[0], block), BF16),
        psend=vm((n_y - 1, rows, block), BF16),
        precv=vm((n_y - 1, rows, block), BF16),
        kvb=vm((n_sp, 2, pieces, piece + SUBLANES, latent), BF16),
        local_kv=vm((rows, 2 * w_key.shape[1]), BF16),
        halo=vm((WINDOW, 2 * w_key.shape[1]), BF16),
        turn=vm((WINDOW, 2 * w_key.shape[1]), BF16),
        queries=vm((rows, w_query.shape[1]), BF16),
        q_full=vm((lat_heads, NOPE + LANES, rows), BF16),
        gates=vm((2, rows, block), F32),
        winb=vm((2, rows, w_query.shape[1]), BF16),
        lat=vm((n_tp, out_parts, rows // out_parts, lat_heads * VDIM), BF16),
        top=vm((lat_heads, 1, rows), F32),
        total=vm((lat_heads, 1, rows), F32),
        acc=vm((lat_heads, VDIM, rows), F32),
        cosine=vm((2, pieces, piece, ROPE), F32),
        sine=vm((2, pieces, piece, ROPE), F32),
        own_sem=dma((2,)),
        sent=dma((1,)),
        small_sem=dma((len(SMALL),)),
        w_sem=dma((len(weights),)),
        f_recv=dma((pieces,)),
        n_sems=dma((1,)),
        q_sems=dma((1,)),
        w_sems=dma((2,)),
        col_own=dma((1,)),
        col_recv=dma((n_y,)),
        pair_recv=dma((n_y - 1,)),
        halo_sem=dma((2,)),
        win_recv=dma((2,)),
        p_recv=dma((n_y - 1,)),
        y_recv=dma((out_parts, n_y - 1)),
        s_recv=dma((out_parts,)),
        z_recv=dma((pieces, n_z - 1)),
        r_recv=dma((2, n_z - 2, n_x - 1)),
        x_recv=dma((n_z, n_x - 1)),
        c_recv=dma((n_z,)),
        d_recv=dma((n_z, n_x - 1)),
    )
    return pl.pallas_call(
        functools.partial(kernel, dims, tuple(scratch)),
        out_shape=pltpu.VMEM((rows, block), BF16),
        in_specs=[hbm] * (1 + len(smalls) + len(weights) + 2),
        out_specs=pl.BlockSpec(memory_space=pltpu.VMEM),
        scratch_shapes=list(scratch.values()),
        compiler_params=pltpu.CompilerParams(
            collective_id=0, has_side_effects=True, vmem_limit_bytes=60 * 1024 * 1024
        ),
    )(features, *smalls, *weights, w_branch_window, w_branch_latent)


def solution(mesh):
    n_sp, n_tp = mesh.shape["sp"], mesh.shape["tp"]
    n_x = 1
    while n_sp % (2 * n_x) == 0 and 8 * n_x * n_x <= n_sp:
        n_x *= 2
    return jax.shard_map(
        functools.partial(on_device, (n_sp, n_tp, n_x)),
        mesh=mesh,
        in_specs=(
            P("sp", "tp"),
            P(),
            P(None, "tp"),
            P(None, "tp"),
            P(None, "tp"),
            P("tp"),
            P(),
            P(),
            P(),
            P(),
            P(),
            P(None, "tp"),
            P(None, "tp"),
            P(None, "tp"),
            P(None, "tp"),
            P("tp", None),
            P("tp", None),
            P(None, "tp"),
            P(None, "tp"),
        ),
        out_specs=P("sp", "tp"),
        check_vma=False,
    )
```

```python
import functools
import types

import jax
import jax.numpy as jnp
import numpy as np
from jax import lax
from jax.experimental import pallas as pl
from jax.experimental.pallas import tpu as pltpu
from jax.sharding import PartitionSpec as P

HEAD = 64
WINDOW = 128
NOPE = 128
ROPE = 64
VDIM = 128


EPS = 1e-06
THETA = 10000.0
NEGATIVE = -1e30
LANES = 128
LOG2_E = 1.4426950408889634
MESH = pl.DeviceIdType.MESH
BF16 = jnp.bfloat16
F32 = jnp.float32
PIECES = 4
SUBLANES = 8
DETOURS = (0, PIECES - 1)


def dot(left, right):
    return jnp.dot(left, right, preferred_element_type=F32)


def dot_t(left, right):
    return lax.dot_general(left, right, (((1,), (1,)), ((), ())), preferred_element_type=F32)


def dot_tl(left, right):
    return lax.dot_general(left, right, (((0,), (0,)), ((), ())), preferred_element_type=F32)


def rms_rows(rows, gain):
    return rows * lax.rsqrt(jnp.mean(rows * rows, axis=-1, keepdims=True) + EPS) * gain


def swap_halves(rows):
    half = rows.shape[1] // 2
    return jnp.concatenate([rows[:, half:], rows[:, :half]], axis=1)


SMALL = ("norm_gain", "sinks", "q_gain", "kv_gain", "frequency")
WEIGHTS = (
    "kv_latent", "rope", "key", "value", "query", "query_latent", "content", "rotary",
    "key_up", "value_up", "gate_window", "gate_latent",
)
def bundle(names, values):
    return types.SimpleNamespace(**dict(zip(names, values)))


UP = ("key_up", "value_up")
MERGED = ("key", "value", "query")


def kernel(dims, names, *refs):
    n_sp, n_tp, n_x = dims
    n_z, n_y = n_sp // n_x, n_tp // 2
    features = refs[0]
    small_hbm = bundle(SMALL, refs[1:6])
    w_hbm = bundle(WEIGHTS, refs[6:18])
    window_hbm, latent_hbm = refs[18:20]
    out = refs[20]
    s = bundle(names, refs[21:])
    small = bundle(SMALL, [getattr(s, "small_" + name) for name in SMALL])
    merged = "w_qkv" in names
    kept = [name for name in WEIGHTS if "w_" + name in names]
    w = bundle(kept, [getattr(s, "w_" + name) for name in kept])
    ownf, feat, normed = s.ownf, s.feat, s.normed
    turn = s.turn
    kvb, local_kv, halo, queries, q_full, latq = s.kvb, s.local_kv, s.halo, s.queries, s.q_full, s.latq
    gates, winb, lat, top, total, acc = s.gates, s.winb, s.lat, s.top, s.total, s.acc
    wcol, columns, psend, precv = s.wcol, s.columns, s.psend, s.precv
    cosine, sine = s.cosine, s.sine

    sp, tp = lax.axis_index("sp"), lax.axis_index("tp")
    z, x = sp // n_x, lax.rem(sp, n_x)
    y, core = tp // 2, lax.rem(tp, 2)
    other = 1 - core
    sibling = y * 2 + other
    rows, block = features.shape
    half = rows // 2
    pieces = normed.shape[1]
    piece = half // pieces
    lat_heads = w_hbm.key_up.shape[1] // NOPE
    kv_width = w_hbm.key.shape[1]
    kv_heads = kv_width // HEAD
    group = w_hbm.query.shape[1] // kv_width
    latent = w_hbm.kv_latent.shape[1]
    out_parts = lat.shape[1]
    out_rows = rows // out_parts

    def remote(src, dst, send, recv, where):
        return pltpu.make_async_remote_copy(
            src_ref=src, dst_ref=dst, send_sem=send, recv_sem=recv,
            device_id=where, device_id_type=MESH,
        )

    to_sibling = {"sp": sp, "tp": sibling}

    def arrival(ref, recv):
        return remote(ref, ref, recv, recv, to_sibling)

    def start(copies):
        for copy in copies:
            copy.start()

    def own_rows(c, h):
        return ownf.at[pl.ds(pl.multiple_of(c * half + h * piece, 16), piece)]

    def feat_rows(j, h):
        return feat.at[j, pl.ds(h * piece, piece)]

    barrier = pltpu.get_barrier_semaphore()

    def greet(where):
        pl.semaphore_signal(barrier, inc=1, device_id=where, device_id_type=MESH)

    for d in range(1, n_tp):
        greet({"sp": sp, "tp": lax.rem(tp + d, n_tp)})
    for d in range(1, n_x):
        greet({"sp": z * n_x + lax.rem(x + d, n_x), "tp": tp})

    @pl.when(z + 1 < n_z)
    def _():
        greet({"sp": sp + n_x, "tp": tp})

    @pl.when(z > 0)
    def _():
        greet({"sp": sp - n_x, "tp": tp})

    own_load = [
        pltpu.make_async_copy(features, ownf, s.own_sem.at[0]),
        pltpu.make_async_copy(
            features.at[pl.ds(pl.multiple_of(core * half, 16), half)], feat.at[tp], s.own_sem.at[1]),
    ]
    start(own_load)
    loads = bundle(SMALL, [
        pltpu.make_async_copy(getattr(small_hbm, name), getattr(small, name), s.small_sem.at[i])
        for i, name in enumerate(SMALL)
    ])
    for name in SMALL:
        getattr(loads, name).start()

    one, none = jnp.int32(1), jnp.int32(0)
    pl.semaphore_wait(
        barrier,
        n_tp - 1 + n_x - 1
        + jnp.where(z + 1 < n_z, one, none) + jnp.where(z > 0, one, none),
    )

    def feature_sends(h):
        sends = []
        for d in range(1, n_y):
            for c in range(2):
                sends.append(remote(
                    own_rows(c, h), feat_rows(tp, h), s.sent.at[0], s.f_recv.at[h],
                    {"sp": sp, "tp": lax.rem(y + d, n_y) * 2 + c}))
        sends.append(remote(
            own_rows(other, h), feat_rows(tp, h), s.sent.at[0], s.f_recv.at[h], to_sibling))
        return sends

    def feature_wait(h):
        arrival(feat.at[pl.ds(0, n_tp - 1), pl.ds(h * piece, piece)], s.f_recv.at[h]).wait_recv()

    for copy in own_load:
        copy.wait()
    for h in range(pieces):
        start(feature_sends(h))

    first = 0
    for i, name in enumerate(WEIGHTS):
        source = getattr(w_hbm, name)
        if name == "key_up":
            to = s.up.at[:, pl.ds(0, lat_heads * NOPE)]
        elif name == "value_up":
            to = s.up.at[:, pl.ds(lat_heads * NOPE, lat_heads * VDIM)]
        elif name in kept:
            to = getattr(w, name)
        else:
            to = s.w_qkv.at[:, pl.ds(first, source.shape[1])]
            first += source.shape[1]
        copy = pltpu.make_async_copy(source, to, s.w_sem.at[i])
        copy.start()
        setattr(loads, name, copy)

    def window_columns():
        local, sends = [], []
        for j in range(n_y):
            local.append(pltpu.make_async_copy(
                window_hbm.at[:, pl.ds(pl.multiple_of((j * 2 + core) * block, LANES), block)],
                wcol.at[core, j], s.w_sems.at[0]))
            sends.append(remote(
                window_hbm.at[:, pl.ds(pl.multiple_of((j * 2 + other) * block, LANES), block)],
                wcol.at[core, j], s.sent.at[0], s.w_sems.at[1], to_sibling))
        return local, sends

    paired = n_z % 2 == 0
    parity = lax.rem(z, 2)
    partner = {"sp": sp + n_x * (1 - 2 * parity), "tp": tp}

    def column_send(to, d):
        return remote(
            latent_hbm.at[:, pl.ds(pl.multiple_of(to * block, LANES), block)],
            columns.at[tp], s.sent.at[0], s.col_recv.at[d], {"sp": sp, "tp": to})

    def when_across(act):
        if paired:
            pl.when(core == parity)(act)
        else:
            act()

    def column_start():
        column_send(sibling, 0).start()

        @when_across
        def _():
            for d in range(1, n_y):
                for c in range(2):
                    column_send(lax.rem(y + d, n_y) * 2 + c, d).start()

    def pair_copy(d):
        ref = columns.at[lax.rem(y + n_y - d, n_y) * 2 + parity]
        return remote(ref, ref, s.sent.at[0], s.pair_recv.at[d - 1], partner)

    def pair_forward():
        if paired:
            for d in range(1, n_y):
                source = lax.rem(y + n_y - d, n_y) * 2 + parity
                arrival(columns.at[source], s.col_recv.at[d]).wait_recv()
                pair_copy(d).start()

    column_local = pltpu.make_async_copy(
        latent_hbm.at[:, pl.ds(pl.multiple_of(tp * block, LANES), block)],
        columns.at[tp], s.col_own.at[0])

    wcol_local, wcol_sends = window_columns()

    loads.frequency.wait()
    positions = (sp * rows + lax.broadcasted_iota(jnp.int32, (rows, ROPE), 0)).astype(F32)
    angles = positions * small.frequency[...]
    lane = lax.broadcasted_iota(jnp.int32, (rows, ROPE), 1)
    cosine[...] = jnp.cos(angles).reshape(cosine.shape)
    turned = jnp.sin(angles)
    sine[...] = jnp.where(lane < ROPE // 2, -turned, turned).reshape(sine.shape)

    def normalize(h):
        squares = jnp.zeros((piece, 1), F32)
        part = slice(h * piece, (h + 1) * piece)
        for j in range(n_tp):
            values = feat[j, part].astype(F32)
            squares = squares + jnp.sum(values * values, axis=-1, keepdims=True)
        scale = lax.rsqrt(squares / (n_tp * block) + EPS)
        for j in range(n_tp):
            span = slice(j * block, (j + 1) * block)
            values = feat[j, part].astype(F32) * scale * small.norm_gain[:, span]
            normed[core, h, :, span] = values.astype(BF16)

    def normed_copy(h):
        return remote(normed.at[core, h], normed.at[core, h], s.sent.at[0], s.n_sems.at[0], to_sibling)

    def latents(h):
        own = normed[core, h]
        rope = dot_t(own, w.rope[...])
        rope = rope * cosine[core, h] + swap_halves(rope) * sine[core, h]
        rope = jnp.concatenate([rope[: piece // 2], rope[piece // 2 :]], axis=1)
        rope = [rope[i : i + SUBLANES] for i in range(0, piece // 2, SUBLANES)]
        rope.append(jnp.zeros((SUBLANES, latent - len(rope) * LANES), F32))
        kvb[sp, core, h, :piece, :] = rms_rows(dot(own, w.kv_latent[...]), small.kv_gain[...]).astype(BF16)
        kvb[sp, core, h, piece:, :] = jnp.concatenate(rope, axis=1).astype(BF16)

    def rope_rows(slot, halves=range(2)):
        parts = []
        for c in halves:
            for h in range(pieces):
                packed = kvb[slot, c, h, piece:, :].astype(F32)
                pair = jnp.concatenate(
                    [packed[:, i * LANES : (i + 1) * LANES] for i in range(piece // 2 // SUBLANES)], axis=0)
                parts += [pair, pltpu.roll(pair, ROPE, 1)]
        return jnp.concatenate(parts, axis=0).astype(BF16)

    def column_slot(k):
        return (z - k) * n_x + x

    def row_slot(k, d):
        return (z - k) * n_x + lax.rem(x + n_x - d, n_x)

    def z_copy(k, h):
        ref = kvb.at[column_slot(k), core, h]
        return remote(ref, ref, s.sent.at[0], s.z_recv.at[h, k], {"sp": sp + n_x, "tp": tp})

    def x_copy(k, d, h):
        ref = kvb.at[column_slot(k), core, h]
        return remote(ref, ref, s.sent.at[0], s.x_recv.at[k, d - 1],
                      {"sp": z * n_x + lax.rem(x + d, n_x), "tp": tp})

    def c_copy(k, h):
        ref = kvb.at[column_slot(k), core, h]
        return remote(ref, ref, s.sent.at[0], s.c_recv.at[k], to_sibling)

    def d_copy(k, d):
        ref = kvb.at[row_slot(k, d), core]
        return remote(ref, ref, s.sent.at[0], s.d_recv.at[k, d - 1], to_sibling)

    def wait_column(k):
        arrival(kvb.at[column_slot(k), other], s.c_recv.at[k]).wait_recv()

    def wait_row(k, d):
        arrival(kvb.at[row_slot(k, d), other], s.d_recv.at[k, d - 1]).wait_recv()

    def sends_row(k, d):
        return (k > 0) | (x + d < n_x)

    def takes_row(k, d):
        return (k > 0) | (x >= d)

    def detoured(k, h, to):
        if h == DETOURS[0]:
            return (k >= 2) & (to > 0)
        return (k >= 3) & (to == 0)

    def pass_on(k, h):
        @pl.when(z + 1 < n_z)
        def _():
            z_copy(k, h).start()

        for d in range(1, n_x):
            to = lax.rem(x + d, n_x)

            @pl.when(sends_row(k, d) & ~detoured(k, h, to) if h in DETOURS else sends_row(k, d))
            def _():
                x_copy(k, d, h).start()

        c_copy(k, h).start()

    def take_column(k, h):
        arrival(kvb.at[column_slot(k), core, h], s.z_recv.at[h, k - 1]).wait_recv()
        pass_on(k, h)

    def detour_copy(k, d, i):
        ref = kvb.at[row_slot(k, d), core, DETOURS[i]]
        return remote(ref, ref, s.sent.at[0], s.r_recv.at[i, k - 1, d - 1], {"sp": sp + n_x, "tp": tp})

    def passes_detour(k, i):
        return (z + 1 < n_z) & detoured(k + 1, DETOURS[i], x)

    def take_row(k, d):
        own = kvb.at[row_slot(k, d), core]
        shorter = functools.reduce(jnp.logical_or, [detoured(k, h, x) for h in DETOURS])

        @pl.when(~shorter)
        def _():
            arrival(own, s.x_recv.at[k, d - 1]).wait_recv()

        @pl.when(shorter)
        def _():
            arrival(own.at[pl.ds(0, pieces - 1)], s.x_recv.at[k, d - 1]).wait_recv()

        for i, h in enumerate(DETOURS):
            @pl.when(detoured(k, h, x))
            def _():
                arrival(own.at[h], s.r_recv.at[i, k - 2, d - 1]).wait_recv()

            @pl.when(passes_detour(k, i))
            def _():
                detour_copy(k, d, i).start()

        d_copy(k, d).start()

    def take_second(lo, hi):
        for h in range(lo, hi):
            @pl.when(z >= 2)
            def _():
                take_column(2, h)

    def take_first(h):
        @pl.when(z >= 1)
        def _():
            take_column(1, h)

    start(wcol_local)
    start(wcol_sends)
    column_local.start()
    for name in ("norm_gain", "kv_gain", "kv_latent", "rope"):
        getattr(loads, name).wait()
    for h in range(pieces):
        feature_wait(h)
        if h == pieces - 1:
            column_start()
        normalize(h)
        normed_copy(h).start()
        latents(h)
        pass_on(0, h)
        if 1 <= h <= pieces // 2:
            take_first(h - 1)

    loads.query_latent.wait()
    loads.q_gain.wait()
    own_normed = normed[core].reshape(half, n_tp * block)
    latq[core] = rms_rows(dot(own_normed, w.query_latent[...]), small.q_gain[...]).astype(BF16)
    latq_copy = remote(latq.at[core], latq.at[core], s.sent.at[0], s.q_sems.at[0], to_sibling)
    latq_copy.start()

    arrival(normed.at[other], s.n_sems.at[0]).wait_recv()

    if n_z > 2:
        take_second(0, 1)

    def all_normed():
        return normed[...].reshape(rows, n_tp * block)

    for name in MERGED:
        getattr(loads, name).wait()
    if merged:
        qkv = dot(all_normed(), s.w_qkv[...]).astype(BF16)
    else:
        qkv = jnp.concatenate([dot(all_normed(), getattr(w, name)[...]) for name in MERGED], axis=1).astype(BF16)
    local_kv[...] = qkv[:, : 2 * kv_width]
    queries[...] = qkv[:, 2 * kv_width :]
    tail = local_kv.at[pl.ds(rows - WINDOW, WINDOW)]
    halo_copy = remote(tail, halo, s.sent.at[0], s.halo_sem.at[0], {"sp": sp + 1, "tp": tp})
    turn_copy = remote(tail, turn, s.sent.at[0], s.halo_sem.at[1], {"sp": z * n_x, "tp": tp})
    relay_copy = remote(turn, halo, s.sent.at[0], s.halo_sem.at[0], {"sp": sp + n_x, "tp": tp})

    @pl.when((x + 1 == n_x) & (z + 1 < n_z))
    def _():
        turn_copy.start()

    take_first(pieces - 2)

    def queries_up():
        arrival(latq.at[other], s.q_sems.at[0]).wait_recv()
        loads.content.wait()
        loads.rotary.wait()
        latent_query = latq[...].reshape(rows, latent)
        content = dot(latent_query, w.content[...])
        rotary = dot(latent_query, w.rotary[...])
        cos_all, sin_all = cosine[...].reshape(rows, ROPE), sine[...].reshape(rows, ROPE)
        padding = jnp.zeros((rows, LANES - ROPE), F32)
        for h in range(lat_heads):
            turned = rotary[:, h * ROPE : (h + 1) * ROPE]
            turned = turned * cos_all + swap_halves(turned) * sin_all
            q_full[h, :NOPE, :] = content[:, h * NOPE : (h + 1) * NOPE].T.astype(BF16)
            q_full[h, NOPE:, :] = jnp.concatenate([turned, padding], axis=1).T.astype(BF16)
        loads.key_up.wait()
        loads.value_up.wait()

    def attend(slot, diagonal, which=None):
        if which is None:
            source = kvb[slot, :, :, :piece, :].reshape(rows, latent)
            rope_part = rope_rows(slot)
        else:
            source = kvb[slot, which, :, :piece, :].reshape(half, latent)
            rope_part = rope_rows(slot, [which])
        both = dot(source, s.up[...]).astype(BF16)
        keys, values = both[:, : lat_heads * NOPE], both[:, lat_heads * NOPE :]
        heads = range(lat_heads)
        scores = []
        for h in heads:
            key = jnp.concatenate([keys[:, h * NOPE : (h + 1) * NOPE], rope_part], axis=1)
            scores.append(dot(key, q_full[h]) * ((NOPE + ROPE) ** (-0.5) * LOG2_E))
        if diagonal:
            live = (lax.broadcasted_iota(jnp.int32, (rows, rows), 0)
                    <= lax.broadcasted_iota(jnp.int32, (rows, rows), 1))
            scores = [jnp.where(live, part, NEGATIVE) for part in scores]
        weights, fades = [], []
        for h in heads:
            peak = jnp.max(scores[h], axis=0, keepdims=True)
            if not diagonal:
                before = top[h]
                peak = jnp.maximum(peak, before)
                fades.append(jnp.exp2(before - peak))
            top[h] = peak
            weights.append(jnp.exp2(scores[h] - peak))
        for h in heads:
            weight_sum = jnp.sum(weights[h], axis=0, keepdims=True)
            part = dot_tl(values[:, h * VDIM : (h + 1) * VDIM], weights[h].astype(BF16))
            if not diagonal:
                weight_sum = total[h] * fades[h] + weight_sum
                part = acc[h] * fades[h] + part
            total[h] = weight_sum
            acc[h] = part

    def take_halo():
        @pl.when(sp > 0)
        def _():
            arrival(halo, s.halo_sem.at[0]).wait_recv()

        @pl.when(sp == 0)
        def _():
            halo[...] = jnp.zeros(halo.shape, BF16)

    def window(blocks):
        row = lax.broadcasted_iota(jnp.int32, (2 * WINDOW, WINDOW), 1)
        column = lax.broadcasted_iota(jnp.int32, (2 * WINDOW, WINDOW), 0)
        offset = row + WINDOW - column
        in_band = (offset >= 0) & (offset < WINDOW)
        in_band = jnp.concatenate([in_band] * group, axis=1)
        later = jnp.concatenate([(sp > 0) | (column >= WINDOW)] * group, axis=1)
        units = [(n, g) for n in blocks for g in range(kv_heads)]
        scores, values, sinks, weights = [], [], [], []
        for n, g in units:
            at = slice(n * WINDOW, (n + 1) * WINDOW)
            earlier = halo[...] if n == 0 else local_kv[(n - 1) * WINDOW : n * WINDOW]
            band = jnp.concatenate([earlier, local_kv[at]], axis=0)
            valid = in_band & later if n == 0 else in_band
            key = band[:, g * HEAD : (g + 1) * HEAD]
            values.append(band[:, kv_width + g * HEAD : kv_width + (g + 1) * HEAD])
            members = range(g * group, (g + 1) * group)
            query = jnp.concatenate([queries[at, q * HEAD : (q + 1) * HEAD] for q in members], axis=0)
            sinks.append(jnp.concatenate([jnp.full((1, WINDOW), small.sinks[0, q], F32) for q in members], axis=1))
            scores.append(jnp.where(valid, dot_t(key, query) * HEAD ** (-0.5), NEGATIVE))
        for u in range(len(units)):
            peak = jnp.maximum(jnp.max(scores[u], axis=0, keepdims=True), sinks[u])
            part = jnp.exp(scores[u] - peak)
            bottom = jnp.sum(part, axis=0, keepdims=True) + jnp.exp(sinks[u] - peak)
            weights.append((part * (1.0 / bottom)).astype(BF16))
        mixed = [dot_tl(values[u], weights[u]) for u in range(len(units))]
        for b, n in enumerate(blocks):
            heads = [
                mixed[b * kv_heads + g][:, i * WINDOW : (i + 1) * WINDOW]
                for g in range(kv_heads) for i in range(group)
            ]
            winb[core, n * WINDOW : (n + 1) * WINDOW, :] = jnp.concatenate(heads, axis=0).T.astype(BF16)

    def win_copy(i):
        ref = winb.at[core, win_rows[i]]
        return remote(ref, ref, s.sent.at[0], s.win_recv.at[i], to_sibling)

    win_rows = (pl.ds(WINDOW, rows - WINDOW), pl.ds(0, WINDOW))

    def window_part(j, at):
        return dot(winb[0, at], wcol[0, j]) + dot(winb[1, at], wcol[1, j])

    def part_copy(d, at):
        return remote(psend.at[d - 1, at], precv.at[d - 1, at], s.sent.at[0], s.p_recv.at[d - 1],
                      {"sp": sp, "tp": lax.rem(y + d, n_y) * 2 + core})

    def window_parts(i):
        at = win_rows[i]
        arrival(winb.at[other, at], s.win_recv.at[i]).wait_recv()
        for d in range(1, n_y):
            psend[d - 1, at] = window_part(lax.rem(y + d, n_y), at).astype(BF16)
            part_copy(d, at).start()

    def gate(b):
        name = WEIGHTS[10 + b]
        getattr(loads, name).wait()

        def step(i, _):
            at = pl.ds(pl.multiple_of(i * 256, LANES), 256)
            gates[b, :, at] = jax.nn.sigmoid(dot(all_normed(), getattr(w, name)[:, at]))
            return 0

        lax.fori_loop(0, block // 256, step, 0)

    def take_rows(k):
        for d in range(1, n_x):
            pl.when(takes_row(k, d))(functools.partial(take_row, k, d))

    def attend_row(k, d):
        wait_row(k, d)
        attend(row_slot(k, d), False)

    loads.sinks.wait()
    window(range(1, rows // WINDOW))
    win_copy(0).start()
    take_first(pieces - 1)
    queries_up()
    if n_z > 2:
        take_second(1, pieces // 2)
    pltpu.make_async_copy(wcol.at[core], wcol.at[core], s.w_sems.at[0]).wait()
    arrival(wcol.at[other], s.w_sems.at[1]).wait_recv()
    window_parts(0)
    take_rows(0)
    wait_column(0)
    attend(sp, True)
    if n_z > 2:
        take_second(pieces // 2, pieces - 1)

    @pl.when(x + 1 < n_x)
    def _():
        halo_copy.start()

    @pl.when((x == 0) & (z + 1 < n_z))
    def _():
        arrival(turn, s.halo_sem.at[1]).wait_recv()
        relay_copy.start()


    def take_pieces(k, lo, hi):
        @pl.when(z >= k)
        def _():
            for h in range(lo, hi):
                take_column(k, h)

    def first_window():
        take_halo()
        window(range(1))
        win_copy(1).start()

    def last_parts():
        window_parts(1)

    def attend_halves(slot, wait):
        def halves(i, _):
            @pl.when(i == 1)
            def _():
                wait()

            attend(slot, False, jnp.where(i == 0, core, other))
            return 0

        lax.fori_loop(0, 2, halves, 0)

    def step(k, _):
        @pl.when(k == 4 - parity)
        def _():
            pair_forward()

        @pl.when((z >= k - 1) & (k < n_z))
        def _():
            wait_column(k - 1)
            attend(column_slot(k - 1), False)

        @pl.when((z >= k - 1) & (k == n_z))
        def _():
            attend_halves(column_slot(k - 1), functools.partial(wait_column, k - 1))

        @pl.when(k == 2)
        def _():
            take_pieces(k, pieces - 1, pieces)

        pl.when(k == 4)(last_parts)

        @pl.when(k > 2)
        def _():
            pl.when(x == 0)(functools.partial(take_pieces, k, 0, 1))
            take_pieces(k, 1, pieces // 2)

        for d in range(1, n_x):
            @pl.when((z >= k - 2) & takes_row(k - 2, d))
            def _():
                attend_row(k - 2, d)

        @pl.when(k > 2)
        def _():
            take_pieces(k, pieces // 2, pieces - 1)

        pl.when(k == 3)(first_window)

        @pl.when(k > 2)
        def _():
            take_pieces(k, pieces - 1, pieces)


        @pl.when(z >= k - 1)
        def _():
            take_rows(k - 1)

        @pl.when(x > 0)
        def _():
            take_pieces(k + 1, 0, 1)

        return 0

    lax.fori_loop(2, max(n_z, 4) + 1, step, 0)

    @pl.when(z == n_z - 1)
    def _():
        for d in range(1, n_x):
            @pl.when(takes_row(n_z - 1, d))
            def _():
                attend_halves(row_slot(n_z - 1, d), functools.partial(wait_row, n_z - 1, d))


    def gather(part):
        own = lat.at[tp, part]
        sends = [
            remote(own, own, s.sent.at[1], s.y_recv.at[part, d - 1],
                   {"sp": sp, "tp": lax.rem(y + d, n_y) * 2 + core})
            for d in range(1, n_y)
        ]
        sends.append(remote(own, own, s.sent.at[1], s.s_recv.at[part], to_sibling))
        return sends

    def forward(part):
        for d in range(1, n_y):
            ref = lat.at[lax.rem(y + n_y - d, n_y) * 2 + core, part]
            arrival(ref, s.y_recv.at[part, d - 1]).wait_recv()
            remote(ref, ref, s.sent.at[1], s.s_recv.at[part], to_sibling).start()

    def arrived(part):
        arrival(lat.at[pl.ds(0, n_y), part], s.s_recv.at[part]).wait_recv()

    for part in range(out_parts):
        at = slice(part * out_rows, (part + 1) * out_rows)
        for h in range(lat_heads):
            lat[tp, part, :, h * VDIM : (h + 1) * VDIM] = (
                acc[h, :, at] * (1.0 / total[h, :, at])).T.astype(BF16)
        start(gather(part))
    gate(0)
    gate(1)
    window_branch = window_part(y, pl.ds(0, rows))
    for d in range(1, n_y):
        arrival(precv.at[d - 1], s.p_recv.at[d - 1]).wait_recv()
        window_branch = window_branch + precv[d - 1].astype(F32)
    gates[0] = gates[0] * window_branch
    column_local.wait()
    arrival(columns.at[sibling], s.col_recv.at[0]).wait_recv()
    for d in range(1, n_y):
        base = lax.rem(y + n_y - d, n_y) * 2
        if paired:
            arrival(columns.at[base + 1 - parity], s.pair_recv.at[d - 1]).wait_recv()
        else:
            arrival(columns.at[pl.ds(base, 2)], s.col_recv.at[d]).wait_recv()
    def leave(ref, send):
        remote(ref, ref, send, send, to_sibling).wait_send()

    leave(ownf.at[pl.ds(0, half)], s.sent.at[0])
    for d in range(1, n_y):
        leave(ownf, s.sent.at[0])
    leave(normed.at[core], s.sent.at[0])
    latq_copy.wait_send()
    leave(wcol.at[core], s.sent.at[0])
    leave(columns.at[tp], s.sent.at[0])

    @when_across
    def _():
        for d in range(1, n_y):
            leave(columns.at[pl.ds(0, 2)], s.sent.at[0])

    if paired:
        for d in range(1, n_y):
            pair_copy(d).wait_send()
    for i in range(2):
        win_copy(i).wait_send()
    for d in range(1, n_y):
        leave(psend.at[d - 1], s.sent.at[0])

    @pl.when((x + 1 < n_x) | (z + 1 < n_z))
    def _():
        halo_copy.wait_send()

    @pl.when((x == 0) & (z + 1 < n_z))
    def _():
        relay_copy.wait_send()

    def drain(k, _):
        @pl.when(z >= k)
        def _():
            own = kvb.at[column_slot(k), core]

            @pl.when(z + 1 < n_z)
            def _():
                leave(own, s.sent.at[0])

            leave(own, s.sent.at[0])
            for d in range(1, n_x):
                to = lax.rem(x + d, n_x)
                fewer = [detoured(k, h, to) for h in DETOURS]

                @pl.when(sends_row(k, d) & ~(fewer[0] | fewer[1]))
                def _():
                    leave(own, s.sent.at[0])

                @pl.when(fewer[0] | fewer[1])
                def _():
                    leave(own.at[pl.ds(0, pieces - 1)], s.sent.at[0])

                for i in range(2):
                    @pl.when(takes_row(k, d) & passes_detour(k, i))
                    def _():
                        detour_copy(k, d, i).wait_send()

                @pl.when(takes_row(k, d))
                def _():
                    leave(own, s.sent.at[0])

        return 0

    lax.fori_loop(0, n_z, drain, 0)

    for part in range(out_parts):
        at = slice(part * out_rows, (part + 1) * out_rows)
        forward(part)
        arrived(part)
        latent_branch = jnp.zeros((out_rows, block), F32)
        for j in range(n_tp):
            latent_branch = latent_branch + dot(lat[j, part], columns[j])
        out[at, :] = (gates[0, at] + gates[1, at] * latent_branch).astype(BF16)

    for _ in range(n_y + n_y - 1):
        leave(lat.at[tp], s.sent.at[1])


def on_device(dims, features, norm_gain, w_query, w_key, w_value, head_sinks, w_query_latent,
              w_kv_latent, w_rope_key, query_latent_gain, kv_latent_gain, w_query_content,
              w_query_rotary, w_key_up, w_value_up, w_branch_window, w_branch_latent,
              w_gate_window, w_gate_latent):
    n_sp, n_tp, n_x = dims
    n_z, n_y = n_sp // n_x, n_tp // 2
    rows, block = features.shape
    width = norm_gain.shape[0]
    latent = w_kv_latent.shape[1]
    lat_heads = w_key_up.shape[1] // NOPE
    half_width = ROPE // 2
    entry = np.arange(ROPE, dtype=np.int32) % half_width
    frequency = (np.float32(THETA) ** (-entry.astype(np.float32) / np.float32(half_width))).astype(np.float32)[None, :]
    weights = (w_kv_latent, w_rope_key.T, w_key, w_value, w_query, w_query_latent, w_query_content,
               w_query_rotary, w_key_up, w_value_up, w_gate_window, w_gate_latent)
    smalls = (norm_gain[None, :], head_sinks[None, :], query_latent_gain[None, :], kv_latent_gain[None, :],
              jnp.asarray(frequency))
    branch_rows = w_branch_window.shape[0]
    pieces = PIECES
    piece = rows // 2 // pieces
    out_parts = rows // LANES
    merge = w_key.shape[1] % LANES == 0
    hbm = pl.BlockSpec(memory_space=pl.ANY)
    dma = pltpu.SemaphoreType.DMA
    vm = pltpu.VMEM
    scratch = dict(
        **{"small_" + n: (pltpu.SMEM if n == "sinks" else vm)(a.shape, F32) for n, a in zip(SMALL, smalls)},
        **{"w_" + n: vm(a.shape, BF16) for n, a in zip(WEIGHTS, weights) if not (merge and n in MERGED or n in UP)},
        up=vm((latent, w_key_up.shape[1] + w_value_up.shape[1]), BF16),
        **(dict(w_qkv=vm((width, 2 * w_key.shape[1] + w_query.shape[1]), BF16)) if merge else {}),
        ownf=vm((rows, block), BF16),
        feat=vm((n_tp, rows // 2, block), BF16),
        normed=vm((2, pieces, piece, width), BF16),
        latq=vm((2, rows // 2, latent), BF16),
        wcol=vm((2, n_y, branch_rows, block), BF16),
        columns=vm((n_tp, w_branch_latent.shape[0], block), BF16),
        psend=vm((n_y - 1, rows, block), BF16),
        precv=vm((n_y - 1, rows, block), BF16),
        kvb=vm((n_sp, 2, pieces, piece + SUBLANES, latent), BF16),
        local_kv=vm((rows, 2 * w_key.shape[1]), BF16),
        halo=vm((WINDOW, 2 * w_key.shape[1]), BF16),
        turn=vm((WINDOW, 2 * w_key.shape[1]), BF16),
        queries=vm((rows, w_query.shape[1]), BF16),
        q_full=vm((lat_heads, NOPE + LANES, rows), BF16),
        gates=vm((2, rows, block), F32),
        winb=vm((2, rows, w_query.shape[1]), BF16),
        lat=vm((n_tp, out_parts, rows // out_parts, lat_heads * VDIM), BF16),
        top=vm((lat_heads, 1, rows), F32),
        total=vm((lat_heads, 1, rows), F32),
        acc=vm((lat_heads, VDIM, rows), F32),
        cosine=vm((2, pieces, piece, ROPE), F32),
        sine=vm((2, pieces, piece, ROPE), F32),
        own_sem=dma((2,)),
        sent=dma((2,)),
        small_sem=dma((len(SMALL),)),
        w_sem=dma((len(weights),)),
        f_recv=dma((pieces,)),
        n_sems=dma((1,)),
        q_sems=dma((1,)),
        w_sems=dma((2,)),
        col_own=dma((1,)),
        col_recv=dma((n_y,)),
        pair_recv=dma((n_y - 1,)),
        halo_sem=dma((2,)),
        win_recv=dma((2,)),
        p_recv=dma((n_y - 1,)),
        y_recv=dma((out_parts, n_y - 1)),
        s_recv=dma((out_parts,)),
        z_recv=dma((pieces, n_z - 1)),
        r_recv=dma((2, n_z - 2, n_x - 1)),
        x_recv=dma((n_z, n_x - 1)),
        c_recv=dma((n_z,)),
        d_recv=dma((n_z, n_x - 1)),
    )
    return pl.pallas_call(
        functools.partial(kernel, dims, tuple(scratch)),
        out_shape=pltpu.VMEM((rows, block), BF16),
        in_specs=[hbm] * (1 + len(smalls) + len(weights) + 2),
        out_specs=pl.BlockSpec(memory_space=pltpu.VMEM),
        scratch_shapes=list(scratch.values()),
        compiler_params=pltpu.CompilerParams(
            collective_id=0, has_side_effects=True, vmem_limit_bytes=60 * 1024 * 1024
        ),
    )(features, *smalls, *weights, w_branch_window, w_branch_latent)


def solution(mesh):
    n_sp, n_tp = mesh.shape["sp"], mesh.shape["tp"]
    n_x = 1
    while n_sp % (2 * n_x) == 0 and 8 * n_x * n_x <= n_sp:
        n_x *= 2
    return jax.shard_map(
        functools.partial(on_device, (n_sp, n_tp, n_x)),
        mesh=mesh,
        in_specs=(
            P("sp", "tp"),
            P(),
            P(None, "tp"),
            P(None, "tp"),
            P(None, "tp"),
            P("tp"),
            P(),
            P(),
            P(),
            P(),
            P(),
            P(None, "tp"),
            P(None, "tp"),
            P(None, "tp"),
            P(None, "tp"),
            P("tp", None),
            P("tp", None),
            P(None, "tp"),
            P(None, "tp"),
        ),
        out_specs=P("sp", "tp"),
        check_vma=False,
    )
```

```python
import functools
import types

import jax
import jax.numpy as jnp
import numpy as np
from jax import lax
from jax.experimental import pallas as pl
from jax.experimental.pallas import tpu as pltpu
from jax.sharding import PartitionSpec as P

HEAD = 64
WINDOW = 128
NOPE = 128
ROPE = 64
VDIM = 128


EPS = 1e-06
THETA = 10000.0
NEGATIVE = -1e30
LANES = 128
LOG2_E = 1.4426950408889634
MESH = pl.DeviceIdType.MESH
BF16 = jnp.bfloat16
F32 = jnp.float32
PIECES = 4
SUBLANES = 8
DETOURS = (0, PIECES - 1)


def dot(left, right):
    return jnp.dot(left, right, preferred_element_type=F32)


def dot_t(left, right):
    return lax.dot_general(left, right, (((1,), (1,)), ((), ())), preferred_element_type=F32)


def dot_tl(left, right):
    return lax.dot_general(left, right, (((0,), (0,)), ((), ())), preferred_element_type=F32)


def rms_rows(rows, gain):
    return rows * lax.rsqrt(jnp.mean(rows * rows, axis=-1, keepdims=True) + EPS) * gain


def swap_halves(rows):
    half = rows.shape[1] // 2
    return jnp.concatenate([rows[:, half:], rows[:, :half]], axis=1)


SMALL = ("norm_gain", "sinks", "q_gain", "kv_gain", "frequency")
WEIGHTS = (
    "kv_latent", "rope", "key", "value", "query", "query_latent", "content", "rotary",
    "key_up", "value_up", "gate_window", "gate_latent",
)
def bundle(names, values):
    return types.SimpleNamespace(**dict(zip(names, values)))


UP = ("key_up", "value_up")
MERGED = ("key", "value", "query")


def kernel(dims, names, *refs):
    n_sp, n_tp, n_x = dims
    n_z, n_y = n_sp // n_x, n_tp // 2
    features = refs[0]
    small_hbm = bundle(SMALL, refs[1:6])
    w_hbm = bundle(WEIGHTS, refs[6:18])
    window_hbm, latent_hbm = refs[18:20]
    out = refs[20]
    s = bundle(names, refs[21:])
    small = bundle(SMALL, [getattr(s, "small_" + name) for name in SMALL])
    merged = "w_qkv" in names
    kept = [name for name in WEIGHTS if "w_" + name in names]
    w = bundle(kept, [getattr(s, "w_" + name) for name in kept])
    ownf, feat, normed = s.ownf, s.feat, s.normed
    turn = s.turn
    kvb, local_kv, halo, queries, q_full, latq = s.kvb, s.local_kv, s.halo, s.queries, s.q_full, s.latq
    gates, winb, lat, top, total, acc = s.gates, s.winb, s.lat, s.top, s.total, s.acc
    wcol, columns, psend, precv = s.wcol, s.columns, s.psend, s.precv
    cosine, sine = s.cosine, s.sine

    sp, tp = lax.axis_index("sp"), lax.axis_index("tp")
    z, x = sp // n_x, lax.rem(sp, n_x)
    y, core = tp // 2, lax.rem(tp, 2)
    other = 1 - core
    sibling = y * 2 + other
    rows, block = features.shape
    half = rows // 2
    pieces = normed.shape[1]
    piece = half // pieces
    lat_heads = w_hbm.key_up.shape[1] // NOPE
    kv_width = w_hbm.key.shape[1]
    kv_heads = kv_width // HEAD
    group = w_hbm.query.shape[1] // kv_width
    latent = w_hbm.kv_latent.shape[1]
    out_parts = lat.shape[1]
    out_rows = rows // out_parts

    def remote(src, dst, send, recv, where):
        return pltpu.make_async_remote_copy(
            src_ref=src, dst_ref=dst, send_sem=send, recv_sem=recv,
            device_id=where, device_id_type=MESH,
        )

    to_sibling = {"sp": sp, "tp": sibling}

    def arrival(ref, recv):
        return remote(ref, ref, recv, recv, to_sibling)

    def start(copies):
        for copy in copies:
            copy.start()

    def own_rows(c, h):
        return ownf.at[pl.ds(pl.multiple_of(c * half + h * piece, 16), piece)]

    def feat_rows(j, h):
        return feat.at[j, pl.ds(h * piece, piece)]

    barrier = pltpu.get_barrier_semaphore()

    def greet(where):
        pl.semaphore_signal(barrier, inc=1, device_id=where, device_id_type=MESH)

    for d in range(1, n_tp):
        greet({"sp": sp, "tp": lax.rem(tp + d, n_tp)})
    for d in range(1, n_x):
        greet({"sp": z * n_x + lax.rem(x + d, n_x), "tp": tp})

    @pl.when(z + 1 < n_z)
    def _():
        greet({"sp": sp + n_x, "tp": tp})

    @pl.when(z > 0)
    def _():
        greet({"sp": sp - n_x, "tp": tp})

    own_load = [
        pltpu.make_async_copy(features, ownf, s.own_sem.at[0]),
        pltpu.make_async_copy(
            features.at[pl.ds(pl.multiple_of(core * half, 16), half)], feat.at[tp], s.own_sem.at[1]),
    ]
    start(own_load)
    loads = bundle(SMALL, [
        pltpu.make_async_copy(getattr(small_hbm, name), getattr(small, name), s.small_sem.at[i])
        for i, name in enumerate(SMALL)
    ])
    for name in SMALL:
        getattr(loads, name).start()

    one, none = jnp.int32(1), jnp.int32(0)
    pl.semaphore_wait(
        barrier,
        n_tp - 1 + n_x - 1
        + jnp.where(z + 1 < n_z, one, none) + jnp.where(z > 0, one, none),
    )

    def feature_sends(h):
        sends = []
        for d in range(1, n_y):
            for c in range(2):
                sends.append(remote(
                    own_rows(c, h), feat_rows(tp, h), s.sent.at[0], s.f_recv.at[h],
                    {"sp": sp, "tp": lax.rem(y + d, n_y) * 2 + c}))
        sends.append(remote(
            own_rows(other, h), feat_rows(tp, h), s.sent.at[0], s.f_recv.at[h], to_sibling))
        return sends

    def feature_wait(h):
        arrival(feat.at[pl.ds(0, n_tp - 1), pl.ds(h * piece, piece)], s.f_recv.at[h]).wait_recv()

    for copy in own_load:
        copy.wait()
    for h in range(pieces):
        start(feature_sends(h))

    first = 0
    slots = [i for i, name in enumerate(WEIGHTS) if name in kept and name not in UP]
    slots += [WEIGHTS.index(UP[0])] + [WEIGHTS.index(MERGED[0])] * merged
    for i, name in enumerate(WEIGHTS):
        source = getattr(w_hbm, name)
        if name == "key_up":
            to = s.up.at[:, pl.ds(0, lat_heads * NOPE)]
        elif name == "value_up":
            to = s.up.at[:, pl.ds(lat_heads * NOPE, lat_heads * VDIM)]
        elif name in kept:
            to = getattr(w, name)
        else:
            to = s.w_qkv.at[:, pl.ds(first, source.shape[1])]
            first += source.shape[1]
        shared = WEIGHTS.index(UP[0]) if name in UP else i if name in kept else WEIGHTS.index(MERGED[0])
        copy = pltpu.make_async_copy(source, to, s.w_sem.at[slots.index(shared)])
        copy.start()
        setattr(loads, name, copy)

    def window_columns():
        local, sends = [], []
        for j in range(n_y):
            local.append(pltpu.make_async_copy(
                window_hbm.at[:, pl.ds(pl.multiple_of((j * 2 + core) * block, LANES), block)],
                wcol.at[core, j], s.w_sems.at[0]))
            sends.append(remote(
                window_hbm.at[:, pl.ds(pl.multiple_of((j * 2 + other) * block, LANES), block)],
                wcol.at[core, j], s.sent.at[0], s.w_sems.at[1], to_sibling))
        return local, sends

    paired = n_z % 2 == 0
    parity = lax.rem(z, 2)
    partner = {"sp": sp + n_x * (1 - 2 * parity), "tp": tp}

    def column_send(to, d):
        return remote(
            latent_hbm.at[:, pl.ds(pl.multiple_of(to * block, LANES), block)],
            columns.at[tp], s.sent.at[0], s.col_recv.at[d], {"sp": sp, "tp": to})

    def when_across(act):
        if paired:
            pl.when(core == parity)(act)
        else:
            act()

    def column_start():
        column_send(sibling, 0).start()

        @when_across
        def _():
            for d in range(1, n_y):
                for c in range(2):
                    column_send(lax.rem(y + d, n_y) * 2 + c, d).start()

    def pair_copy(d):
        ref = columns.at[lax.rem(y + n_y - d, n_y) * 2 + parity]
        return remote(ref, ref, s.sent.at[0], s.pair_recv.at[d - 1], partner)

    def pair_forward():
        if paired:
            for d in range(1, n_y):
                source = lax.rem(y + n_y - d, n_y) * 2 + parity
                arrival(columns.at[source], s.col_recv.at[d]).wait_recv()
                pair_copy(d).start()

    column_local = pltpu.make_async_copy(
        latent_hbm.at[:, pl.ds(pl.multiple_of(tp * block, LANES), block)],
        columns.at[tp], s.col_own.at[0])

    wcol_local, wcol_sends = window_columns()

    loads.frequency.wait()
    positions = (sp * rows + lax.broadcasted_iota(jnp.int32, (rows, ROPE), 0)).astype(F32)
    angles = positions * small.frequency[...]
    lane = lax.broadcasted_iota(jnp.int32, (rows, ROPE), 1)
    cosine[...] = jnp.cos(angles).reshape(cosine.shape)
    turned = jnp.sin(angles)
    sine[...] = jnp.where(lane < ROPE // 2, -turned, turned).reshape(sine.shape)

    def normalize(h):
        squares = jnp.zeros((piece, 1), F32)
        part = slice(h * piece, (h + 1) * piece)
        for j in range(n_tp):
            values = feat[j, part].astype(F32)
            squares = squares + jnp.sum(values * values, axis=-1, keepdims=True)
        scale = lax.rsqrt(squares / (n_tp * block) + EPS)
        for j in range(n_tp):
            span = slice(j * block, (j + 1) * block)
            values = feat[j, part].astype(F32) * scale * small.norm_gain[:, span]
            normed[core, h, :, span] = values.astype(BF16)

    def normed_copy(h):
        return remote(normed.at[core, h], normed.at[core, h], s.sent.at[0], s.n_sems.at[0], to_sibling)

    def latents(h):
        own = normed[core, h]
        rope = dot_t(own, w.rope[...])
        rope = rope * cosine[core, h] + swap_halves(rope) * sine[core, h]
        rope = jnp.concatenate([rope[: piece // 2], rope[piece // 2 :]], axis=1)
        rope = [rope[i : i + SUBLANES] for i in range(0, piece // 2, SUBLANES)]
        rope.append(jnp.zeros((SUBLANES, latent - len(rope) * LANES), F32))
        kvb[sp, core, h, :piece, :] = rms_rows(dot(own, w.kv_latent[...]), small.kv_gain[...]).astype(BF16)
        kvb[sp, core, h, piece:, :] = jnp.concatenate(rope, axis=1).astype(BF16)

    def rope_rows(slot, halves=range(2)):
        parts = []
        for c in halves:
            for h in range(pieces):
                packed = kvb[slot, c, h, piece:, :].astype(F32)
                pair = jnp.concatenate(
                    [packed[:, i * LANES : (i + 1) * LANES] for i in range(piece // 2 // SUBLANES)], axis=0)
                parts += [pair, pltpu.roll(pair, ROPE, 1)]
        return jnp.concatenate(parts, axis=0).astype(BF16)

    def column_slot(k):
        return (z - k) * n_x + x

    def row_slot(k, d):
        return (z - k) * n_x + lax.rem(x + n_x - d, n_x)

    def z_copy(k, h):
        ref = kvb.at[column_slot(k), core, h]
        return remote(ref, ref, s.sent.at[0], s.z_recv.at[h, k], {"sp": sp + n_x, "tp": tp})

    def x_copy(k, d, h):
        ref = kvb.at[column_slot(k), core, h]
        return remote(ref, ref, s.sent.at[0], s.x_recv.at[k, d - 1],
                      {"sp": z * n_x + lax.rem(x + d, n_x), "tp": tp})

    def c_copy(k, h):
        ref = kvb.at[column_slot(k), core, h]
        return remote(ref, ref, s.sent.at[0], s.c_recv.at[k], to_sibling)

    def d_copy(k, d):
        ref = kvb.at[row_slot(k, d), core]
        return remote(ref, ref, s.sent.at[0], s.d_recv.at[k, d - 1], to_sibling)

    def wait_column(k):
        arrival(kvb.at[column_slot(k), other], s.c_recv.at[k]).wait_recv()

    def wait_row(k, d):
        arrival(kvb.at[row_slot(k, d), other], s.d_recv.at[k, d - 1]).wait_recv()

    def sends_row(k, d):
        return (k > 0) | (x + d < n_x)

    def takes_row(k, d):
        return (k > 0) | (x >= d)

    def detoured(k, h, to):
        if h == DETOURS[0]:
            return (k >= 2) & (to > 0)
        return (k >= 3) & (to == 0)

    def pass_on(k, h):
        @pl.when(z + 1 < n_z)
        def _():
            z_copy(k, h).start()

        for d in range(1, n_x):
            to = lax.rem(x + d, n_x)

            @pl.when(sends_row(k, d) & ~detoured(k, h, to) if h in DETOURS else sends_row(k, d))
            def _():
                x_copy(k, d, h).start()

        c_copy(k, h).start()

    def take_column(k, h):
        arrival(kvb.at[column_slot(k), core, h], s.z_recv.at[h, k - 1]).wait_recv()
        pass_on(k, h)

    def detour_copy(k, d, i):
        ref = kvb.at[row_slot(k, d), core, DETOURS[i]]
        return remote(ref, ref, s.sent.at[0], s.r_recv.at[i, k - 1, d - 1], {"sp": sp + n_x, "tp": tp})

    def passes_detour(k, i):
        return (z + 1 < n_z) & detoured(k + 1, DETOURS[i], x)

    def take_row(k, d):
        own = kvb.at[row_slot(k, d), core]
        shorter = functools.reduce(jnp.logical_or, [detoured(k, h, x) for h in DETOURS])

        @pl.when(~shorter)
        def _():
            arrival(own, s.x_recv.at[k, d - 1]).wait_recv()

        @pl.when(shorter)
        def _():
            arrival(own.at[pl.ds(0, pieces - 1)], s.x_recv.at[k, d - 1]).wait_recv()

        for i, h in enumerate(DETOURS):
            @pl.when(detoured(k, h, x))
            def _():
                arrival(own.at[h], s.r_recv.at[i, k - 2, d - 1]).wait_recv()

            @pl.when(passes_detour(k, i))
            def _():
                detour_copy(k, d, i).start()

        d_copy(k, d).start()

    def take_second(lo, hi):
        for h in range(lo, hi):
            @pl.when(z >= 2)
            def _():
                take_column(2, h)

    def take_first(h):
        @pl.when(z >= 1)
        def _():
            take_column(1, h)

    start(wcol_local)
    start(wcol_sends)
    column_local.start()
    for name in ("norm_gain", "kv_gain", "kv_latent", "rope"):
        getattr(loads, name).wait()
    for h in range(pieces):
        feature_wait(h)
        if h == pieces - 1:
            column_start()
        normalize(h)
        normed_copy(h).start()
        latents(h)
        pass_on(0, h)
        if 1 <= h <= pieces // 2:
            take_first(h - 1)

    loads.query_latent.wait()
    loads.q_gain.wait()
    own_normed = normed[core].reshape(half, n_tp * block)
    latq[core] = rms_rows(dot(own_normed, w.query_latent[...]), small.q_gain[...]).astype(BF16)
    latq_copy = remote(latq.at[core], latq.at[core], s.sent.at[0], s.q_sems.at[0], to_sibling)
    latq_copy.start()

    arrival(normed.at[other], s.n_sems.at[0]).wait_recv()

    if n_z > 2:
        take_second(0, 1)

    def all_normed():
        return normed[...].reshape(rows, n_tp * block)

    if merged:
        sem = s.w_sem.at[slots.index(WEIGHTS.index(MERGED[0]))]
        pltpu.make_async_copy(s.w_qkv, s.w_qkv, sem).wait()
    else:
        for name in MERGED:
            getattr(loads, name).wait()
    if merged:
        qkv = dot(all_normed(), s.w_qkv[...]).astype(BF16)
    else:
        qkv = jnp.concatenate([dot(all_normed(), getattr(w, name)[...]) for name in MERGED], axis=1).astype(BF16)
    local_kv[...] = qkv[:, : 2 * kv_width]
    queries[...] = qkv[:, 2 * kv_width :]
    tail = local_kv.at[pl.ds(rows - WINDOW, WINDOW)]
    halo_copy = remote(tail, halo, s.sent.at[0], s.halo_sem.at[0], {"sp": sp + 1, "tp": tp})
    turn_copy = remote(tail, turn, s.sent.at[0], s.halo_sem.at[1], {"sp": z * n_x, "tp": tp})
    relay_copy = remote(turn, halo, s.sent.at[0], s.halo_sem.at[0], {"sp": sp + n_x, "tp": tp})

    @pl.when((x + 1 == n_x) & (z + 1 < n_z))
    def _():
        turn_copy.start()

    take_first(pieces - 2)

    def queries_up():
        arrival(latq.at[other], s.q_sems.at[0]).wait_recv()
        loads.content.wait()
        loads.rotary.wait()
        latent_query = latq[...].reshape(rows, latent)
        content = dot(latent_query, w.content[...])
        rotary = dot(latent_query, w.rotary[...])
        cos_all, sin_all = cosine[...].reshape(rows, ROPE), sine[...].reshape(rows, ROPE)
        padding = jnp.zeros((rows, LANES - ROPE), F32)
        for h in range(lat_heads):
            turned = rotary[:, h * ROPE : (h + 1) * ROPE]
            turned = turned * cos_all + swap_halves(turned) * sin_all
            q_full[h, :NOPE, :] = content[:, h * NOPE : (h + 1) * NOPE].T.astype(BF16)
            q_full[h, NOPE:, :] = jnp.concatenate([turned, padding], axis=1).T.astype(BF16)
        pltpu.make_async_copy(s.up, s.up, s.w_sem.at[slots.index(WEIGHTS.index(UP[0]))]).wait()

    def attend(slot, diagonal, which=None):
        if which is None:
            source = kvb[slot, :, :, :piece, :].reshape(rows, latent)
            rope_part = rope_rows(slot)
        else:
            source = kvb[slot, which, :, :piece, :].reshape(half, latent)
            rope_part = rope_rows(slot, [which])
        both = dot(source, s.up[...]).astype(BF16)
        keys, values = both[:, : lat_heads * NOPE], both[:, lat_heads * NOPE :]
        heads = range(lat_heads)
        scores = []
        for h in heads:
            key = jnp.concatenate([keys[:, h * NOPE : (h + 1) * NOPE], rope_part], axis=1)
            scores.append(dot(key, q_full[h]) * ((NOPE + ROPE) ** (-0.5) * LOG2_E))
        if diagonal:
            live = (lax.broadcasted_iota(jnp.int32, (rows, rows), 0)
                    <= lax.broadcasted_iota(jnp.int32, (rows, rows), 1))
            scores = [jnp.where(live, part, NEGATIVE) for part in scores]
        weights, fades = [], []
        for h in heads:
            peak = jnp.max(scores[h], axis=0, keepdims=True)
            if not diagonal:
                before = top[h]
                peak = jnp.maximum(peak, before)
                fades.append(jnp.exp2(before - peak))
            top[h] = peak
            weights.append(jnp.exp2(scores[h] - peak))
        for h in heads:
            weight_sum = jnp.sum(weights[h], axis=0, keepdims=True)
            part = dot_tl(values[:, h * VDIM : (h + 1) * VDIM], weights[h].astype(BF16))
            if not diagonal:
                weight_sum = total[h] * fades[h] + weight_sum
                part = acc[h] * fades[h] + part
            total[h] = weight_sum
            acc[h] = part

    def take_halo():
        @pl.when(sp > 0)
        def _():
            arrival(halo, s.halo_sem.at[0]).wait_recv()

        @pl.when(sp == 0)
        def _():
            halo[...] = jnp.zeros(halo.shape, BF16)

    def window(blocks):
        row = lax.broadcasted_iota(jnp.int32, (2 * WINDOW, WINDOW), 1)
        column = lax.broadcasted_iota(jnp.int32, (2 * WINDOW, WINDOW), 0)
        offset = row + WINDOW - column
        in_band = (offset >= 0) & (offset < WINDOW)
        in_band = jnp.concatenate([in_band] * group, axis=1)
        later = jnp.concatenate([(sp > 0) | (column >= WINDOW)] * group, axis=1)
        units = [(n, g) for n in blocks for g in range(kv_heads)]
        scores, values, sinks, weights = [], [], [], []
        for n, g in units:
            at = slice(n * WINDOW, (n + 1) * WINDOW)
            earlier = halo[...] if n == 0 else local_kv[(n - 1) * WINDOW : n * WINDOW]
            band = jnp.concatenate([earlier, local_kv[at]], axis=0)
            valid = in_band & later if n == 0 else in_band
            key = band[:, g * HEAD : (g + 1) * HEAD]
            values.append(band[:, kv_width + g * HEAD : kv_width + (g + 1) * HEAD])
            members = range(g * group, (g + 1) * group)
            query = jnp.concatenate([queries[at, q * HEAD : (q + 1) * HEAD] for q in members], axis=0)
            sinks.append(jnp.concatenate([jnp.full((1, WINDOW), small.sinks[0, q], F32) for q in members], axis=1))
            scores.append(jnp.where(valid, dot_t(key, query) * HEAD ** (-0.5), NEGATIVE))
        for u in range(len(units)):
            peak = jnp.maximum(jnp.max(scores[u], axis=0, keepdims=True), sinks[u])
            part = jnp.exp(scores[u] - peak)
            bottom = jnp.sum(part, axis=0, keepdims=True) + jnp.exp(sinks[u] - peak)
            weights.append((part * (1.0 / bottom)).astype(BF16))
        mixed = [dot_tl(values[u], weights[u]) for u in range(len(units))]
        for b, n in enumerate(blocks):
            heads = [
                mixed[b * kv_heads + g][:, i * WINDOW : (i + 1) * WINDOW]
                for g in range(kv_heads) for i in range(group)
            ]
            winb[core, n * WINDOW : (n + 1) * WINDOW, :] = jnp.concatenate(heads, axis=0).T.astype(BF16)

    def win_copy(i):
        ref = winb.at[core, win_rows[i]]
        return remote(ref, ref, s.sent.at[0], s.win_recv.at[i], to_sibling)

    win_rows = (pl.ds(WINDOW, rows - WINDOW), pl.ds(0, WINDOW))

    def window_part(j, at):
        return dot(winb[0, at], wcol[0, j]) + dot(winb[1, at], wcol[1, j])

    def part_copy(d, at):
        return remote(psend.at[d - 1, at], precv.at[d - 1, at], s.sent.at[0], s.p_recv.at[d - 1],
                      {"sp": sp, "tp": lax.rem(y + d, n_y) * 2 + core})

    def window_parts(i):
        at = win_rows[i]
        arrival(winb.at[other, at], s.win_recv.at[i]).wait_recv()
        for d in range(1, n_y):
            psend[d - 1, at] = window_part(lax.rem(y + d, n_y), at).astype(BF16)
            part_copy(d, at).start()

    def gate(b):
        name = WEIGHTS[10 + b]
        getattr(loads, name).wait()

        def step(i, _):
            at = pl.ds(pl.multiple_of(i * 256, LANES), 256)
            gates[b, :, at] = jax.nn.sigmoid(dot(all_normed(), getattr(w, name)[:, at]))
            return 0

        lax.fori_loop(0, block // 256, step, 0)

    def take_rows(k):
        for d in range(1, n_x):
            pl.when(takes_row(k, d))(functools.partial(take_row, k, d))

    def attend_row(k, d):
        wait_row(k, d)
        attend(row_slot(k, d), False)

    loads.sinks.wait()
    window(range(1, rows // WINDOW))
    win_copy(0).start()
    take_first(pieces - 1)
    queries_up()
    if n_z > 2:
        take_second(1, pieces // 2)
    pltpu.make_async_copy(wcol.at[core], wcol.at[core], s.w_sems.at[0]).wait()
    arrival(wcol.at[other], s.w_sems.at[1]).wait_recv()
    window_parts(0)
    take_rows(0)
    wait_column(0)
    @pl.when((x == 0) & (z + 1 < n_z))
    def _():
        arrival(turn, s.halo_sem.at[1]).wait_recv()
        relay_copy.start()

    attend(sp, True)
    if n_z > 2:
        take_second(pieces // 2, pieces - 1)

    @pl.when(x + 1 < n_x)
    def _():
        halo_copy.start()


    def take_pieces(k, lo, hi):
        @pl.when(z >= k)
        def _():
            for h in range(lo, hi):
                take_column(k, h)

    def first_window():
        take_halo()
        window(range(1))
        win_copy(1).start()

    def last_parts():
        window_parts(1)

    def attend_halves(slot, wait):
        def halves(i, _):
            @pl.when(i == 1)
            def _():
                wait()

            attend(slot, False, jnp.where(i == 0, core, other))
            return 0

        lax.fori_loop(0, 2, halves, 0)

    def step(k, _):
        @pl.when(k == 4 - parity)
        def _():
            pair_forward()

        @pl.when((z >= k - 1) & (k < n_z))
        def _():
            wait_column(k - 1)
            attend(column_slot(k - 1), False)

        @pl.when((z >= k - 1) & (k == n_z))
        def _():
            attend_halves(column_slot(k - 1), functools.partial(wait_column, k - 1))

        @pl.when(k == 2)
        def _():
            take_pieces(k, pieces - 1, pieces)

        pl.when(k == 4)(last_parts)

        @pl.when(k > 2)
        def _():
            pl.when(x == 0)(functools.partial(take_pieces, k, 0, 1))
            take_pieces(k, 1, pieces // 2)

        for d in range(1, n_x):
            @pl.when((z >= k - 2) & takes_row(k - 2, d))
            def _():
                attend_row(k - 2, d)

        @pl.when(k > 2)
        def _():
            take_pieces(k, pieces // 2, pieces - 1)

        pl.when(k == 3)(first_window)

        @pl.when(k > 2)
        def _():
            take_pieces(k, pieces - 1, pieces)


        @pl.when(z >= k - 1)
        def _():
            take_rows(k - 1)

        @pl.when(x > 0)
        def _():
            take_pieces(k + 1, 0, 1)

        return 0

    lax.fori_loop(2, max(n_z, 4) + 1, step, 0)

    @pl.when(z == n_z - 1)
    def _():
        for d in range(1, n_x):
            @pl.when(takes_row(n_z - 1, d))
            def _():
                attend_halves(row_slot(n_z - 1, d), functools.partial(wait_row, n_z - 1, d))


    def gather(part):
        own = lat.at[tp, part]
        sends = [
            remote(own, own, s.sent.at[1], s.y_recv.at[part, d - 1],
                   {"sp": sp, "tp": lax.rem(y + d, n_y) * 2 + core})
            for d in range(1, n_y)
        ]
        sends.append(remote(own, own, s.sent.at[1], s.s_recv.at[part], to_sibling))
        return sends

    def forward(part):
        for d in range(1, n_y):
            ref = lat.at[lax.rem(y + n_y - d, n_y) * 2 + core, part]
            arrival(ref, s.y_recv.at[part, d - 1]).wait_recv()
            remote(ref, ref, s.sent.at[1], s.s_recv.at[part], to_sibling).start()

    def arrived(part):
        arrival(lat.at[pl.ds(0, n_y), part], s.s_recv.at[part]).wait_recv()

    for part in range(out_parts):
        at = slice(part * out_rows, (part + 1) * out_rows)
        for h in range(lat_heads):
            lat[tp, part, :, h * VDIM : (h + 1) * VDIM] = (
                acc[h, :, at] * (1.0 / total[h, :, at])).T.astype(BF16)
        start(gather(part))
    gate(0)
    gate(1)
    window_branch = window_part(y, pl.ds(0, rows))
    for d in range(1, n_y):
        arrival(precv.at[d - 1], s.p_recv.at[d - 1]).wait_recv()
        window_branch = window_branch + precv[d - 1].astype(F32)
    gates[0] = gates[0] * window_branch
    column_local.wait()
    arrival(columns.at[sibling], s.col_recv.at[0]).wait_recv()
    for d in range(1, n_y):
        base = lax.rem(y + n_y - d, n_y) * 2
        if paired:
            arrival(columns.at[base + 1 - parity], s.pair_recv.at[d - 1]).wait_recv()
        else:
            arrival(columns.at[pl.ds(base, 2)], s.col_recv.at[d]).wait_recv()
    def leave(ref, send):
        remote(ref, ref, send, send, to_sibling).wait_send()

    leave(ownf.at[pl.ds(0, half)], s.sent.at[0])
    for d in range(1, n_y):
        leave(ownf, s.sent.at[0])
    leave(normed.at[core], s.sent.at[0])
    latq_copy.wait_send()
    leave(wcol.at[core], s.sent.at[0])
    leave(columns.at[tp], s.sent.at[0])

    @when_across
    def _():
        for d in range(1, n_y):
            leave(columns.at[pl.ds(0, 2)], s.sent.at[0])

    if paired:
        for d in range(1, n_y):
            pair_copy(d).wait_send()
    for i in range(2):
        win_copy(i).wait_send()
    for d in range(1, n_y):
        leave(psend.at[d - 1], s.sent.at[0])

    @pl.when((x + 1 < n_x) | (z + 1 < n_z))
    def _():
        halo_copy.wait_send()

    @pl.when((x == 0) & (z + 1 < n_z))
    def _():
        relay_copy.wait_send()

    def drain(k, _):
        @pl.when(z >= k)
        def _():
            own = kvb.at[column_slot(k), core]

            @pl.when(z + 1 < n_z)
            def _():
                leave(own, s.sent.at[0])

            leave(own, s.sent.at[0])
            for d in range(1, n_x):
                to = lax.rem(x + d, n_x)
                fewer = [detoured(k, h, to) for h in DETOURS]

                @pl.when(sends_row(k, d) & ~(fewer[0] | fewer[1]))
                def _():
                    leave(own, s.sent.at[0])

                @pl.when(fewer[0] | fewer[1])
                def _():
                    leave(own.at[pl.ds(0, pieces - 1)], s.sent.at[0])

                for i in range(2):
                    @pl.when(takes_row(k, d) & passes_detour(k, i))
                    def _():
                        detour_copy(k, d, i).wait_send()

                @pl.when(takes_row(k, d))
                def _():
                    leave(own, s.sent.at[0])

        return 0

    lax.fori_loop(0, n_z, drain, 0)

    for part in range(out_parts):
        at = slice(part * out_rows, (part + 1) * out_rows)
        forward(part)
        arrived(part)
        latent_branch = jnp.zeros((out_rows, block), F32)
        for j in range(n_tp):
            latent_branch = latent_branch + dot(lat[j, part], columns[j])
        out[at, :] = (gates[0, at] + gates[1, at] * latent_branch).astype(BF16)

    for _ in range(n_y + n_y - 1):
        leave(lat.at[tp], s.sent.at[1])


def on_device(dims, features, norm_gain, w_query, w_key, w_value, head_sinks, w_query_latent,
              w_kv_latent, w_rope_key, query_latent_gain, kv_latent_gain, w_query_content,
              w_query_rotary, w_key_up, w_value_up, w_branch_window, w_branch_latent,
              w_gate_window, w_gate_latent):
    n_sp, n_tp, n_x = dims
    n_z, n_y = n_sp // n_x, n_tp // 2
    rows, block = features.shape
    width = norm_gain.shape[0]
    latent = w_kv_latent.shape[1]
    lat_heads = w_key_up.shape[1] // NOPE
    half_width = ROPE // 2
    entry = np.arange(ROPE, dtype=np.int32) % half_width
    frequency = (np.float32(THETA) ** (-entry.astype(np.float32) / np.float32(half_width))).astype(np.float32)[None, :]
    weights = (w_kv_latent, w_rope_key.T, w_key, w_value, w_query, w_query_latent, w_query_content,
               w_query_rotary, w_key_up, w_value_up, w_gate_window, w_gate_latent)
    smalls = (norm_gain[None, :], head_sinks[None, :], query_latent_gain[None, :], kv_latent_gain[None, :],
              jnp.asarray(frequency))
    branch_rows = w_branch_window.shape[0]
    pieces = PIECES
    piece = rows // 2 // pieces
    out_parts = rows // LANES
    merge = w_key.shape[1] % LANES == 0
    hbm = pl.BlockSpec(memory_space=pl.ANY)
    dma = pltpu.SemaphoreType.DMA
    vm = pltpu.VMEM
    scratch = dict(
        **{"small_" + n: (pltpu.SMEM if n == "sinks" else vm)(a.shape, F32) for n, a in zip(SMALL, smalls)},
        **{"w_" + n: vm(a.shape, BF16) for n, a in zip(WEIGHTS, weights) if not (merge and n in MERGED or n in UP)},
        up=vm((latent, w_key_up.shape[1] + w_value_up.shape[1]), BF16),
        **(dict(w_qkv=vm((width, 2 * w_key.shape[1] + w_query.shape[1]), BF16)) if merge else {}),
        ownf=vm((rows, block), BF16),
        feat=vm((n_tp, rows // 2, block), BF16),
        normed=vm((2, pieces, piece, width), BF16),
        latq=vm((2, rows // 2, latent), BF16),
        wcol=vm((2, n_y, branch_rows, block), BF16),
        columns=vm((n_tp, w_branch_latent.shape[0], block), BF16),
        psend=vm((n_y - 1, rows, block), BF16),
        precv=vm((n_y - 1, rows, block), BF16),
        kvb=vm((n_sp, 2, pieces, piece + SUBLANES, latent), BF16),
        local_kv=vm((rows, 2 * w_key.shape[1]), BF16),
        halo=vm((WINDOW, 2 * w_key.shape[1]), BF16),
        turn=vm((WINDOW, 2 * w_key.shape[1]), BF16),
        queries=vm((rows, w_query.shape[1]), BF16),
        q_full=vm((lat_heads, NOPE + LANES, rows), BF16),
        gates=vm((2, rows, block), F32),
        winb=vm((2, rows, w_query.shape[1]), BF16),
        lat=vm((n_tp, out_parts, rows // out_parts, lat_heads * VDIM), BF16),
        top=vm((lat_heads, 1, rows), F32),
        total=vm((lat_heads, 1, rows), F32),
        acc=vm((lat_heads, VDIM, rows), F32),
        cosine=vm((2, pieces, piece, ROPE), F32),
        sine=vm((2, pieces, piece, ROPE), F32),
        own_sem=dma((2,)),
        sent=dma((2,)),
        small_sem=dma((len(SMALL),)),
        w_sem=dma((len(weights) - 1 - 2 * merge,)),
        f_recv=dma((pieces,)),
        n_sems=dma((1,)),
        q_sems=dma((1,)),
        w_sems=dma((2,)),
        col_own=dma((1,)),
        col_recv=dma((n_y,)),
        pair_recv=dma((n_y - 1,)),
        halo_sem=dma((2,)),
        win_recv=dma((2,)),
        p_recv=dma((n_y - 1,)),
        y_recv=dma((out_parts, n_y - 1)),
        s_recv=dma((out_parts,)),
        z_recv=dma((pieces, n_z - 1)),
        r_recv=dma((2, n_z - 2, n_x - 1)),
        x_recv=dma((n_z, n_x - 1)),
        c_recv=dma((n_z,)),
        d_recv=dma((n_z, n_x - 1)),
    )
    return pl.pallas_call(
        functools.partial(kernel, dims, tuple(scratch)),
        out_shape=pltpu.VMEM((rows, block), BF16),
        in_specs=[hbm] * (1 + len(smalls) + len(weights) + 2),
        out_specs=pl.BlockSpec(memory_space=pltpu.VMEM),
        scratch_shapes=list(scratch.values()),
        compiler_params=pltpu.CompilerParams(
            collective_id=0, has_side_effects=True, vmem_limit_bytes=60 * 1024 * 1024
        ),
    )(features, *smalls, *weights, w_branch_window, w_branch_latent)


def solution(mesh):
    n_sp, n_tp = mesh.shape["sp"], mesh.shape["tp"]
    n_x = 1
    while n_sp % (2 * n_x) == 0 and 8 * n_x * n_x <= n_sp:
        n_x *= 2
    return jax.shard_map(
        functools.partial(on_device, (n_sp, n_tp, n_x)),
        mesh=mesh,
        in_specs=(
            P("sp", "tp"),
            P(),
            P(None, "tp"),
            P(None, "tp"),
            P(None, "tp"),
            P("tp"),
            P(),
            P(),
            P(),
            P(),
            P(),
            P(None, "tp"),
            P(None, "tp"),
            P(None, "tp"),
            P(None, "tp"),
            P("tp", None),
            P("tp", None),
            P(None, "tp"),
            P(None, "tp"),
        ),
        out_specs=P("sp", "tp"),
        check_vma=False,
    )
```
